256 devices in a mesh: kv: 32 (over z, x), tp: 8 (over y, core).
Axes of the slice: x: 4, y: 4, z: 8, core: 2. Of those that a mesh axis runs over, the one named last changes fastest.
Arguments:
- tokens: bfloat16 [384, 2048], P('tp', 'kv'), may hold values from -10.5 to 10.5
- norm_gain: float32 [2048], P('kv'), may hold values from 0.1 to 1.9
- w_query: bfloat16 [2048, 2048], P('kv', 'tp'), may hold values from -0.125 to 0.125
- w_forget: bfloat16 [2048, 2048], P('kv', 'tp'), may hold values from -0.125 to 0.125
- w_input: bfloat16 [2048, 2048], P('kv', 'tp'), may hold values from -0.125 to 0.125
- w_gate: bfloat16 [2048, 2048], P('kv', 'tp'), may hold values from -0.125 to 0.125
- lower_bound: float32 [2048], P('tp'), may hold values from 0 to 0.9
- head_gain: float32 [16, 128], P('tp'), may hold values from 0.1 to 1.9
- recur_state: float32 [384, 16, 128, 128], P('kv', 'tp'), may hold values from -3 to 3
- w_out: bfloat16 [2048, 2048], P('tp', 'kv'), may hold values from -0.125 to 0.125
- mixer_gain: float32 [2048], P('kv'), may hold values from 0.1 to 1.9
- w_up: bfloat16 [2048, 8192], P('kv', 'tp'), may hold values from -0.125 to 0.125
- w_down: bfloat16 [8192, 2048], P('tp', 'kv'), may hold values from -0.0625 to 0.0625
Outputs:
- next_tokens: bfloat16 [384, 2048], P('tp', 'kv')
- next_state: float32 [384, 16, 128, 128], P('kv', 'tp')
The draws below stay inside these ranges and needn't reach their ends.
All inputs are finite; a program needn't handle non-finite values.
Results may differ from the reference program's by a relative error of at most 0.03.
Values may be sent and summed in bfloat16 or wider, within the bound.
A program may use at most 64 MiB of HBM per device.

```python
import jax
import jax.numpy as jnp
from jax import lax

D = 2048
HEADS = 16
KEY = 128
VAL = 128
FF = 8192
SEQS = 384
N_TP = 8


def draw_tokens(key, part):
    first_key = jax.random.fold_in(key, 11)
    column = jnp.arange(D, dtype=jnp.float32) / D - 0.5
    base_draw = jnp.clip(jax.random.normal(first_key, (SEQS, D), jnp.float32), -6.0, 6.0)
    values = base_draw * jnp.exp(jnp.log(3.0) * column)[None, :]
    return values.astype(jnp.bfloat16)


def block_scale(own_key, shape, pieces, least, high):
    factor_of, own = 1.0, jax.random.fold_in(own_key, 6)
    for axis_at, parts in pieces:
        heights = jnp.exp(jax.random.uniform(jax.random.fold_in(own, axis_at), (parts,), jnp.float32, least / len(pieces), high / len(pieces)))
        factor_of = factor_of * jnp.repeat(heights, shape[axis_at] // parts).reshape([-1 if axis == axis_at else 1 for axis in range(len(shape))])
    return factor_of


def noise(key, dims, width, most, split=(), held_as=jnp.bfloat16):
    drawn = width * jax.random.normal(key, dims, jnp.float32)
    if split:
        drawn = drawn * block_scale(key, dims, split, -0.22, 0.18)
    return jnp.clip(drawn, -most, most).astype(held_as)


def setup_inputs(seed: int = 0) -> dict:
    key_list = jax.random.split(jax.random.key(seed), 14)
    return {
        "tokens": draw_tokens(jax.random.fold_in(key_list[13], 71), 0),
        "norm_gain": jnp.clip(1.0 + 0.18 * jax.random.normal(key_list[1], (D,), jnp.float32), 0.1, 1.9),
        "w_query": noise(key_list[2], (D, HEADS * KEY), D ** -0.5, 0.125, ((0, 32), (1, 8))),
        "w_forget": noise(key_list[3], (D, HEADS * KEY), D ** -0.5, 0.125, ((0, 32), (1, 8))),
        "w_input": noise(key_list[4], (D, HEADS * VAL), D ** -0.5, 0.125, ((0, 32), (1, 8))),
        "w_gate": noise(key_list[5], (D, HEADS * VAL), D ** -0.5, 0.125, ((0, 32), (1, 8))),
        "lower_bound": jnp.clip(0.9 * jax.random.uniform(key_list[6], (HEADS * KEY,), jnp.float32) ** block_scale(key_list[6], (HEADS * KEY,), ((0, 8),), -0.2, 0.2), 0.0, 0.9),
        "head_gain": jnp.clip(1.0 + 0.18 * jax.random.normal(key_list[7], (HEADS, VAL), jnp.float32), 0.1, 1.9),
        "recur_state": noise(key_list[8], (SEQS, HEADS, KEY, VAL), 0.5, 3.0, ((0, 32), (1, 8)), jnp.float32),
        "w_out": noise(key_list[9], (HEADS * VAL, D), (HEADS * VAL) ** -0.5, 0.125, ((0, 8), (1, 32))),
        "mixer_gain": jnp.clip(1.0 + 0.18 * jax.random.normal(key_list[10], (D,), jnp.float32), 0.1, 1.9),
        "w_up": noise(key_list[11], (D, FF), D ** -0.5, 0.125, ((0, 32), (1, 8))),
        "w_down": noise(key_list[12], (FF, D), FF ** -0.5, 0.0625, ((0, 8), (1, 32))),
    }


NORM_EPS = 1e-05

def project(row_block, norm_scale, weight):
    tokens_f = row_block.astype(jnp.float32)
    row_scale = lax.rsqrt(lax.optimization_barrier(jnp.mean(tokens_f * tokens_f, axis=1)) + NORM_EPS)
    normed = (tokens_f * norm_scale).astype(jnp.bfloat16)
    return jnp.dot(normed, weight, preferred_element_type=jnp.float32) * row_scale[:, None]

def grouped(values_bf, weight):
    count = values_bf.shape[0]
    grouped_vals = values_bf.reshape(count, N_TP, -1).astype(jnp.float32)
    grouped_mats = weight.reshape(N_TP, -1, weight.shape[1]).astype(jnp.float32)
    partials = jnp.einsum('rgc,gcd->grd', grouped_vals, grouped_mats)
    return lax.optimization_barrier(jnp.sum(partials.astype(jnp.bfloat16).astype(jnp.float32), axis=0))

def reference(tokens, norm_gain, w_query, w_forget, w_input, w_gate, lower_bound, head_gain, recur_state, w_out, mixer_gain, w_up, w_down):
    count = tokens.shape[0]
    queries = project(tokens, norm_gain, w_query).reshape(count, HEADS, KEY)
    forget_raw = project(tokens, norm_gain, w_forget).reshape(count, HEADS, KEY)
    values_in = project(tokens, norm_gain, w_input).reshape(count, HEADS, VAL)
    gate_raw = project(tokens, norm_gain, w_gate)
    bound = lower_bound.reshape(HEADS, KEY)
    forget = bound + (1.0 - bound) * jax.nn.sigmoid(forget_raw)
    next_state = forget[..., None] * recur_state + (1.0 - forget)[..., None] * values_in[:, :, None, :]
    read_out = jnp.einsum('rhk,rhkv->rhv', queries, next_state, precision=lax.Precision.HIGHEST)
    read_out = read_out * lax.rsqrt(lax.optimization_barrier(jnp.mean(read_out * read_out, axis=2, keepdims=True)) + NORM_EPS) * head_gain
    mixture = (read_out.reshape(count, HEADS * VAL) * jax.nn.silu(gate_raw)).astype(jnp.bfloat16)
    mixed_rows = (tokens.astype(jnp.float32) + grouped(mixture, w_out)).astype(jnp.bfloat16)
    hidden_pre = project(mixed_rows, mixer_gain, w_up)
    hidden = jnp.square(jax.nn.relu(hidden_pre)).astype(jnp.bfloat16)
    next_tokens = (mixed_rows.astype(jnp.float32) + grouped(hidden, w_down)).astype(jnp.bfloat16)
    return (next_tokens, next_state)
```

```python
import functools

import jax
import jax.numpy as jnp
from jax import lax
from jax.experimental import pallas as pl
from jax.experimental.pallas import tpu as pltpu
from jax.sharding import PartitionSpec as P

NORM_EPS = 1e-05
MESH = pl.DeviceIdType.MESH
F32 = jnp.float32
BF16 = jnp.bfloat16

NZ, NX, NT = 8, 4, 8
WIDTH = 2048.0


def far_first(step, size):
    return ((step + 1) // 2) * (1 - 2 * (step % 2)) + size // 2


def wait_for(ref, sem):
    pltpu.make_async_copy(ref, ref, sem).wait()


def swap_lanes(value):
    return pltpu.roll(value, 64, 1)


def dot_t(a, b):
    return lax.dot_general(a, b, (((1,), (1,)), ((), ())), preferred_element_type=F32)


def low_lanes(shape):
    return lax.broadcasted_iota(jnp.int32, shape, 1) < 64


def unpacked(pieces):
    low = low_lanes(pieces[0].shape)
    swapped = [swap_lanes(p) for p in pieces]
    first = [jnp.where(low, pieces[i], swapped[i + 1]).astype(BF16) for i in (0, 2)]
    second = [jnp.where(low, swapped[i], pieces[i + 1]).astype(BF16) for i in (0, 2)]
    return jnp.concatenate(
        [jnp.concatenate(first, axis=1), jnp.concatenate(second, axis=1)], axis=0
    )


def row_squares(pieces):
    total = pieces[0] * pieces[0]
    for p in pieces[1:]:
        total = total + p * p
    total = jnp.concatenate([total, jnp.zeros((64, 128), F32)], axis=0)
    high = total.astype(BF16)
    rest = (total - high.astype(F32)).astype(BF16)
    lane = lax.broadcasted_iota(jnp.int32, (8, 128), 1)
    row = lax.broadcasted_iota(jnp.int32, (8, 128), 0)
    pick = jnp.where((lane // 64) == row, 1.0, 0.0).astype(BF16)
    dims = (((1,), (1,)), ((), ()))
    sums = lax.dot_general(pick, high, dims, preferred_element_type=F32)
    sums = sums + lax.dot_general(pick, rest, dims, preferred_element_type=F32)
    return sums[0:2, :]


def column_of(values, base, period):
    lane = lax.broadcasted_iota(jnp.int32, (24, 256), 1)
    row = lax.broadcasted_iota(jnp.int32, (24, 256), 0)
    return jnp.sum(
        jnp.where(lane == base + row % period, values, 0.0), axis=1, keepdims=True
    )


def kernel(
    tokens_hbm,
    gains_hbm,
    wq_hbm,
    wf_hbm,
    wi_hbm,
    wg_hbm,
    bound_hbm,
    head_gain_hbm,
    state_hbm,
    wout_hbm,
    wup_hbm,
    wdown_hbm,
    out_ref,
    next_hbm,
    tok_v,
    gain_v,
    w4_v,
    bound_v,
    head_gain_v,
    state_v,
    next_v,
    wout_v,
    wup_v,
    wdown_v,
    gains,
    w_first,
    w_up,
    w_down,
    w_out,
    tok_all,
    sq1,
    proj_out,
    proj_in,
    mix_own,
    mix_all,
    mixed_all,
    sq2,
    up_out,
    up_in,
    hidden_all,
    down_out,
    down_in,
    read_v,
    in_sems,
    send_sems,
    recv_sems,
):
    kv, t = lax.axis_index("kv"), lax.axis_index("tp")
    z, x = kv // NX, kv % NX
    y, core = t // 2, t % 2
    rows_at = (t + NZ - z) % NZ
    has_self = t == (2 * z) % NZ

    def in_plane(i):
        px = (x + far_first(i // 8, 4)) % 4
        py = (y + far_first((i % 8) // 2, 4)) % 4
        pc = (core + 1 - i % 2) % 2
        return px, 2 * py + pc

    def in_column(i):
        pz = (z + far_first(i // 4, 8)) % 8
        px = (x + far_first(i % 4, 4)) % 4
        return pz, px

    def copy_to(src, dst, k, pkv, pt):
        return pltpu.make_async_remote_copy(
            src_ref=src,
            dst_ref=dst,
            send_sem=send_sems.at[k],
            recv_sem=recv_sems.at[k],
            device_id=(pkv, pt),
            device_id_type=MESH,
        )

    barrier = pltpu.get_barrier_semaphore()

    def tell(pkv, pt):
        pl.semaphore_signal(barrier, inc=1, device_id=(pkv, pt), device_id_type=MESH)

    def greet_plane(i, c):
        px, pt = in_plane(i)
        tell(z * NX + px, pt)
        return c

    def greet_column(i, c):
        pz, px = in_column(i)
        tell(pz * NX + px, t)
        return c

    lax.fori_loop(0, 31, greet_column, 0)

    def greet_mix(i, c):
        skv, st = rows_at * NX + i // 8, i % 8

        @pl.when(jnp.logical_or(skv != kv, st != t))
        def _():
            tell(skv, st)

        return c

    lax.fori_loop(0, 32, greet_mix, 0)
    lax.fori_loop(0, 31, greet_plane, 0)

    loads = [
        pltpu.make_async_copy(tokens_hbm, tok_v, in_sems.at[0]),
        pltpu.make_async_copy(gains_hbm, gain_v, in_sems.at[1]),
        pltpu.make_async_copy(wq_hbm, w4_v.at[0], in_sems.at[2]),
        pltpu.make_async_copy(wf_hbm, w4_v.at[1], in_sems.at[3]),
        pltpu.make_async_copy(wi_hbm, w4_v.at[2], in_sems.at[4]),
        pltpu.make_async_copy(wg_hbm, w4_v.at[3], in_sems.at[5]),
        pltpu.make_async_copy(wout_hbm, wout_v, in_sems.at[6]),
        pltpu.make_async_copy(wup_hbm, wup_v, in_sems.at[7]),
        pltpu.make_async_copy(wdown_hbm, wdown_v, in_sems.at[8]),
        pltpu.make_async_copy(bound_hbm, bound_v, in_sems.at[9]),
        pltpu.make_async_copy(head_gain_hbm, head_gain_v, in_sems.at[10]),
        pltpu.make_async_copy(state_hbm, state_v, in_sems.at[11]),
    ]
    for load in loads:
        load.start()

    loads[0].wait()
    tok_f = tok_v[...].astype(F32)
    tok_all[x * NT + t] = jnp.concatenate([tok_f[0:24], tok_f[24:48]], axis=1).astype(BF16)
    loads[1].wait()
    g = gain_v[...]
    gains[x] = jnp.concatenate([g, g], axis=1)
    for k in range(2, 9):
        loads[k].wait()
    w_first[x] = w4_v[x]
    w_up[x] = wup_v[:, pl.ds(pl.multiple_of(x * 256, 256), 256)]
    w_out[t] = wout_v[...]
    w_down[x] = wdown_v[:, pl.ds(pl.multiple_of(x * 256, 256), 256)]

    pl.semaphore_wait(barrier, 31 + 31 + 32 - has_self.astype(jnp.int32))

    def send_tokens(i, c):
        px, pt = in_plane(i)
        copy_to(tok_all.at[x * NT + t], tok_all.at[x * NT + t], 0, z * NX + px, pt).start()
        return c

    def send_first(i, c):
        px = (x + far_first(i, 4)) % 4
        copy_to(gains.at[x], gains.at[x], 1, z * NX + px, t).start()
        copy_to(w4_v.at[px], w_first.at[x], 2, z * NX + px, t).start()
        return c

    lax.fori_loop(0, 3, send_first, 0)
    lax.fori_loop(0, 31, send_tokens, 0)

    wait_for(gains.at[pl.ds(0, 3)], recv_sems.at[1])
    wait_for(tok_all.at[pl.ds(0, 31)], recv_sems.at[0])

    def send_wout(i, c):
        py = (y + far_first(i // 2, 4)) % 4
        pt = 2 * py + (core + 1 - i % 2) % 2
        copy_to(w_out.at[t], w_out.at[t], 3, kv, pt).start()
        return c

    lax.fori_loop(0, 7, send_wout, 0)

    raw = [
        tok_all[pl.ds(NT * q, NT)].astype(F32).reshape(192, 128) for q in range(NX)
    ]
    sq1[z] = row_squares(raw)
    lhs = unpacked([raw[q] * gains[q, 0:1, :] for q in range(NX)])
    wait_for(w_first.at[pl.ds(0, 3)], recv_sems.at[2])
    partial = jnp.dot(lhs, w_first[...].reshape(256, 256), preferred_element_type=F32)

    for half in range(2):
        for pz in range(NZ):
            at = half * 192 + pz * 24
            left = partial[at : at + 24, 0:128]
            right = partial[at : at + 24, 128:256]
            proj_out[pz * NX + 2 * half] = jnp.concatenate(
                [left[0:12], right[0:12]], axis=0
            ).astype(BF16)
            proj_out[pz * NX + 2 * half + 1] = jnp.concatenate(
                [left[12:24], right[12:24]], axis=0
            ).astype(BF16)

    def send_sq1(i, c):
        pz = (z + far_first(i, 8)) % 8
        copy_to(sq1.at[z], sq1.at[z], 4, pz * NX + x, t).start()
        return c

    def send_proj(i, c):
        pz, px = in_column(i)
        copy_to(proj_out.at[pz * NX + px], proj_in.at[kv], 5, pz * NX + px, t).start()
        return c

    lax.fori_loop(0, 7, send_sq1, 0)
    lax.fori_loop(0, 31, send_proj, 0)
    proj_in[kv] = proj_out[kv]

    def send_ffn(i, c):
        px = (x + far_first(i, 4)) % 4
        cols = pl.ds(pl.multiple_of(px * 256, 256), 256)
        copy_to(wup_v.at[:, cols], w_up.at[x], 6, z * NX + px, t).start()
        copy_to(wdown_v.at[:, cols], w_down.at[x], 7, z * NX + px, t).start()
        return c

    lax.fori_loop(0, 3, send_ffn, 0)

    for k in range(9, 12):
        loads[k].wait()
    wait_for(sq1.at[pl.ds(0, 7)], recv_sems.at[4])
    wait_for(proj_in.at[pl.ds(0, 31)], recv_sems.at[5])

    squares = sq1[0]
    for q in range(1, NZ):
        squares = squares + sq1[q]
    square_row = jnp.where(x // 2 == 0, squares[0:1, :], squares[1:2, :])
    row_scale = lax.rsqrt(
        column_of(square_row, z * 24 + (x % 2) * 12, 12) / WIDTH + NORM_EPS
    )
    owned = []
    for q in range(NX):
        total = proj_in[q].astype(F32)
        for r in range(1, NZ):
            total = total + proj_in[r * NX + q].astype(F32)
        owned.append(total * row_scale)
    queries, forget_raw, values_in, gate_raw = owned
    head0 = lax.broadcasted_iota(jnp.int32, (24, 128), 0) < 12
    bound = jnp.where(head0, bound_v[0:1, :], bound_v[1:2, :])
    head_gain = jnp.where(head0, head_gain_v[0:1, :], head_gain_v[1:2, :])
    forget = bound + (1.0 - bound) * jax.nn.sigmoid(forget_raw)
    pad = jnp.zeros((104, 128), F32)
    forget_t = jnp.concatenate([forget, pad], axis=0).T
    queries_t = jnp.concatenate([queries, pad], axis=0).T
    for j in range(24):
        h, s = j // 12, j % 12
        f = forget_t[:, j : j + 1]
        nxt = f * state_v[s, h] + (1.0 - f) * values_in[j : j + 1, :]
        next_v[s, h] = nxt
        read_v[j : j + 1, :] = jnp.sum(queries_t[:, j : j + 1] * nxt, axis=0, keepdims=True)
    store = pltpu.make_async_copy(next_v, next_hbm, in_sems.at[12])
    store.start()
    read = read_v[...]
    read = read * lax.rsqrt(jnp.mean(read * read, axis=1, keepdims=True) + NORM_EPS) * head_gain
    mix_own[...] = (read * jax.nn.silu(gate_raw)).astype(BF16)

    def send_mix(i, c):
        pz, px = (z + far_first(i // 4, 8)) % 8, (x + far_first(i % 4, 4)) % 4
        pt = (z + pz) % NZ
        away = jnp.logical_or(pz * NX + px != kv, pt != t)

        @pl.when(away)
        def _():
            copy_to(mix_own, mix_all.at[t * NX + x], 8, pz * NX + px, pt).start()

        return c

    lax.fori_loop(0, 32, send_mix, 0)

    @pl.when(has_self)
    def _():
        mix_all[t * NX + x] = mix_own[...]

    wait_for(w_out.at[pl.ds(0, 7)], recv_sems.at[3])

    @pl.when(has_self)
    def _():
        wait_for(mix_all.at[pl.ds(0, 31)], recv_sems.at[8])

    @pl.when(jnp.logical_not(has_self))
    def _():
        wait_for(mix_all, recv_sems.at[8])

    acc = jnp.zeros((96, 128), F32)
    for q in range(NT):
        both = jnp.concatenate([w_out[q, :, 0:128], w_out[q, :, 128:256]], axis=0)
        acc = acc + dot_t(mix_all[4 * q : 4 * q + 4].reshape(96, 128), both)
    folded = []
    for q in range(NX):
        part = acc[24 * q : 24 * q + 24]
        turned = swap_lanes(jnp.concatenate([part[12:24], part[0:12]], axis=0))
        folded.append(part + turned)
    low = low_lanes((24, 128))
    top = jnp.where(low, folded[0], swap_lanes(folded[2]))
    bottom = jnp.where(low, swap_lanes(folded[1]), folded[3])
    attn = jnp.where(head0, top, bottom)
    own_at = x * NT + rows_at
    mixed_all[own_at] = (tok_all[own_at].astype(F32) + attn).astype(BF16)

    def send_mixed(i, c):
        px, pt = in_plane(i)
        copy_to(mixed_all.at[own_at], mixed_all.at[own_at], 9, z * NX + px, pt).start()
        return c

    lax.fori_loop(0, 31, send_mixed, 0)
    wait_for(w_up.at[pl.ds(0, 3)], recv_sems.at[6])
    wait_for(mixed_all.at[pl.ds(0, 31)], recv_sems.at[9])

    raw2 = [
        mixed_all[pl.ds(NT * q, NT)].astype(F32).reshape(192, 128) for q in range(NX)
    ]
    sq2[z] = row_squares(raw2)
    lhs2 = unpacked([raw2[q] * gains[q, 1:2, :] for q in range(NX)])
    partial2 = jnp.dot(lhs2, w_up[...].reshape(256, 256), preferred_element_type=F32)
    for half in range(2):
        for pz in range(NZ):
            at = half * 192 + pz * 24
            up_out[pz, half] = partial2[at : at + 24].astype(BF16)

    def send_up(i, c):
        pz = (z + far_first(i, 8)) % 8
        copy_to(sq2.at[z], sq2.at[z], 10, pz * NX + x, t).start()
        copy_to(up_out.at[pz], up_in.at[z], 11, pz * NX + x, t).start()
        return c

    lax.fori_loop(0, 7, send_up, 0)
    up_in[z] = up_out[z]
    wait_for(sq2.at[pl.ds(0, 7)], recv_sems.at[10])
    squares2 = sq2[0]
    for q in range(1, NZ):
        squares2 = squares2 + sq2[q]
    scales = [
        lax.rsqrt(column_of(squares2[q : q + 1, :], z * 24, 24) / WIDTH + NORM_EPS)
        for q in range(2)
    ]
    wait_for(up_in.at[pl.ds(0, 7)], recv_sems.at[11])

    for half in range(2):
        total = up_in[0, half].astype(F32)
        for q in range(1, NZ):
            total = total + up_in[q, half].astype(F32)
        total = jnp.maximum(total * scales[half], 0.0)
        hidden_all[z, half] = (total * total).astype(BF16)

    def send_hidden(i, c):
        pz = (z + far_first(i, 8)) % 8
        copy_to(hidden_all.at[z], hidden_all.at[z], 12, pz * NX + x, t).start()
        return c

    lax.fori_loop(0, 7, send_hidden, 0)
    wait_for(w_down.at[pl.ds(0, 3)], recv_sems.at[7])
    wait_for(hidden_all.at[pl.ds(0, 7)], recv_sems.at[12])

    partial3 = dot_t(hidden_all[...].reshape(384, 256), w_down[...].reshape(256, 256))
    for pt in range(NT):
        for pair in range(2):
            upper = partial3[48 * pt : 48 * pt + 24, 128 * pair : 128 * pair + 128]
            lower = partial3[48 * pt + 24 : 48 * pt + 48, 128 * pair : 128 * pair + 128]
            down_out[pt * NX + 2 * pair] = jnp.where(low, upper, swap_lanes(lower)).astype(BF16)
            down_out[pt * NX + 2 * pair + 1] = jnp.where(low, swap_lanes(upper), lower).astype(
                BF16
            )

    def send_down(i, c):
        px, pt = in_plane(i)
        copy_to(
            down_out.at[pt * NX + px], down_in.at[t * NX + x], 13, z * NX + px, pt
        ).start()
        return c

    lax.fori_loop(0, 31, send_down, 0)
    down_in[t * NX + x] = down_out[t * NX + x]
    wait_for(down_in.at[pl.ds(0, 31)], recv_sems.at[13])
    total = down_in[0].astype(F32)
    for q in range(1, 32):
        total = total + down_in[q].astype(F32)
    total = mixed_all[x * NT + t].astype(F32) + total
    out_ref[...] = jnp.concatenate([total[:, 0:64], total[:, 64:128]], axis=0).astype(BF16)

    store.wait()
    wait_for(tok_all.at[pl.ds(0, 31)], send_sems.at[0])
    wait_for(gains.at[pl.ds(0, 3)], send_sems.at[1])
    wait_for(w_first.at[pl.ds(0, 3)], send_sems.at[2])
    wait_for(w_out.at[pl.ds(0, 7)], send_sems.at[3])
    wait_for(sq1.at[pl.ds(0, 7)], send_sems.at[4])
    wait_for(proj_in.at[pl.ds(0, 31)], send_sems.at[5])
    wait_for(w_up.at[pl.ds(0, 3)], send_sems.at[6])
    wait_for(w_down.at[pl.ds(0, 3)], send_sems.at[7])

    @pl.when(has_self)
    def _():
        wait_for(mix_all.at[pl.ds(0, 31)], send_sems.at[8])

    @pl.when(jnp.logical_not(has_self))
    def _():
        wait_for(mix_all, send_sems.at[8])

    wait_for(mixed_all.at[pl.ds(0, 31)], send_sems.at[9])
    wait_for(sq2.at[pl.ds(0, 7)], send_sems.at[10])
    wait_for(up_in.at[pl.ds(0, 7)], send_sems.at[11])
    wait_for(hidden_all.at[pl.ds(0, 7)], send_sems.at[12])
    wait_for(down_in.at[pl.ds(0, 31)], send_sems.at[13])


def body(
    tokens,
    norm_gain,
    w_query,
    w_forget,
    w_input,
    w_gate,
    lower_bound,
    head_gain,
    recur_state,
    w_out,
    mixer_gain,
    w_up,
    w_down,
):
    gains = jnp.stack([norm_gain, mixer_gain])
    bound = lower_bound.reshape(2, 128)
    any_spec = pl.BlockSpec(memory_space=pl.ANY)
    return pl.pallas_call(
        kernel,
        out_shape=(
            jax.ShapeDtypeStruct(tokens.shape, tokens.dtype),
            jax.ShapeDtypeStruct(recur_state.shape, recur_state.dtype),
        ),
        in_specs=[any_spec] * 12,
        out_specs=(pl.BlockSpec(memory_space=pltpu.VMEM), any_spec),
        scratch_shapes=[
            pltpu.VMEM((48, 64), BF16),
            pltpu.VMEM((2, 64), F32),
            pltpu.VMEM((4, 64, 256), BF16),
            pltpu.VMEM((2, 128), F32),
            pltpu.VMEM((2, 128), F32),
            pltpu.VMEM((12, 2, 128, 128), F32),
            pltpu.VMEM((12, 2, 128, 128), F32),
            pltpu.VMEM((64, 256), BF16),
            pltpu.VMEM((64, 1024), BF16),
            pltpu.VMEM((64, 1024), BF16),
            pltpu.VMEM((4, 2, 128), F32),
            pltpu.VMEM((4, 64, 256), BF16),
            pltpu.VMEM((4, 64, 256), BF16),
            pltpu.VMEM((4, 64, 256), BF16),
            pltpu.VMEM((8, 64, 256), BF16),
            pltpu.VMEM((32, 24, 128), BF16),
            pltpu.VMEM((8, 2, 256), F32),
            pltpu.VMEM((32, 24, 128), BF16),
            pltpu.VMEM((32, 24, 128), BF16),
            pltpu.VMEM((24, 128), BF16),
            pltpu.VMEM((32, 24, 128), BF16),
            pltpu.VMEM((32, 24, 128), BF16),
            pltpu.VMEM((8, 2, 256), F32),
            pltpu.VMEM((8, 2, 24, 256), BF16),
            pltpu.VMEM((8, 2, 24, 256), BF16),
            pltpu.VMEM((8, 2, 24, 256), BF16),
            pltpu.VMEM((32, 24, 128), BF16),
            pltpu.VMEM((32, 24, 128), BF16),
            pltpu.VMEM((24, 128), F32),
            pltpu.SemaphoreType.DMA((13,)),
            pltpu.SemaphoreType.DMA((14,)),
            pltpu.SemaphoreType.DMA((14,)),
        ],
        compiler_params=pltpu.CompilerParams(collective_id=0, has_side_effects=True),
        name="decode_layer",
    )(
        tokens,
        gains,
        w_query,
        w_forget,
        w_input,
        w_gate,
        bound,
        head_gain,
        recur_state,
        w_out.T,
        w_up,
        w_down.T,
    )


def solution(mesh):
    in_specs = (
        P("tp", "kv"),
        P("kv"),
        P("kv", "tp"),
        P("kv", "tp"),
        P("kv", "tp"),
        P("kv", "tp"),
        P("tp"),
        P("tp", None),
        P("kv", "tp", None, None),
        P("tp", "kv"),
        P("kv"),
        P("kv", "tp"),
        P("tp", "kv"),
    )
    out_specs = (P("tp", "kv"), P("kv", "tp", None, None))
    return jax.shard_map(body, mesh=mesh, in_specs=in_specs, out_specs=out_specs, check_vma=False)
```

```python
import functools

import jax
import jax.numpy as jnp
from jax import lax
from jax.experimental import pallas as pl
from jax.experimental.pallas import tpu as pltpu
from jax.sharding import PartitionSpec as P

NORM_EPS = 1e-05
MESH = pl.DeviceIdType.MESH
F32 = jnp.float32
BF16 = jnp.bfloat16

NZ, NX, NT = 8, 4, 8
WIDTH = 2048.0


def far_first(step, size):
    return ((step + 1) // 2) * (1 - 2 * (step % 2)) + size // 2


def wait_for(ref, sem):
    pltpu.make_async_copy(ref, ref, sem).wait()


def swap_lanes(value):
    return pltpu.roll(value, 64, 1)


def dot_t(a, b):
    return lax.dot_general(a, b, (((1,), (1,)), ((), ())), preferred_element_type=F32)


def low_lanes(shape):
    return lax.broadcasted_iota(jnp.int32, shape, 1) < 64


def unpacked(pieces):
    low = low_lanes(pieces[0].shape)
    swapped = [swap_lanes(p) for p in pieces]
    first = [jnp.where(low, pieces[i], swapped[i + 1]).astype(BF16) for i in (0, 2)]
    second = [jnp.where(low, swapped[i], pieces[i + 1]).astype(BF16) for i in (0, 2)]
    return jnp.concatenate(
        [jnp.concatenate(first, axis=1), jnp.concatenate(second, axis=1)], axis=0
    )


def row_squares(pieces):
    total = pieces[0] * pieces[0]
    for p in pieces[1:]:
        total = total + p * p
    total = jnp.concatenate([total, jnp.zeros((64, 128), F32)], axis=0)
    high = total.astype(BF16)
    rest = (total - high.astype(F32)).astype(BF16)
    lane = lax.broadcasted_iota(jnp.int32, (8, 128), 1)
    row = lax.broadcasted_iota(jnp.int32, (8, 128), 0)
    pick = jnp.where((lane // 64) == row, 1.0, 0.0).astype(BF16)
    dims = (((1,), (1,)), ((), ()))
    sums = lax.dot_general(pick, high, dims, preferred_element_type=F32)
    sums = sums + lax.dot_general(pick, rest, dims, preferred_element_type=F32)
    return sums[0:2, :]


def column_of(values, base, period):
    lane = lax.broadcasted_iota(jnp.int32, (24, 256), 1)
    row = lax.broadcasted_iota(jnp.int32, (24, 256), 0)
    return jnp.sum(
        jnp.where(lane == base + row % period, values, 0.0), axis=1, keepdims=True
    )


def kernel(
    tokens_hbm,
    norm_gain_hbm,
    mixer_gain_hbm,
    wq_hbm,
    wf_hbm,
    wi_hbm,
    wg_hbm,
    bound_hbm,
    head_gain_hbm,
    state_hbm,
    wout_hbm,
    wup_hbm,
    wdown_hbm,
    out_ref,
    next_v,
    tok_v,
    gain_v,
    w4_v,
    bound_v,
    head_gain_v,
    state_v,
    wout_v,
    wup_v,
    wdown_v,
    gains,
    w_first,
    w_up,
    w_down,
    w_out,
    tok_all,
    sq1,
    proj_out,
    proj_in,
    mix_own,
    mix_all,
    mixed_all,
    sq2,
    up_out,
    up_in,
    hidden_all,
    down_out,
    down_in,
    read_v,
    in_sems,
    send_sems,
    recv_sems,
    far_sem,
):
    kv, t = lax.axis_index("kv"), lax.axis_index("tp")
    z, x = kv // NX, kv % NX
    y, core = t // 2, t % 2
    rows_at = (t + NZ - z) % NZ
    has_self = t == (2 * z) % NZ

    def in_plane(i):
        px = (x + far_first(i // 8, 4)) % 4
        py = (y + far_first((i % 8) // 2, 4)) % 4
        pc = (core + 1 - i % 2) % 2
        return px, 2 * py + pc

    def in_column(i):
        pz = (z + far_first(i // 4, 8)) % 8
        px = (x + far_first(i % 4, 4)) % 4
        return pz, px

    def copy_to(src, dst, k, pkv, pt):
        return pltpu.make_async_remote_copy(
            src_ref=src,
            dst_ref=dst,
            send_sem=send_sems.at[k],
            recv_sem=recv_sems.at[k],
            device_id=(pkv, pt),
            device_id_type=MESH,
        )

    leaving, mix_sent = [], []

    def finish():
        for ref, k in leaving:
            wait_for(ref, send_sems.at[k])
        if mix_sent:
            @pl.when(has_self)
            def _():
                wait_for(mix_all.at[pl.ds(0, 31)], send_sems.at[8])

            @pl.when(jnp.logical_not(has_self))
            def _():
                wait_for(mix_all, send_sems.at[8])

    barrier = pltpu.get_barrier_semaphore()

    def tell(pkv, pt):
        pl.semaphore_signal(barrier, inc=1, device_id=(pkv, pt), device_id_type=MESH)

    def greet_plane(i, c):
        px, pt = in_plane(i)
        tell(z * NX + px, pt)
        return c

    def greet_near(i, c):
        pz = (z + (i // 8 + 1) * (1 - 2 * ((i // 4) % 2)) + NZ) % NZ
        tell(pz * NX + (x + i) % NX, t)
        return c

    lax.fori_loop(0, 31, greet_plane, 0)
    lax.fori_loop(0, 16, greet_near, 0)

    loads = [
        pltpu.make_async_copy(tokens_hbm, tok_v, in_sems.at[0]),
        pltpu.make_async_copy(norm_gain_hbm, gain_v.at[0], in_sems.at[1]),
        pltpu.make_async_copy(wq_hbm, w4_v.at[0], in_sems.at[2]),
        pltpu.make_async_copy(wf_hbm, w4_v.at[1], in_sems.at[3]),
        pltpu.make_async_copy(wi_hbm, w4_v.at[2], in_sems.at[4]),
        pltpu.make_async_copy(wg_hbm, w4_v.at[3], in_sems.at[5]),
        pltpu.make_async_copy(wout_hbm, wout_v, in_sems.at[6]),
        pltpu.make_async_copy(wup_hbm, wup_v, in_sems.at[7]),
        pltpu.make_async_copy(wdown_hbm, wdown_v, in_sems.at[8]),
        pltpu.make_async_copy(bound_hbm, bound_v, in_sems.at[9]),
        pltpu.make_async_copy(head_gain_hbm, head_gain_v, in_sems.at[10]),
        pltpu.make_async_copy(state_hbm, state_v, in_sems.at[11]),
        pltpu.make_async_copy(mixer_gain_hbm, gain_v.at[1], in_sems.at[12]),
    ]
    for load in loads:
        load.start()

    loads[0].wait()
    tok_f = tok_v[...].astype(F32)
    tok_all[x * NT + t] = jnp.concatenate([tok_f[0:24], tok_f[24:48]], axis=1).astype(BF16)
    loads[1].wait()
    loads[12].wait()
    for q in range(2):
        g = gain_v[q]
        gains[x, q : q + 1, :] = jnp.concatenate([g, g], axis=1)
    for k in range(2, 9):
        loads[k].wait()
    w_first[x] = w4_v[x]
    w_up[x] = wup_v[:, pl.ds(pl.multiple_of(x * 256, 256), 256)]
    w_out[t] = wout_v[...]
    w_down[x] = wdown_v[:, pl.ds(pl.multiple_of(x * 256, 256), 256)]

    pl.semaphore_wait(barrier, 31 + 16)
    for step in (2, 6):
        pl.semaphore_signal(
            far_sem, inc=1, device_id=((z + step) % NZ * NX + x, t), device_id_type=MESH
        )

    def send_tokens(i, c):
        px, pt = in_plane(i)
        copy_to(tok_all.at[x * NT + t], tok_all.at[x * NT + t], 0, z * NX + px, pt).start()
        return c

    def send_first(i, c):
        px = (x + far_first(i, 4)) % 4
        copy_to(gains.at[x], gains.at[x], 1, z * NX + px, t).start()
        copy_to(w4_v.at[px], w_first.at[x], 2, z * NX + px, t).start()
        return c

    lax.fori_loop(0, 3, send_first, 0)
    lax.fori_loop(0, 31, send_tokens, 0)

    leaving.append((tok_all.at[pl.ds(0, 31)], 0))
    leaving.append((gains.at[pl.ds(0, 3)], 1))
    leaving.append((w_first.at[pl.ds(0, 3)], 2))
    wait_for(gains.at[pl.ds(0, 3)], recv_sems.at[1])
    wait_for(tok_all.at[pl.ds(0, 31)], recv_sems.at[0])

    def send_wout(i, c):
        py = (y + far_first(i // 2, 4)) % 4
        pt = 2 * py + (core + 1 - i % 2) % 2
        copy_to(w_out.at[t], w_out.at[t], 3, kv, pt).start()
        return c

    lax.fori_loop(0, 7, send_wout, 0)
    leaving.append((w_out.at[pl.ds(0, 7)], 3))

    raw = [
        tok_all[pl.ds(NT * q, NT)].astype(F32).reshape(192, 128) for q in range(NX)
    ]
    sq1[z] = row_squares(raw)
    lhs = unpacked([raw[q] * gains[q, 0:1, :] for q in range(NX)])
    wait_for(w_first.at[pl.ds(0, 3)], recv_sems.at[2])
    partial = jnp.dot(lhs, w_first[...].reshape(256, 256), preferred_element_type=F32)

    for half in range(2):
        for pz in range(NZ):
            at = half * 192 + pz * 24
            left = partial[at : at + 24, 0:128]
            right = partial[at : at + 24, 128:256]
            proj_out[pz * NX + 2 * half] = jnp.concatenate(
                [left[0:12], right[0:12]], axis=0
            ).astype(BF16)
            proj_out[pz * NX + 2 * half + 1] = jnp.concatenate(
                [left[12:24], right[12:24]], axis=0
            ).astype(BF16)

    pl.semaphore_wait(far_sem, 2)

    def send_sq1(i, c):
        pz = (z + far_first(i, 8)) % 8
        copy_to(sq1.at[z], sq1.at[z], 4, pz * NX + x, t).start()
        return c

    def send_proj(i, c):
        pz, px = in_column(i)
        copy_to(proj_out.at[pz * NX + px], proj_in.at[kv], 5, pz * NX + px, t).start()
        return c

    lax.fori_loop(0, 7, send_sq1, 0)
    lax.fori_loop(0, 31, send_proj, 0)
    proj_in[kv] = proj_out[kv]
    leaving.append((sq1.at[pl.ds(0, 7)], 4))
    leaving.append((proj_in.at[pl.ds(0, 31)], 5))

    def send_ffn(i, c):
        px = (x + far_first(i, 4)) % 4
        cols = pl.ds(pl.multiple_of(px * 256, 256), 256)
        copy_to(wup_v.at[:, cols], w_up.at[x], 6, z * NX + px, t).start()
        copy_to(wdown_v.at[:, cols], w_down.at[x], 7, z * NX + px, t).start()
        return c

    lax.fori_loop(0, 3, send_ffn, 0)
    leaving.append((w_up.at[pl.ds(0, 3)], 6))
    leaving.append((w_down.at[pl.ds(0, 3)], 7))

    for k in range(9, 12):
        loads[k].wait()
    wait_for(sq1.at[pl.ds(0, 7)], recv_sems.at[4])
    wait_for(proj_in.at[pl.ds(0, 31)], recv_sems.at[5])

    squares = sq1[0]
    for q in range(1, NZ):
        squares = squares + sq1[q]
    square_row = jnp.where(x // 2 == 0, squares[0:1, :], squares[1:2, :])
    row_scale = lax.rsqrt(
        column_of(square_row, z * 24 + (x % 2) * 12, 12) / WIDTH + NORM_EPS
    )
    owned = []
    for q in range(NX):
        total = proj_in[q].astype(F32)
        for r in range(1, NZ):
            total = total + proj_in[r * NX + q].astype(F32)
        owned.append(total * row_scale)
    queries, forget_raw, values_in, gate_raw = owned
    head0 = lax.broadcasted_iota(jnp.int32, (24, 128), 0) < 12
    bound = jnp.where(head0, bound_v[0:1, :], bound_v[1:2, :])
    head_gain = jnp.where(head0, head_gain_v[0:1, :], head_gain_v[1:2, :])
    forget = bound + (1.0 - bound) * jax.nn.sigmoid(forget_raw)
    pad = jnp.zeros((104, 128), F32)
    forget_t = jnp.concatenate([forget, pad], axis=0).T
    queries_t = jnp.concatenate([queries, pad], axis=0).T
    for j in range(24):
        h, s = j // 12, j % 12
        f = forget_t[:, j : j + 1]
        nxt = f * state_v[s, h] + (1.0 - f) * values_in[j : j + 1, :]
        next_v[s, h] = nxt
        read_v[j : j + 1, :] = jnp.sum(queries_t[:, j : j + 1] * nxt, axis=0, keepdims=True)
    read = read_v[...]
    read = read * lax.rsqrt(jnp.mean(read * read, axis=1, keepdims=True) + NORM_EPS) * head_gain
    mix_own[...] = (read * jax.nn.silu(gate_raw)).astype(BF16)

    def send_mix(i, c):
        pz, px = (z + far_first(i // 4, 8)) % 8, (x + far_first(i % 4, 4)) % 4
        pt = (z + pz) % NZ
        away = jnp.logical_or(pz * NX + px != kv, pt != t)

        @pl.when(away)
        def _():
            copy_to(mix_own, mix_all.at[t * NX + x], 8, pz * NX + px, pt).start()

        return c

    lax.fori_loop(0, 32, send_mix, 0)

    @pl.when(has_self)
    def _():
        mix_all[t * NX + x] = mix_own[...]

    mix_sent.append(1)
    wait_for(w_out.at[pl.ds(0, 7)], recv_sems.at[3])

    @pl.when(has_self)
    def _():
        wait_for(mix_all.at[pl.ds(0, 31)], recv_sems.at[8])

    @pl.when(jnp.logical_not(has_self))
    def _():
        wait_for(mix_all, recv_sems.at[8])

    acc = jnp.zeros((96, 128), F32)
    for q in range(NT):
        both = jnp.concatenate([w_out[q, :, 0:128], w_out[q, :, 128:256]], axis=0)
        acc = acc + dot_t(mix_all[4 * q : 4 * q + 4].reshape(96, 128), both)
    folded = []
    for q in range(NX):
        part = acc[24 * q : 24 * q + 24]
        turned = swap_lanes(jnp.concatenate([part[12:24], part[0:12]], axis=0))
        folded.append(part + turned)
    low = low_lanes((24, 128))
    top = jnp.where(low, folded[0], swap_lanes(folded[2]))
    bottom = jnp.where(low, swap_lanes(folded[1]), folded[3])
    attn = jnp.where(head0, top, bottom)
    own_at = x * NT + rows_at
    mixed_all[own_at] = (tok_all[own_at].astype(F32) + attn).astype(BF16)

    def send_mixed(i, c):
        px, pt = in_plane(i)
        copy_to(mixed_all.at[own_at], mixed_all.at[own_at], 9, z * NX + px, pt).start()
        return c

    lax.fori_loop(0, 31, send_mixed, 0)
    leaving.append((mixed_all.at[pl.ds(0, 31)], 9))
    wait_for(w_up.at[pl.ds(0, 3)], recv_sems.at[6])
    wait_for(mixed_all.at[pl.ds(0, 31)], recv_sems.at[9])

    raw2 = [
        mixed_all[pl.ds(NT * q, NT)].astype(F32).reshape(192, 128) for q in range(NX)
    ]
    sq2[z] = row_squares(raw2)
    lhs2 = unpacked([raw2[q] * gains[q, 1:2, :] for q in range(NX)])
    partial2 = jnp.dot(lhs2, w_up[...].reshape(256, 256), preferred_element_type=F32)
    for half in range(2):
        for pz in range(NZ):
            at = half * 192 + pz * 24
            up_out[pz, half] = partial2[at : at + 24].astype(BF16)

    def send_up(i, c):
        pz = (z + far_first(i, 8)) % 8
        copy_to(sq2.at[z], sq2.at[z], 10, pz * NX + x, t).start()
        copy_to(up_out.at[pz], up_in.at[z], 11, pz * NX + x, t).start()
        return c

    lax.fori_loop(0, 7, send_up, 0)
    up_in[z] = up_out[z]
    leaving.append((sq2.at[pl.ds(0, 7)], 10))
    leaving.append((up_in.at[pl.ds(0, 7)], 11))
    wait_for(sq2.at[pl.ds(0, 7)], recv_sems.at[10])
    squares2 = sq2[0]
    for q in range(1, NZ):
        squares2 = squares2 + sq2[q]
    scales = [
        lax.rsqrt(column_of(squares2[q : q + 1, :], z * 24, 24) / WIDTH + NORM_EPS)
        for q in range(2)
    ]
    wait_for(up_in.at[pl.ds(0, 7)], recv_sems.at[11])

    for half in range(2):
        total = up_in[0, half].astype(F32)
        for q in range(1, NZ):
            total = total + up_in[q, half].astype(F32)
        total = jnp.maximum(total * scales[half], 0.0)
        hidden_all[z, half] = (total * total).astype(BF16)

    def send_hidden(i, c):
        pz = (z + far_first(i, 8)) % 8
        copy_to(hidden_all.at[z], hidden_all.at[z], 12, pz * NX + x, t).start()
        return c

    lax.fori_loop(0, 7, send_hidden, 0)
    leaving.append((hidden_all.at[pl.ds(0, 7)], 12))
    wait_for(w_down.at[pl.ds(0, 3)], recv_sems.at[7])
    wait_for(hidden_all.at[pl.ds(0, 7)], recv_sems.at[12])

    partial3 = dot_t(hidden_all[...].reshape(384, 256), w_down[...].reshape(256, 256))
    for pt in range(NT):
        for pair in range(2):
            upper = partial3[48 * pt : 48 * pt + 24, 128 * pair : 128 * pair + 128]
            lower = partial3[48 * pt + 24 : 48 * pt + 48, 128 * pair : 128 * pair + 128]
            down_out[pt * NX + 2 * pair] = jnp.where(low, upper, swap_lanes(lower)).astype(BF16)
            down_out[pt * NX + 2 * pair + 1] = jnp.where(low, swap_lanes(upper), lower).astype(
                BF16
            )

    def send_down(i, c):
        px, pt = in_plane(i)
        copy_to(
            down_out.at[pt * NX + px], down_in.at[t * NX + x], 13, z * NX + px, pt
        ).start()
        return c

    lax.fori_loop(0, 31, send_down, 0)
    down_in[t * NX + x] = down_out[t * NX + x]
    leaving.append((down_in.at[pl.ds(0, 31)], 13))
    wait_for(down_in.at[pl.ds(0, 31)], recv_sems.at[13])
    total = down_in[0].astype(F32)
    for q in range(1, 32):
        total = total + down_in[q].astype(F32)
    total = mixed_all[x * NT + t].astype(F32) + total
    out_ref[...] = jnp.concatenate([total[:, 0:64], total[:, 64:128]], axis=0).astype(BF16)

    finish()


def body(
    tokens,
    norm_gain,
    w_query,
    w_forget,
    w_input,
    w_gate,
    lower_bound,
    head_gain,
    recur_state,
    w_out,
    mixer_gain,
    w_up,
    w_down,
):
    bound = lower_bound.reshape(2, 128)
    any_spec = pl.BlockSpec(memory_space=pltpu.HBM)
    vmem_spec = pl.BlockSpec(memory_space=pltpu.VMEM)
    return pl.pallas_call(
        kernel,
        out_shape=(
            jax.ShapeDtypeStruct(tokens.shape, tokens.dtype),
            jax.ShapeDtypeStruct(recur_state.shape, recur_state.dtype),
        ),
        in_specs=[any_spec] * 13,
        out_specs=(vmem_spec, vmem_spec),
        scratch_shapes=[
            pltpu.VMEM((48, 64), BF16),
            pltpu.VMEM((2, 1, 64), F32),
            pltpu.VMEM((4, 64, 256), BF16),
            pltpu.VMEM((2, 128), F32),
            pltpu.VMEM((2, 128), F32),
            pltpu.VMEM((12, 2, 128, 128), F32),
            pltpu.VMEM((64, 256), BF16),
            pltpu.VMEM((64, 1024), BF16),
            pltpu.VMEM((64, 1024), BF16),
            pltpu.VMEM((4, 2, 128), F32),
            pltpu.VMEM((4, 64, 256), BF16),
            pltpu.VMEM((4, 64, 256), BF16),
            pltpu.VMEM((4, 64, 256), BF16),
            pltpu.VMEM((8, 64, 256), BF16),
            pltpu.VMEM((32, 24, 128), BF16),
            pltpu.VMEM((8, 2, 256), F32),
            pltpu.VMEM((32, 24, 128), BF16),
            pltpu.VMEM((32, 24, 128), BF16),
            pltpu.VMEM((24, 128), BF16),
            pltpu.VMEM((32, 24, 128), BF16),
            pltpu.VMEM((32, 24, 128), BF16),
            pltpu.VMEM((8, 2, 256), F32),
            pltpu.VMEM((8, 2, 24, 256), BF16),
            pltpu.VMEM((8, 2, 24, 256), BF16),
            pltpu.VMEM((8, 2, 24, 256), BF16),
            pltpu.VMEM((32, 24, 128), BF16),
            pltpu.VMEM((32, 24, 128), BF16),
            pltpu.VMEM((24, 128), F32),
            pltpu.SemaphoreType.DMA((13,)),
            pltpu.SemaphoreType.DMA((14,)),
            pltpu.SemaphoreType.DMA((14,)),
            pltpu.SemaphoreType.REGULAR,
        ],
        compiler_params=pltpu.CompilerParams(collective_id=0, has_side_effects=True, vmem_limit_bytes=16 * 1024 * 1024),
        name="decode_layer",
    )(*(pltpu.with_memory_space_constraint(a, pltpu.HBM) for a in (
        tokens,
        norm_gain.reshape(1, 64),
        mixer_gain.reshape(1, 64),
        w_query,
        w_forget,
        w_input,
        w_gate,
        bound,
        head_gain,
        recur_state,
        w_out.T,
        w_up,
        w_down.T,
    )))


def solution(mesh):
    in_specs = (
        P("tp", "kv"),
        P("kv"),
        P("kv", "tp"),
        P("kv", "tp"),
        P("kv", "tp"),
        P("kv", "tp"),
        P("tp"),
        P("tp", None),
        P("kv", "tp", None, None),
        P("tp", "kv"),
        P("kv"),
        P("kv", "tp"),
        P("tp", "kv"),
    )
    out_specs = (P("tp", "kv"), P("kv", "tp", None, None))
    return jax.shard_map(body, mesh=mesh, in_specs=in_specs, out_specs=out_specs, check_vma=False)
```

```python
import itertools

import jax
import jax.numpy as jnp
from jax import lax
from jax.experimental import pallas as pl
from jax.experimental.pallas import tpu as pltpu
from jax.sharding import PartitionSpec as P

NORM_EPS = 1e-05
MESH = pl.DeviceIdType.MESH
F32 = jnp.float32
BF16 = jnp.bfloat16

NZ, NX, NT = 8, 4, 8
WIDTH = 2048.0


def hops(step, size):
    return min(step, size - step)


def by_distance(sizes):
    steps = list(itertools.product(*(range(n) for n in sizes)))[1:]
    return sorted(steps, key=lambda d: (-sum(hops(s, n) for s, n in zip(d, sizes)), d))


PLANE = by_distance((4, 4, 2))
COLUMN = by_distance((8, 4))
ALONG_X = by_distance((4,))
ALONG_Y = by_distance((4, 2))
ALONG_Z = by_distance((8,))


def wait_for(ref, sem):
    pltpu.make_async_copy(ref, ref, sem).wait()


def swap_lanes(value):
    return pltpu.roll(value, 64, 1)


def dot_t(a, b):
    return lax.dot_general(a, b, (((1,), (1,)), ((), ())), preferred_element_type=F32)


def low_lanes(shape):
    return lax.broadcasted_iota(jnp.int32, shape, 1) < 64


def unpacked(pieces):
    low = low_lanes(pieces[0].shape)
    swapped = [swap_lanes(p) for p in pieces]
    first = [jnp.where(low, pieces[i], swapped[i + 1]).astype(BF16) for i in (0, 2)]
    second = [jnp.where(low, swapped[i], pieces[i + 1]).astype(BF16) for i in (0, 2)]
    return jnp.concatenate(
        [jnp.concatenate(first, axis=1), jnp.concatenate(second, axis=1)], axis=0
    )


def row_squares(pieces):
    total = pieces[0] * pieces[0]
    for p in pieces[1:]:
        total = total + p * p
    total = jnp.concatenate([total, jnp.zeros((64, 128), F32)], axis=0)
    high = total.astype(BF16)
    rest = (total - high.astype(F32)).astype(BF16)
    lane = lax.broadcasted_iota(jnp.int32, (8, 128), 1)
    row = lax.broadcasted_iota(jnp.int32, (8, 128), 0)
    pick = jnp.where((lane // 64) == row, 1.0, 0.0).astype(BF16)
    dims = (((1,), (1,)), ((), ()))
    sums = lax.dot_general(pick, high, dims, preferred_element_type=F32)
    sums = sums + lax.dot_general(pick, rest, dims, preferred_element_type=F32)
    return sums[0:2, :]


def column_of(values, base, period):
    lane = lax.broadcasted_iota(jnp.int32, (24, 256), 1)
    row = lax.broadcasted_iota(jnp.int32, (24, 256), 0)
    return jnp.sum(
        jnp.where(lane == base + row % period, values, 0.0), axis=1, keepdims=True
    )


def kernel(
    tokens_hbm,
    norm_gain_hbm,
    mixer_gain_hbm,
    wq_hbm,
    wf_hbm,
    wi_hbm,
    wg_hbm,
    bound_hbm,
    head_gain_hbm,
    state_hbm,
    wout_hbm,
    wup_hbm,
    wdown_hbm,
    out_ref,
    next_v,
    tok_v,
    gain_v,
    w4_v,
    bound_v,
    head_gain_v,
    state_v,
    wout_v,
    wup_v,
    wdown_v,
    gains,
    w_first,
    w_up,
    w_down,
    w_out,
    tok_all,
    sq1,
    proj_out,
    proj_in,
    mix_own,
    mix_all,
    mixed_all,
    sq2,
    up_out,
    up_in,
    hidden_all,
    down_out,
    down_in,
    read_v,
    in_sems,
    send_sems,
    recv_sems,
    far_sem,
):
    kv, t = lax.axis_index("kv"), lax.axis_index("tp")
    z, x = kv // NX, kv % NX
    y, core = t // 2, t % 2
    rows_at = (t + NZ - z) % NZ
    has_self = t == (2 * z) % NZ

    xs = [(x + d) % 4 for d in range(4)]
    ys = [(y + d) % 4 for d in range(4)]
    zs = [(z + d) % 8 for d in range(8)]
    cores = [core, 1 - core]
    kvs = [[pz * NX + px for px in xs] for pz in zs]
    ts = [[2 * py + pc for pc in cores] for py in ys]

    def copy_to(src, dst, k, pkv, pt):
        return pltpu.make_async_remote_copy(
            src_ref=src,
            dst_ref=dst,
            send_sem=send_sems.at[k],
            recv_sem=recv_sems.at[k],
            device_id=(pkv, pt),
            device_id_type=MESH,
        )

    leaving, mix_sent = [], []

    def finish():
        for ref, k in leaving:
            wait_for(ref, send_sems.at[k])
        if mix_sent:
            @pl.when(has_self)
            def _():
                wait_for(mix_all.at[pl.ds(0, 31)], send_sems.at[8])

            @pl.when(jnp.logical_not(has_self))
            def _():
                wait_for(mix_all, send_sems.at[8])

    barrier = pltpu.get_barrier_semaphore()

    def tell(pkv, pt):
        pl.semaphore_signal(barrier, inc=1, device_id=(pkv, pt), device_id_type=MESH)

    for dx, dy, dc in PLANE:
        tell(kvs[0][dx], ts[dy][dc])
    for dz in (2, 6, 1, 7):
        for dx in (2, 1, 3, 0):
            tell(kvs[dz][dx], t)

    loads = [
        pltpu.make_async_copy(tokens_hbm, tok_v, in_sems.at[0]),
        pltpu.make_async_copy(norm_gain_hbm, gain_v.at[0], in_sems.at[1]),
        pltpu.make_async_copy(wq_hbm, w4_v.at[0], in_sems.at[2]),
        pltpu.make_async_copy(wf_hbm, w4_v.at[1], in_sems.at[3]),
        pltpu.make_async_copy(wi_hbm, w4_v.at[2], in_sems.at[4]),
        pltpu.make_async_copy(wg_hbm, w4_v.at[3], in_sems.at[5]),
        pltpu.make_async_copy(wout_hbm, wout_v, in_sems.at[6]),
        pltpu.make_async_copy(wup_hbm, wup_v, in_sems.at[7]),
        pltpu.make_async_copy(wdown_hbm, wdown_v, in_sems.at[8]),
        pltpu.make_async_copy(bound_hbm, bound_v, in_sems.at[9]),
        pltpu.make_async_copy(head_gain_hbm, head_gain_v, in_sems.at[10]),
        pltpu.make_async_copy(state_hbm, state_v, in_sems.at[11]),
        pltpu.make_async_copy(mixer_gain_hbm, gain_v.at[1], in_sems.at[12]),
    ]
    for load in loads:
        load.start()

    loads[0].wait()
    tok_f = tok_v[...].astype(F32)
    tok_all[x * NT + t] = jnp.concatenate([tok_f[0:24], tok_f[24:48]], axis=1).astype(BF16)
    loads[1].wait()
    loads[12].wait()
    for q in range(2):
        g = gain_v[q]
        gains[x, q : q + 1, :] = jnp.concatenate([g, g], axis=1)
    for k in range(2, 9):
        loads[k].wait()
    w_first[x] = w4_v[x]
    w_up[x] = wup_v[:, pl.ds(pl.multiple_of(x * 256, 256), 256)]
    w_out[t] = wout_v[...]
    w_down[x] = wdown_v[:, pl.ds(pl.multiple_of(x * 256, 256), 256)]

    pl.semaphore_wait(barrier, 31 + 16)
    for step in (2, 6):
        pl.semaphore_signal(
            far_sem, inc=1, device_id=(kvs[step][0], t), device_id_type=MESH
        )

    for (dx,) in ALONG_X:
        copy_to(gains.at[x], gains.at[x], 1, kvs[0][dx], t).start()
        copy_to(w4_v.at[xs[dx]], w_first.at[x], 2, kvs[0][dx], t).start()
    own_tok = tok_all.at[x * NT + t]
    for dx, dy, dc in PLANE:
        copy_to(own_tok, own_tok, 0, kvs[0][dx], ts[dy][dc]).start()
    leaving.append((tok_all.at[pl.ds(0, 31)], 0))
    leaving.append((gains.at[pl.ds(0, 3)], 1))
    leaving.append((w_first.at[pl.ds(0, 3)], 2))
    wait_for(gains.at[pl.ds(0, 3)], recv_sems.at[1])
    wait_for(tok_all.at[pl.ds(0, 31)], recv_sems.at[0])

    for dy, dc in ALONG_Y:
        copy_to(w_out.at[t], w_out.at[t], 3, kv, ts[dy][dc]).start()
    leaving.append((w_out.at[pl.ds(0, 7)], 3))

    raw = [
        tok_all[pl.ds(NT * q, NT)].astype(F32).reshape(192, 128) for q in range(NX)
    ]
    sq1[z] = row_squares(raw)
    lhs = unpacked([raw[q] * gains[q, 0:1, :] for q in range(NX)])
    wait_for(w_first.at[pl.ds(0, 3)], recv_sems.at[2])
    partial = jnp.dot(lhs, w_first[...].reshape(256, 256), preferred_element_type=F32)

    for half in range(2):
        for pz in range(NZ):
            at = half * 192 + pz * 24
            left = partial[at : at + 24, 0:128]
            right = partial[at : at + 24, 128:256]
            proj_out[pz * NX + 2 * half] = jnp.concatenate(
                [left[0:12], right[0:12]], axis=0
            ).astype(BF16)
            proj_out[pz * NX + 2 * half + 1] = jnp.concatenate(
                [left[12:24], right[12:24]], axis=0
            ).astype(BF16)

    pl.semaphore_wait(far_sem, 2)

    for (dz,) in ALONG_Z:
        copy_to(sq1.at[z], sq1.at[z], 4, kvs[dz][0], t).start()
    for dz, dx in COLUMN:
        copy_to(proj_out.at[kvs[dz][dx]], proj_in.at[kv], 5, kvs[dz][dx], t).start()
    proj_in[kv] = proj_out[kv]
    leaving.append((sq1.at[pl.ds(0, 7)], 4))
    leaving.append((proj_in.at[pl.ds(0, 31)], 5))

    for (dx,) in ALONG_X:
        cols = pl.ds(pl.multiple_of(xs[dx] * 256, 256), 256)
        copy_to(wup_v.at[:, cols], w_up.at[x], 6, kvs[0][dx], t).start()
        copy_to(wdown_v.at[:, cols], w_down.at[x], 7, kvs[0][dx], t).start()
    leaving.append((w_up.at[pl.ds(0, 3)], 6))
    leaving.append((w_down.at[pl.ds(0, 3)], 7))

    for k in range(9, 12):
        loads[k].wait()
    wait_for(sq1.at[pl.ds(0, 7)], recv_sems.at[4])
    wait_for(proj_in.at[pl.ds(0, 31)], recv_sems.at[5])

    squares = sq1[0]
    for q in range(1, NZ):
        squares = squares + sq1[q]
    square_row = jnp.where(x // 2 == 0, squares[0:1, :], squares[1:2, :])
    row_scale = lax.rsqrt(
        column_of(square_row, z * 24 + (x % 2) * 12, 12) / WIDTH + NORM_EPS
    )
    owned = []
    for q in range(NX):
        total = proj_in[q].astype(F32)
        for r in range(1, NZ):
            total = total + proj_in[r * NX + q].astype(F32)
        owned.append(total * row_scale)
    queries, forget_raw, values_in, gate_raw = owned
    head0 = lax.broadcasted_iota(jnp.int32, (24, 128), 0) < 12
    bound = jnp.where(head0, bound_v[0:1, :], bound_v[1:2, :])
    head_gain = jnp.where(head0, head_gain_v[0:1, :], head_gain_v[1:2, :])
    forget = bound + (1.0 - bound) * jax.nn.sigmoid(forget_raw)
    pad = jnp.zeros((104, 128), F32)
    kept = queries * forget
    kept_t = jnp.concatenate([kept, pad], axis=0).T
    fresh = jnp.sum(queries * (1.0 - forget), axis=1, keepdims=True) * values_in
    for j in range(24):
        read_v[j : j + 1, :] = jnp.sum(
            kept_t[:, j : j + 1] * state_v[j % 12, j // 12], axis=0, keepdims=True
        )
    read = read_v[...] + fresh
    read = read * lax.rsqrt(jnp.mean(read * read, axis=1, keepdims=True) + NORM_EPS) * head_gain
    mix_own[...] = (read * jax.nn.silu(gate_raw)).astype(BF16)

    mix_at = t * NX + x
    for dz, dx in COLUMN:
        copy_to(mix_own, mix_all.at[mix_at], 8, kvs[dz][dx], (z + zs[dz]) % NZ).start()

    @pl.when(jnp.logical_not(has_self))
    def _():
        copy_to(mix_own, mix_all.at[mix_at], 8, kv, (2 * z) % NZ).start()

    @pl.when(has_self)
    def _():
        mix_all[mix_at] = mix_own[...]

    mix_sent.append(1)
    forget_t = jnp.concatenate([forget, pad], axis=0).T
    for j in range(24):
        f = forget_t[:, j : j + 1]
        next_v[j % 12, j // 12] = f * state_v[j % 12, j // 12] + (1.0 - f) * values_in[j : j + 1, :]
    wait_for(w_out.at[pl.ds(0, 7)], recv_sems.at[3])

    @pl.when(has_self)
    def _():
        wait_for(mix_all.at[pl.ds(0, 31)], recv_sems.at[8])

    @pl.when(jnp.logical_not(has_self))
    def _():
        wait_for(mix_all, recv_sems.at[8])

    acc = jnp.zeros((96, 128), F32)
    for q in range(NT):
        both = jnp.concatenate([w_out[q, :, 0:128], w_out[q, :, 128:256]], axis=0)
        acc = acc + dot_t(mix_all[4 * q : 4 * q + 4].reshape(96, 128), both)
    folded = []
    for q in range(NX):
        part = acc[24 * q : 24 * q + 24]
        turned = swap_lanes(jnp.concatenate([part[12:24], part[0:12]], axis=0))
        folded.append(part + turned)
    low = low_lanes((24, 128))
    top = jnp.where(low, folded[0], swap_lanes(folded[2]))
    bottom = jnp.where(low, swap_lanes(folded[1]), folded[3])
    attn = jnp.where(head0, top, bottom)
    own_at = x * NT + rows_at
    mixed_all[own_at] = (tok_all[own_at].astype(F32) + attn).astype(BF16)

    for dx, dy, dc in PLANE:
        copy_to(mixed_all.at[own_at], mixed_all.at[own_at], 9, kvs[0][dx], ts[dy][dc]).start()
    leaving.append((mixed_all.at[pl.ds(0, 31)], 9))
    wait_for(w_up.at[pl.ds(0, 3)], recv_sems.at[6])
    wait_for(mixed_all.at[pl.ds(0, 31)], recv_sems.at[9])

    raw2 = [
        mixed_all[pl.ds(NT * q, NT)].astype(F32).reshape(192, 128) for q in range(NX)
    ]
    sq2[z] = row_squares(raw2)
    lhs2 = unpacked([raw2[q] * gains[q, 1:2, :] for q in range(NX)])
    partial2 = jnp.dot(lhs2, w_up[...].reshape(256, 256), preferred_element_type=F32)
    for half in range(2):
        for pz in range(NZ):
            at = half * 192 + pz * 24
            up_out[pz, half] = partial2[at : at + 24].astype(BF16)

    for (dz,) in ALONG_Z:
        copy_to(sq2.at[z], sq2.at[z], 10, kvs[dz][0], t).start()
        copy_to(up_out.at[zs[dz]], up_in.at[z], 11, kvs[dz][0], t).start()
    up_in[z] = up_out[z]
    leaving.append((sq2.at[pl.ds(0, 7)], 10))
    leaving.append((up_in.at[pl.ds(0, 7)], 11))
    wait_for(sq2.at[pl.ds(0, 7)], recv_sems.at[10])
    squares2 = sq2[0]
    for q in range(1, NZ):
        squares2 = squares2 + sq2[q]
    scales = [
        lax.rsqrt(column_of(squares2[q : q + 1, :], z * 24, 24) / WIDTH + NORM_EPS)
        for q in range(2)
    ]
    wait_for(up_in.at[pl.ds(0, 7)], recv_sems.at[11])

    for half in range(2):
        total = up_in[0, half].astype(F32)
        for q in range(1, NZ):
            total = total + up_in[q, half].astype(F32)
        total = jnp.maximum(total * scales[half], 0.0)
        hidden_all[z, half] = (total * total).astype(BF16)

    for (dz,) in ALONG_Z:
        copy_to(hidden_all.at[z], hidden_all.at[z], 12, kvs[dz][0], t).start()
    leaving.append((hidden_all.at[pl.ds(0, 7)], 12))
    wait_for(w_down.at[pl.ds(0, 3)], recv_sems.at[7])
    wait_for(hidden_all.at[pl.ds(0, 7)], recv_sems.at[12])

    partial3 = dot_t(hidden_all[...].reshape(384, 256), w_down[...].reshape(256, 256))
    for pt in range(NT):
        for pair in range(2):
            upper = partial3[48 * pt : 48 * pt + 24, 128 * pair : 128 * pair + 128]
            lower = partial3[48 * pt + 24 : 48 * pt + 48, 128 * pair : 128 * pair + 128]
            down_out[pt * NX + 2 * pair] = jnp.where(low, upper, swap_lanes(lower)).astype(BF16)
            down_out[pt * NX + 2 * pair + 1] = jnp.where(low, swap_lanes(upper), lower).astype(
                BF16
            )

    for dx, dy, dc in PLANE:
        copy_to(
            down_out.at[ts[dy][dc] * NX + xs[dx]],
            down_in.at[t * NX + x],
            13,
            kvs[0][dx],
            ts[dy][dc],
        ).start()
    down_in[t * NX + x] = down_out[t * NX + x]
    leaving.append((down_in.at[pl.ds(0, 31)], 13))
    wait_for(down_in.at[pl.ds(0, 31)], recv_sems.at[13])
    total = down_in[0].astype(F32)
    for q in range(1, 32):
        total = total + down_in[q].astype(F32)
    total = mixed_all[x * NT + t].astype(F32) + total
    out_ref[...] = jnp.concatenate([total[:, 0:64], total[:, 64:128]], axis=0).astype(BF16)

    finish()


def body(
    tokens,
    norm_gain,
    w_query,
    w_forget,
    w_input,
    w_gate,
    lower_bound,
    head_gain,
    recur_state,
    w_out,
    mixer_gain,
    w_up,
    w_down,
):
    bound = lower_bound.reshape(2, 128)
    any_spec = pl.BlockSpec(memory_space=pltpu.HBM)
    vmem_spec = pl.BlockSpec(memory_space=pltpu.VMEM)
    return pl.pallas_call(
        kernel,
        out_shape=(
            jax.ShapeDtypeStruct(tokens.shape, tokens.dtype),
            jax.ShapeDtypeStruct(recur_state.shape, recur_state.dtype),
        ),
        in_specs=[any_spec] * 13,
        out_specs=(vmem_spec, vmem_spec),
        scratch_shapes=[
            pltpu.VMEM((48, 64), BF16),
            pltpu.VMEM((2, 1, 64), F32),
            pltpu.VMEM((4, 64, 256), BF16),
            pltpu.VMEM((2, 128), F32),
            pltpu.VMEM((2, 128), F32),
            pltpu.VMEM((12, 2, 128, 128), F32),
            pltpu.VMEM((64, 256), BF16),
            pltpu.VMEM((64, 1024), BF16),
            pltpu.VMEM((64, 1024), BF16),
            pltpu.VMEM((4, 2, 128), F32),
            pltpu.VMEM((4, 64, 256), BF16),
            pltpu.VMEM((4, 64, 256), BF16),
            pltpu.VMEM((4, 64, 256), BF16),
            pltpu.VMEM((8, 64, 256), BF16),
            pltpu.VMEM((32, 24, 128), BF16),
            pltpu.VMEM((8, 2, 256), F32),
            pltpu.VMEM((32, 24, 128), BF16),
            pltpu.VMEM((32, 24, 128), BF16),
            pltpu.VMEM((24, 128), BF16),
            pltpu.VMEM((32, 24, 128), BF16),
            pltpu.VMEM((32, 24, 128), BF16),
            pltpu.VMEM((8, 2, 256), F32),
            pltpu.VMEM((8, 2, 24, 256), BF16),
            pltpu.VMEM((8, 2, 24, 256), BF16),
            pltpu.VMEM((8, 2, 24, 256), BF16),
            pltpu.VMEM((32, 24, 128), BF16),
            pltpu.VMEM((32, 24, 128), BF16),
            pltpu.VMEM((24, 128), F32),
            pltpu.SemaphoreType.DMA((13,)),
            pltpu.SemaphoreType.DMA((14,)),
            pltpu.SemaphoreType.DMA((14,)),
            pltpu.SemaphoreType.REGULAR,
        ],
        compiler_params=pltpu.CompilerParams(collective_id=0, has_side_effects=True, vmem_limit_bytes=16 * 1024 * 1024),
        name="decode_layer",
    )(*(pltpu.with_memory_space_constraint(a, pltpu.HBM) for a in (
        tokens,
        norm_gain.reshape(1, 64),
        mixer_gain.reshape(1, 64),
        w_query,
        w_forget,
        w_input,
        w_gate,
        bound,
        head_gain,
        recur_state,
        w_out.T,
        w_up,
        w_down.T,
    )))


def solution(mesh):
    in_specs = (
        P("tp", "kv"),
        P("kv"),
        P("kv", "tp"),
        P("kv", "tp"),
        P("kv", "tp"),
        P("kv", "tp"),
        P("tp"),
        P("tp", None),
        P("kv", "tp", None, None),
        P("tp", "kv"),
        P("kv"),
        P("kv", "tp"),
        P("tp", "kv"),
    )
    out_specs = (P("tp", "kv"), P("kv", "tp", None, None))
    return jax.shard_map(body, mesh=mesh, in_specs=in_specs, out_specs=out_specs, check_vma=False)
```

```python
import itertools

import jax
import jax.numpy as jnp
from jax import lax
from jax.experimental import pallas as pl
from jax.experimental.pallas import tpu as pltpu
from jax.sharding import PartitionSpec as P

NORM_EPS = 1e-05
MESH = pl.DeviceIdType.MESH
F32 = jnp.float32
BF16 = jnp.bfloat16

NZ, NX, NT = 8, 4, 8
WIDTH = 2048.0
FIRST_TOKENS = 16


def hops(step, size):
    return min(step, size - step)


def by_distance(sizes):
    steps = list(itertools.product(*(range(n) for n in sizes)))[1:]
    return sorted(steps, key=lambda d: (-sum(hops(s, n) for s, n in zip(d, sizes)), d))


PLANE = by_distance((4, 4, 2))
COLUMN = by_distance((8, 4))
ALONG_X = by_distance((4,))
ALONG_Y = by_distance((4, 2))
ALONG_Z = by_distance((8,))
NEAR_Y = [(0, 0)] + ALONG_Y[::-1]
NEAR_Z = [0, 1, 7, 2, 6, 3, 5, 4]


def wait_for(ref, sem):
    pltpu.make_async_copy(ref, ref, sem).wait()


def swap_lanes(value):
    return pltpu.roll(value, 64, 1)


def dot_t(a, b):
    return lax.dot_general(a, b, (((1,), (1,)), ((), ())), preferred_element_type=F32)


def low_lanes(shape):
    return lax.broadcasted_iota(jnp.int32, shape, 1) < 64


def unpacked(pieces):
    low = low_lanes(pieces[0].shape)
    swapped = [swap_lanes(p) for p in pieces]
    first = [jnp.where(low, pieces[i], swapped[i + 1]) for i in (0, 2)]
    second = [jnp.where(low, swapped[i], pieces[i + 1]) for i in (0, 2)]
    return jnp.concatenate(
        [jnp.concatenate(first, axis=1), jnp.concatenate(second, axis=1)], axis=0
    ).astype(BF16)


def row_squares(pieces):
    total = pieces[0] * pieces[0]
    for p in pieces[1:]:
        total = total + p * p
    total = jnp.concatenate([total, jnp.zeros((104, 128), F32)], axis=0)
    high = total.astype(BF16)
    rest = (total - high.astype(F32)).astype(BF16)
    lane = lax.broadcasted_iota(jnp.int32, (8, 128), 1)
    row = lax.broadcasted_iota(jnp.int32, (8, 128), 0)
    pick = jnp.where((lane // 64) == row, 1.0, 0.0).astype(BF16)
    sums = dot_t(pick, high) + dot_t(pick, rest)
    return sums[0:2, :]


def column_of(values, base, period):
    lane = lax.broadcasted_iota(jnp.int32, (24, 128), 1)
    row = lax.broadcasted_iota(jnp.int32, (24, 128), 0)
    return jnp.sum(
        jnp.where(lane == base + row % period, values, 0.0), axis=1, keepdims=True
    )


def kernel(
    tokens_hbm,
    norm_gain_hbm,
    mixer_gain_hbm,
    wq_hbm,
    wf_hbm,
    wi_hbm,
    wg_hbm,
    bound_hbm,
    head_gain_hbm,
    state_hbm,
    wout_hbm,
    wup_hbm,
    wdown_hbm,
    out_ref,
    next_v,
    tok_v,
    gain_v,
    w4_v,
    bound_v,
    head_gain_v,
    state_v,
    wout_v,
    wup_v,
    wdown_v,
    gains,
    w_first,
    w_up,
    w_down,
    w_out,
    tok_all,
    sq_out,
    sq1,
    proj_out,
    proj_in,
    mix_own,
    mix_all,
    mixed_all,
    sq_out2,
    sq2,
    up_out,
    up_in,
    hidden_own,
    hidden_all,
    down_out,
    down_in,
    read_v,
    in_sems,
    send_sems,
    recv_sems,
    tok_sems,
    mixed_sems,
    hidden_sems,
    far_sem,
):
    kv, t = lax.axis_index("kv"), lax.axis_index("tp")
    z, x = kv // NX, kv % NX
    y, core = t // 2, t % 2
    rows_at = (t + NZ - z) % NZ
    has_self = t == (2 * z) % NZ

    xs = [(x + d) % 4 for d in range(4)]
    ys = [(y + d) % 4 for d in range(4)]
    zs = [(z + d) % 8 for d in range(8)]
    cores = [core, 1 - core]
    kvs = [[pz * NX + px for px in xs] for pz in zs]
    ts = [[2 * py + pc for pc in cores] for py in ys]
    sibling = ts[0][1]

    def copy_to(src, dst, k, pkv, pt, arrived=None):
        return pltpu.make_async_remote_copy(
            src_ref=src,
            dst_ref=dst,
            send_sem=send_sems.at[k],
            recv_sem=recv_sems.at[k] if arrived is None else arrived,
            device_id=(pkv, pt),
            device_id_type=MESH,
        )

    leaving, mix_sent = [], []

    def finish():
        for ref, k in leaving:
            wait_for(ref, send_sems.at[k])
        if mix_sent:
            @pl.when(has_self)
            def _():
                wait_for(mix_all.at[pl.ds(0, 31)], send_sems.at[8])

            @pl.when(jnp.logical_not(has_self))
            def _():
                wait_for(mix_all, send_sems.at[8])

    barrier = pltpu.get_barrier_semaphore()

    def tell(pkv, pt):
        pl.semaphore_signal(barrier, inc=1, device_id=(pkv, pt), device_id_type=MESH)

    for dx, dy, dc in PLANE:
        tell(kvs[0][dx], ts[dy][dc])
    for dz in (2, 6, 1, 7):
        for dx in (2, 1, 3, 0):
            tell(kvs[dz][dx], sibling)
    for dz in (2, 6):
        tell(kvs[dz][0], t)

    loads = [
        pltpu.make_async_copy(tokens_hbm, tok_v, in_sems.at[0]),
        pltpu.make_async_copy(norm_gain_hbm, gain_v.at[0], in_sems.at[1]),
        pltpu.make_async_copy(wq_hbm, w4_v.at[0], in_sems.at[2]),
        pltpu.make_async_copy(wf_hbm, w4_v.at[1], in_sems.at[3]),
        pltpu.make_async_copy(wi_hbm, w4_v.at[2], in_sems.at[4]),
        pltpu.make_async_copy(wg_hbm, w4_v.at[3], in_sems.at[5]),
        pltpu.make_async_copy(wout_hbm, wout_v, in_sems.at[6]),
        pltpu.make_async_copy(wup_hbm, wup_v, in_sems.at[7]),
        pltpu.make_async_copy(wdown_hbm, wdown_v, in_sems.at[8]),
        pltpu.make_async_copy(bound_hbm, bound_v, in_sems.at[9]),
        pltpu.make_async_copy(head_gain_hbm, head_gain_v, in_sems.at[10]),
        pltpu.make_async_copy(state_hbm, state_v, in_sems.at[11]),
        pltpu.make_async_copy(mixer_gain_hbm, gain_v.at[1], in_sems.at[12]),
    ]
    for load in loads:
        load.start()

    loads[0].wait()
    tok_f = tok_v[...].astype(F32)
    tok_all[x * NT + t] = jnp.concatenate([tok_f[0:24], tok_f[24:48]], axis=1).astype(BF16)
    loads[1].wait()
    loads[12].wait()
    for q in range(2):
        g = gain_v[q]
        gains[x, q : q + 1, :] = jnp.concatenate([g, g], axis=1)
    for k in range(2, 9):
        loads[k].wait()
    w_up[x] = wup_v[:, pl.ds(pl.multiple_of(x * 256, 256), 256)]
    w_out[t] = wout_v[...]
    w_down[x] = wdown_v[:, pl.ds(pl.multiple_of(x * 256, 256), 256)]

    pl.semaphore_wait(barrier, 31 + 16 + 2)
    for step in (2, 6):
        pl.semaphore_signal(
            far_sem, inc=1, device_id=(kvs[step][0], t), device_id_type=MESH
        )

    own_tok = tok_all.at[x * NT + t]

    def send_tokens(steps):
        for dx, dy, dc in steps:
            copy_to(own_tok, own_tok, 0, kvs[0][dx], ts[dy][dc], tok_sems.at[t]).start()

    send_tokens(PLANE[:FIRST_TOKENS])
    for (dx,) in ALONG_X:
        copy_to(gains.at[x], gains.at[x], 1, kvs[0][dx], t).start()
    for dx in (2, 1, 3, 0):
        copy_to(w4_v.at[xs[dx]], w_first.at[x], 2, kvs[0][dx], sibling).start()
    send_tokens(PLANE[FIRST_TOKENS:])
    leaving.append((tok_all.at[pl.ds(0, 31)], 0))
    leaving.append((gains.at[pl.ds(0, 3)], 1))
    leaving.append((w_first, 2))

    for dy, dc in ALONG_Y:
        copy_to(w_out.at[t], w_out.at[t], 3, kv, ts[dy][dc]).start()
    leaving.append((w_out.at[pl.ds(0, 7)], 3))

    wait_for(gains.at[pl.ds(0, 3)], recv_sems.at[1])
    wait_for(w_first, recv_sems.at[2])

    pl.semaphore_wait(far_sem, 2)
    for dy, dc in NEAR_Y:
        pz = ts[dy][dc]
        wait_for(tok_all.at[pl.ds(0, 3 if dy == dc == 0 else 4)], tok_sems.at[pz])
        raw = [tok_all[q * NT + pz].astype(F32) for q in range(NX)]
        lhs = unpacked([raw[q] * gains[q, 0:1, :] for q in range(NX)])
        partial = jnp.dot(lhs, w_first[...].reshape(256, 256), preferred_element_type=F32)
        for half in range(2):
            left = partial[24 * half : 24 * half + 24, 0:128]
            right = partial[24 * half : 24 * half + 24, 128:256]
            proj_out[pz * NX + 2 * half] = jnp.concatenate(
                [left[0:12], right[0:12]], axis=0
            ).astype(BF16)
            proj_out[pz * NX + 2 * half + 1] = jnp.concatenate(
                [left[12:24], right[12:24]], axis=0
            ).astype(BF16)
        sq_out[pz] = row_squares(raw)
        for dx in (2, 1, 3, 0):
            to = pz * NX + xs[dx]
            copy_to(proj_out.at[to], proj_in.at[kv], 5, to, sibling).start()
        copy_to(sq_out.at[pz], sq1.at[z], 4, pz * NX + x, sibling).start()
    leaving.append((sq1, 4))
    leaving.append((proj_in, 5))

    for (dx,) in ALONG_X:
        cols = pl.ds(pl.multiple_of(xs[dx] * 256, 256), 256)
        copy_to(wup_v.at[:, cols], w_up.at[x], 6, kvs[0][dx], t).start()
        copy_to(wdown_v.at[:, cols], w_down.at[x], 7, kvs[0][dx], t).start()
    leaving.append((w_up.at[pl.ds(0, 3)], 6))
    leaving.append((w_down.at[pl.ds(0, 3)], 7))

    for k in range(9, 12):
        loads[k].wait()
    wait_for(sq1, recv_sems.at[4])
    wait_for(proj_in, recv_sems.at[5])

    squares = sq1[0]
    for q in range(1, NZ):
        squares = squares + sq1[q]
    square_row = jnp.where(x // 2 == 0, squares[0:1, :], squares[1:2, :])
    row_scale = lax.rsqrt(
        column_of(square_row, (x % 2) * 12, 12) / WIDTH + NORM_EPS
    )
    owned = []
    for q in range(NX):
        total = proj_in[q].astype(F32)
        for r in range(1, NZ):
            total = total + proj_in[r * NX + q].astype(F32)
        owned.append(total * row_scale)
    queries, forget_raw, values_in, gate_raw = owned
    head0 = lax.broadcasted_iota(jnp.int32, (24, 128), 0) < 12
    bound = jnp.where(head0, bound_v[0:1, :], bound_v[1:2, :])
    head_gain = jnp.where(head0, head_gain_v[0:1, :], head_gain_v[1:2, :])
    forget = bound + (1.0 - bound) * jax.nn.sigmoid(forget_raw)
    pad = jnp.zeros((104, 128), F32)
    kept = queries * forget
    kept_t = jnp.concatenate([kept, pad], axis=0).T
    fresh = jnp.sum(queries * (1.0 - forget), axis=1, keepdims=True) * values_in
    for j in range(24):
        read_v[j : j + 1, :] = jnp.sum(
            kept_t[:, j : j + 1] * state_v[j % 12, j // 12], axis=0, keepdims=True
        )
    read = read_v[...] + fresh
    read = read * lax.rsqrt(jnp.mean(read * read, axis=1, keepdims=True) + NORM_EPS) * head_gain
    mix_own[...] = (read * jax.nn.silu(gate_raw)).astype(BF16)

    mix_at = t * NX + x
    for dz, dx in COLUMN:
        copy_to(mix_own, mix_all.at[mix_at], 8, kvs[dz][dx], (z + zs[dz]) % NZ).start()

    @pl.when(jnp.logical_not(has_self))
    def _():
        copy_to(mix_own, mix_all.at[mix_at], 8, kv, (2 * z) % NZ).start()

    @pl.when(has_self)
    def _():
        mix_all[mix_at] = mix_own[...]

    mix_sent.append(1)
    forget_t = jnp.concatenate([forget, pad], axis=0).T
    for j in range(24):
        f = forget_t[:, j : j + 1]
        next_v[j % 12, j // 12] = f * state_v[j % 12, j // 12] + (1.0 - f) * values_in[j : j + 1, :]
    wait_for(w_out.at[pl.ds(0, 7)], recv_sems.at[3])

    @pl.when(has_self)
    def _():
        wait_for(mix_all.at[pl.ds(0, 31)], recv_sems.at[8])

    @pl.when(jnp.logical_not(has_self))
    def _():
        wait_for(mix_all, recv_sems.at[8])

    acc = jnp.zeros((96, 128), F32)
    for q in range(NT):
        both = jnp.concatenate([w_out[q, :, 0:128], w_out[q, :, 128:256]], axis=0)
        acc = acc + dot_t(mix_all[4 * q : 4 * q + 4].reshape(96, 128), both)
    folded = []
    for q in range(NX):
        part = acc[24 * q : 24 * q + 24]
        turned = swap_lanes(jnp.concatenate([part[12:24], part[0:12]], axis=0))
        folded.append(part + turned)
    low = low_lanes((24, 128))
    top = jnp.where(low, folded[0], swap_lanes(folded[2]))
    bottom = jnp.where(low, swap_lanes(folded[1]), folded[3])
    attn = jnp.where(head0, top, bottom)
    own_at = x * NT + rows_at
    mixed_all[own_at] = (tok_all[own_at].astype(F32) + attn).astype(BF16)

    own_mixed = mixed_all.at[own_at]
    for dx, dy, dc in PLANE:
        copy_to(own_mixed, own_mixed, 9, kvs[0][dx], ts[dy][dc], mixed_sems.at[rows_at]).start()
    leaving.append((mixed_all.at[pl.ds(0, 31)], 9))
    wait_for(w_up.at[pl.ds(0, 3)], recv_sems.at[6])

    for dy, dc in NEAR_Y:
        pz = (ts[dy][dc] + NZ - z) % NZ
        wait_for(mixed_all.at[pl.ds(0, 3 if dy == dc == 0 else 4)], mixed_sems.at[pz])
        raw = [mixed_all[q * NT + pz].astype(F32) for q in range(NX)]
        lhs = unpacked([raw[q] * gains[q, 1:2, :] for q in range(NX)])
        partial = jnp.dot(lhs, w_up[...].reshape(256, 256), preferred_element_type=F32)
        up_out[pz] = partial.reshape(2, 24, 256).astype(BF16)
        sq_out2[pz] = row_squares(raw)
        copy_to(up_out.at[pz], up_in.at[z], 11, pz * NX + x, sibling).start()
        copy_to(sq_out2.at[pz], sq2.at[z], 10, pz * NX + x, sibling).start()
    leaving.append((sq2, 10))
    leaving.append((up_in, 11))
    wait_for(sq2, recv_sems.at[10])
    squares2 = sq2[0]
    for q in range(1, NZ):
        squares2 = squares2 + sq2[q]
    scales = [
        lax.rsqrt(column_of(squares2[q : q + 1, :], 0, 24) / WIDTH + NORM_EPS) for q in range(2)
    ]
    wait_for(up_in, recv_sems.at[11])

    for half in range(2):
        total = up_in[0, half].astype(F32)
        for q in range(1, NZ):
            total = total + up_in[q, half].astype(F32)
        total = jnp.maximum(total * scales[half], 0.0)
        hidden_own[half] = (total * total).astype(BF16)

    for dz in NEAR_Z[::-1]:
        copy_to(hidden_own, hidden_all.at[z], 12, kvs[dz][0], sibling, hidden_sems.at[z]).start()
    leaving.append((hidden_all, 12))
    wait_for(w_down.at[pl.ds(0, 3)], recv_sems.at[7])

    down_at = t * NX + x
    for dz in NEAR_Z:
        pt = zs[dz]
        wait_for(hidden_all.at[pt], hidden_sems.at[pt])
        partial = dot_t(hidden_all[pt].reshape(48, 256), w_down[...].reshape(256, 256))
        for pair in range(2):
            upper = partial[0:24, 128 * pair : 128 * pair + 128]
            lower = partial[24:48, 128 * pair : 128 * pair + 128]
            down_out[pt * NX + 2 * pair] = jnp.where(low, upper, swap_lanes(lower)).astype(BF16)
            down_out[pt * NX + 2 * pair + 1] = jnp.where(low, swap_lanes(upper), lower).astype(
                BF16
            )
        for dx in (2, 1, 3):
            copy_to(
                down_out.at[pt * NX + xs[dx]], down_in.at[down_at], 13, kvs[0][dx], pt
            ).start()

        @pl.when(pt != t)
        def _():
            copy_to(down_out.at[pt * NX + x], down_in.at[down_at], 13, kv, pt).start()

        @pl.when(pt == t)
        def _():
            down_in[down_at] = down_out[down_at]

    leaving.append((down_in.at[pl.ds(0, 31)], 13))
    wait_for(down_in.at[pl.ds(0, 31)], recv_sems.at[13])
    total = down_in[0].astype(F32)
    for q in range(1, 32):
        total = total + down_in[q].astype(F32)
    total = mixed_all[x * NT + t].astype(F32) + total
    out_ref[...] = jnp.concatenate([total[:, 0:64], total[:, 64:128]], axis=0).astype(BF16)

    finish()


def place(out_v, next_v, out_hbm, next_hbm, sems):
    copies = [
        pltpu.make_async_copy(
            next_v.at[pl.ds(2 * q, 2)], next_hbm.at[pl.ds(2 * q, 2)], sems.at[q]
        )
        for q in range(6)
    ]
    copies.append(pltpu.make_async_copy(out_v, out_hbm, sems.at[6]))
    for copy in copies:
        copy.start()
    for copy in copies:
        copy.wait()


def body(
    tokens,
    norm_gain,
    w_query,
    w_forget,
    w_input,
    w_gate,
    lower_bound,
    head_gain,
    recur_state,
    w_out,
    mixer_gain,
    w_up,
    w_down,
):
    bound = lower_bound.reshape(2, 128)
    any_spec = pl.BlockSpec(memory_space=pltpu.HBM)
    vmem_spec = pl.BlockSpec(memory_space=pltpu.VMEM)
    out, next_state = pl.pallas_call(
        kernel,
        out_shape=(
            jax.ShapeDtypeStruct(tokens.shape, tokens.dtype),
            jax.ShapeDtypeStruct(recur_state.shape, recur_state.dtype),
        ),
        in_specs=[any_spec] * 13,
        out_specs=(vmem_spec, vmem_spec),
        scratch_shapes=[
            pltpu.VMEM((48, 64), BF16),
            pltpu.VMEM((2, 1, 64), F32),
            pltpu.VMEM((4, 64, 256), BF16),
            pltpu.VMEM((2, 128), F32),
            pltpu.VMEM((2, 128), F32),
            pltpu.VMEM((12, 2, 128, 128), F32),
            pltpu.VMEM((64, 256), BF16),
            pltpu.VMEM((64, 1024), BF16),
            pltpu.VMEM((64, 1024), BF16),
            pltpu.VMEM((4, 2, 128), F32),
            pltpu.VMEM((4, 64, 256), BF16),
            pltpu.VMEM((4, 64, 256), BF16),
            pltpu.VMEM((4, 64, 256), BF16),
            pltpu.VMEM((8, 64, 256), BF16),
            pltpu.VMEM((32, 24, 128), BF16),
            pltpu.VMEM((8, 2, 128), F32),
            pltpu.VMEM((8, 2, 128), F32),
            pltpu.VMEM((32, 24, 128), BF16),
            pltpu.VMEM((32, 24, 128), BF16),
            pltpu.VMEM((24, 128), BF16),
            pltpu.VMEM((32, 24, 128), BF16),
            pltpu.VMEM((32, 24, 128), BF16),
            pltpu.VMEM((8, 2, 128), F32),
            pltpu.VMEM((8, 2, 128), F32),
            pltpu.VMEM((8, 2, 24, 256), BF16),
            pltpu.VMEM((8, 2, 24, 256), BF16),
            pltpu.VMEM((2, 24, 256), BF16),
            pltpu.VMEM((8, 2, 24, 256), BF16),
            pltpu.VMEM((32, 24, 128), BF16),
            pltpu.VMEM((32, 24, 128), BF16),
            pltpu.VMEM((24, 128), F32),
            pltpu.SemaphoreType.DMA((13,)),
            pltpu.SemaphoreType.DMA((14,)),
            pltpu.SemaphoreType.DMA((14,)),
            pltpu.SemaphoreType.DMA((8,)),
            pltpu.SemaphoreType.DMA((8,)),
            pltpu.SemaphoreType.DMA((8,)),
            pltpu.SemaphoreType.REGULAR,
        ],
        compiler_params=pltpu.CompilerParams(collective_id=0, has_side_effects=True, vmem_limit_bytes=16 * 1024 * 1024),
        name="decode_layer",
    )(*(pltpu.with_memory_space_constraint(a, pltpu.HBM) for a in (
        tokens,
        norm_gain.reshape(1, 64),
        mixer_gain.reshape(1, 64),
        w_query,
        w_forget,
        w_input,
        w_gate,
        bound,
        head_gain,
        recur_state,
        w_out.T,
        w_up,
        w_down.T,
    )))
    return pl.pallas_call(
        place,
        out_shape=(
            jax.ShapeDtypeStruct(out.shape, out.dtype),
            jax.ShapeDtypeStruct(next_state.shape, next_state.dtype),
        ),
        in_specs=[vmem_spec, vmem_spec],
        out_specs=(any_spec, any_spec),
        scratch_shapes=[pltpu.SemaphoreType.DMA((7,))],
        compiler_params=pltpu.CompilerParams(vmem_limit_bytes=4 * 1024 * 1024),
        name="place_outputs",
    )(out, next_state)


def solution(mesh):
    in_specs = (
        P("tp", "kv"),
        P("kv"),
        P("kv", "tp"),
        P("kv", "tp"),
        P("kv", "tp"),
        P("kv", "tp"),
        P("tp"),
        P("tp", None),
        P("kv", "tp", None, None),
        P("tp", "kv"),
        P("kv"),
        P("kv", "tp"),
        P("tp", "kv"),
    )
    out_specs = (P("tp", "kv"), P("kv", "tp", None, None))
    return jax.shard_map(body, mesh=mesh, in_specs=in_specs, out_specs=out_specs, check_vma=False)
```

```python
import itertools

import jax
import jax.numpy as jnp
from jax import lax
from jax.experimental import pallas as pl
from jax.experimental.pallas import tpu as pltpu
from jax.sharding import PartitionSpec as P

NORM_EPS = 1e-05
MESH = pl.DeviceIdType.MESH
F32 = jnp.float32
BF16 = jnp.bfloat16

NZ, NX, NT = 8, 4, 8
WIDTH = 2048.0


def hops(step, size):
    return min(step, size - step)


def by_distance(sizes):
    steps = list(itertools.product(*(range(n) for n in sizes)))[1:]
    return sorted(steps, key=lambda d: (-sum(hops(s, n) for s, n in zip(d, sizes)), d))


PLANE = by_distance((4, 4, 2))
COLUMN = by_distance((8, 4))
ALONG_X = by_distance((4,))
ALONG_Y = by_distance((4, 2))
ALONG_Z = by_distance((8,))
NEAR_Z = [0, 1, 7, 2, 6, 3, 5, 4]


def wait_for(ref, sem):
    pltpu.make_async_copy(ref, ref, sem).wait()


def swap_lanes(value):
    return pltpu.roll(value, 64, 1)


def dot_t(a, b):
    return lax.dot_general(a, b, (((1,), (1,)), ((), ())), preferred_element_type=F32)


def low_lanes(shape):
    return lax.broadcasted_iota(jnp.int32, shape, 1) < 64


def unpacked(pieces):
    low = low_lanes(pieces[0].shape)
    swapped = [swap_lanes(p) for p in pieces]
    first = [jnp.where(low, pieces[i], swapped[i + 1]).astype(BF16) for i in (0, 2)]
    second = [jnp.where(low, swapped[i], pieces[i + 1]).astype(BF16) for i in (0, 2)]
    return jnp.concatenate(
        [jnp.concatenate(first, axis=1), jnp.concatenate(second, axis=1)], axis=0
    )


def row_squares(pieces):
    total = pieces[0] * pieces[0]
    for p in pieces[1:]:
        total = total + p * p
    total = jnp.concatenate([total, jnp.zeros((64, 128), F32)], axis=0)
    high = total.astype(BF16)
    rest = (total - high.astype(F32)).astype(BF16)
    lane = lax.broadcasted_iota(jnp.int32, (8, 128), 1)
    row = lax.broadcasted_iota(jnp.int32, (8, 128), 0)
    pick = jnp.where((lane // 64) == row, 1.0, 0.0).astype(BF16)
    dims = (((1,), (1,)), ((), ()))
    sums = lax.dot_general(pick, high, dims, preferred_element_type=F32)
    sums = sums + lax.dot_general(pick, rest, dims, preferred_element_type=F32)
    return sums[0:2, :]


def column_of(values, base, period):
    lane = lax.broadcasted_iota(jnp.int32, (24, 256), 1)
    row = lax.broadcasted_iota(jnp.int32, (24, 256), 0)
    return jnp.sum(
        jnp.where(lane == base + row % period, values, 0.0), axis=1, keepdims=True
    )


def kernel(
    tokens_hbm,
    norm_gain_hbm,
    mixer_gain_hbm,
    wq_hbm,
    wf_hbm,
    wi_hbm,
    wg_hbm,
    bound_hbm,
    head_gain_hbm,
    state_hbm,
    wout_hbm,
    wup_hbm,
    wdown_hbm,
    out_ref,
    next_v,
    tok_v,
    gain_v,
    w4_v,
    bound_v,
    head_gain_v,
    state_v,
    wout_v,
    wup_v,
    wdown_v,
    gains,
    w_first,
    w_up,
    w_down,
    w_out,
    tok_all,
    sq1,
    proj_out,
    proj_in,
    mix_own,
    mix_all,
    mixed_all,
    sq2,
    up_out,
    up_in,
    hidden_all,
    down_out,
    down_in,
    read_v,
    in_sems,
    send_sems,
    recv_sems,
    hidden_sems,
    far_sem,
):
    kv, t = lax.axis_index("kv"), lax.axis_index("tp")
    z, x = kv // NX, kv % NX
    y, core = t // 2, t % 2
    rows_at = (t + NZ - z) % NZ
    has_self = t == (2 * z) % NZ

    xs = [(x + d) % 4 for d in range(4)]
    ys = [(y + d) % 4 for d in range(4)]
    zs = [(z + d) % 8 for d in range(8)]
    cores = [core, 1 - core]
    kvs = [[pz * NX + px for px in xs] for pz in zs]
    ts = [[2 * py + pc for pc in cores] for py in ys]

    def copy_to(src, dst, k, pkv, pt, arrived=None):
        return pltpu.make_async_remote_copy(
            src_ref=src,
            dst_ref=dst,
            send_sem=send_sems.at[k],
            recv_sem=recv_sems.at[k] if arrived is None else arrived,
            device_id=(pkv, pt),
            device_id_type=MESH,
        )

    leaving, mix_sent = [], []

    def finish():
        for ref, k in leaving:
            wait_for(ref, send_sems.at[k])
        if mix_sent:
            @pl.when(has_self)
            def _():
                wait_for(mix_all.at[pl.ds(0, 31)], send_sems.at[8])

            @pl.when(jnp.logical_not(has_self))
            def _():
                wait_for(mix_all, send_sems.at[8])

    barrier = pltpu.get_barrier_semaphore()

    def tell(pkv, pt):
        pl.semaphore_signal(barrier, inc=1, device_id=(pkv, pt), device_id_type=MESH)

    for dx, dy, dc in PLANE:
        tell(kvs[0][dx], ts[dy][dc])
    for dz in (2, 6, 1, 7):
        for dx in (2, 1, 3, 0):
            tell(kvs[dz][dx], t)

    loads = [
        pltpu.make_async_copy(tokens_hbm, tok_v, in_sems.at[0]),
        pltpu.make_async_copy(norm_gain_hbm, gain_v.at[0], in_sems.at[1]),
        pltpu.make_async_copy(wq_hbm, w4_v.at[0], in_sems.at[2]),
        pltpu.make_async_copy(wf_hbm, w4_v.at[1], in_sems.at[3]),
        pltpu.make_async_copy(wi_hbm, w4_v.at[2], in_sems.at[4]),
        pltpu.make_async_copy(wg_hbm, w4_v.at[3], in_sems.at[5]),
        pltpu.make_async_copy(wout_hbm, wout_v, in_sems.at[6]),
        pltpu.make_async_copy(wup_hbm, wup_v, in_sems.at[7]),
        pltpu.make_async_copy(wdown_hbm, wdown_v, in_sems.at[8]),
        pltpu.make_async_copy(bound_hbm, bound_v, in_sems.at[9]),
        pltpu.make_async_copy(head_gain_hbm, head_gain_v, in_sems.at[10]),
        pltpu.make_async_copy(state_hbm, state_v, in_sems.at[11]),
        pltpu.make_async_copy(mixer_gain_hbm, gain_v.at[1], in_sems.at[12]),
    ]
    for load in loads:
        load.start()

    loads[0].wait()
    tok_f = tok_v[...].astype(F32)
    tok_all[x * NT + t] = jnp.concatenate([tok_f[0:24], tok_f[24:48]], axis=1).astype(BF16)
    loads[1].wait()
    loads[12].wait()
    for q in range(2):
        g = gain_v[q]
        gains[x, q : q + 1, :] = jnp.concatenate([g, g], axis=1)
    for k in range(2, 9):
        loads[k].wait()
    w_first[x] = w4_v[x]
    w_up[x] = wup_v[:, pl.ds(pl.multiple_of(x * 256, 256), 256)]
    w_out[t] = wout_v[...]
    w_down[x] = wdown_v[:, pl.ds(pl.multiple_of(x * 256, 256), 256)]

    pl.semaphore_wait(barrier, 31 + 16)
    for step in (2, 6):
        pl.semaphore_signal(
            far_sem, inc=1, device_id=(kvs[step][0], t), device_id_type=MESH
        )

    for (dx,) in ALONG_X:
        copy_to(gains.at[x], gains.at[x], 1, kvs[0][dx], t).start()
    own_tok = tok_all.at[x * NT + t]
    for dx, dy, dc in PLANE:
        copy_to(own_tok, own_tok, 0, kvs[0][dx], ts[dy][dc]).start()
    for (dx,) in ALONG_X:
        copy_to(w4_v.at[xs[dx]], w_first.at[x], 2, kvs[0][dx], t).start()
    leaving.append((tok_all.at[pl.ds(0, 31)], 0))
    leaving.append((gains.at[pl.ds(0, 3)], 1))
    leaving.append((w_first.at[pl.ds(0, 3)], 2))
    wait_for(gains.at[pl.ds(0, 3)], recv_sems.at[1])
    wait_for(tok_all.at[pl.ds(0, 31)], recv_sems.at[0])

    for dy, dc in ALONG_Y:
        copy_to(w_out.at[t], w_out.at[t], 3, kv, ts[dy][dc]).start()
    leaving.append((w_out.at[pl.ds(0, 7)], 3))

    raw = [
        tok_all[pl.ds(NT * q, NT)].astype(F32).reshape(192, 128) for q in range(NX)
    ]
    sq1[z] = row_squares(raw)
    lhs = unpacked([raw[q] * gains[q, 0:1, :] for q in range(NX)])
    wait_for(w_first.at[pl.ds(0, 3)], recv_sems.at[2])
    partial = jnp.dot(lhs, w_first[...].reshape(256, 256), preferred_element_type=F32)

    for half in range(2):
        for pz in range(NZ):
            at = half * 192 + pz * 24
            left = partial[at : at + 24, 0:128]
            right = partial[at : at + 24, 128:256]
            proj_out[pz * NX + 2 * half] = jnp.concatenate(
                [left[0:12], right[0:12]], axis=0
            ).astype(BF16)
            proj_out[pz * NX + 2 * half + 1] = jnp.concatenate(
                [left[12:24], right[12:24]], axis=0
            ).astype(BF16)

    pl.semaphore_wait(far_sem, 2)

    for (dz,) in ALONG_Z:
        copy_to(sq1.at[z], sq1.at[z], 4, kvs[dz][0], t).start()
    for dz, dx in COLUMN:
        copy_to(proj_out.at[kvs[dz][dx]], proj_in.at[kv], 5, kvs[dz][dx], t).start()
    proj_in[kv] = proj_out[kv]
    leaving.append((sq1.at[pl.ds(0, 7)], 4))
    leaving.append((proj_in.at[pl.ds(0, 31)], 5))

    for (dx,) in ALONG_X:
        cols = pl.ds(pl.multiple_of(xs[dx] * 256, 256), 256)
        copy_to(wup_v.at[:, cols], w_up.at[x], 6, kvs[0][dx], t).start()
        copy_to(wdown_v.at[:, cols], w_down.at[x], 7, kvs[0][dx], t).start()
    leaving.append((w_up.at[pl.ds(0, 3)], 6))
    leaving.append((w_down.at[pl.ds(0, 3)], 7))

    for k in range(9, 12):
        loads[k].wait()
    wait_for(sq1.at[pl.ds(0, 7)], recv_sems.at[4])
    wait_for(proj_in.at[pl.ds(0, 31)], recv_sems.at[5])

    squares = sq1[0]
    for q in range(1, NZ):
        squares = squares + sq1[q]
    square_row = jnp.where(x // 2 == 0, squares[0:1, :], squares[1:2, :])
    row_scale = lax.rsqrt(
        column_of(square_row, z * 24 + (x % 2) * 12, 12) / WIDTH + NORM_EPS
    )
    owned = []
    for q in range(NX):
        total = proj_in[q].astype(F32)
        for r in range(1, NZ):
            total = total + proj_in[r * NX + q].astype(F32)
        owned.append(total * row_scale)
    queries, forget_raw, values_in, gate_raw = owned
    head0 = lax.broadcasted_iota(jnp.int32, (24, 128), 0) < 12
    bound = jnp.where(head0, bound_v[0:1, :], bound_v[1:2, :])
    head_gain = jnp.where(head0, head_gain_v[0:1, :], head_gain_v[1:2, :])
    forget = bound + (1.0 - bound) * jax.nn.sigmoid(forget_raw)
    pad = jnp.zeros((104, 128), F32)
    kept = queries * forget
    kept_t = jnp.concatenate([kept, pad], axis=0).T
    fresh = jnp.sum(queries * (1.0 - forget), axis=1, keepdims=True) * values_in
    for j in range(24):
        read_v[j : j + 1, :] = jnp.sum(
            kept_t[:, j : j + 1] * state_v[j % 12, j // 12], axis=0, keepdims=True
        )
    read = read_v[...] + fresh
    read = read * lax.rsqrt(jnp.mean(read * read, axis=1, keepdims=True) + NORM_EPS) * head_gain
    mix_own[...] = (read * jax.nn.silu(gate_raw)).astype(BF16)

    mix_at = t * NX + x
    for dz, dx in COLUMN:
        copy_to(mix_own, mix_all.at[mix_at], 8, kvs[dz][dx], (z + zs[dz]) % NZ).start()

    @pl.when(jnp.logical_not(has_self))
    def _():
        copy_to(mix_own, mix_all.at[mix_at], 8, kv, (2 * z) % NZ).start()

    @pl.when(has_self)
    def _():
        mix_all[mix_at] = mix_own[...]

    mix_sent.append(1)
    forget_t = jnp.concatenate([forget, pad], axis=0).T
    for j in range(24):
        f = forget_t[:, j : j + 1]
        next_v[j % 12, j // 12] = f * state_v[j % 12, j // 12] + (1.0 - f) * values_in[j : j + 1, :]
    wait_for(w_out.at[pl.ds(0, 7)], recv_sems.at[3])

    @pl.when(has_self)
    def _():
        wait_for(mix_all.at[pl.ds(0, 31)], recv_sems.at[8])

    @pl.when(jnp.logical_not(has_self))
    def _():
        wait_for(mix_all, recv_sems.at[8])

    acc = jnp.zeros((96, 128), F32)
    for q in range(NT):
        both = jnp.concatenate([w_out[q, :, 0:128], w_out[q, :, 128:256]], axis=0)
        acc = acc + dot_t(mix_all[4 * q : 4 * q + 4].reshape(96, 128), both)
    folded = []
    for q in range(NX):
        part = acc[24 * q : 24 * q + 24]
        turned = swap_lanes(jnp.concatenate([part[12:24], part[0:12]], axis=0))
        folded.append(part + turned)
    low = low_lanes((24, 128))
    top = jnp.where(low, folded[0], swap_lanes(folded[2]))
    bottom = jnp.where(low, swap_lanes(folded[1]), folded[3])
    attn = jnp.where(head0, top, bottom)
    own_at = x * NT + rows_at
    mixed_all[own_at] = (tok_all[own_at].astype(F32) + attn).astype(BF16)

    for dx, dy, dc in PLANE:
        copy_to(mixed_all.at[own_at], mixed_all.at[own_at], 9, kvs[0][dx], ts[dy][dc]).start()
    leaving.append((mixed_all.at[pl.ds(0, 31)], 9))
    wait_for(w_up.at[pl.ds(0, 3)], recv_sems.at[6])
    wait_for(mixed_all.at[pl.ds(0, 31)], recv_sems.at[9])

    raw2 = [
        mixed_all[pl.ds(NT * q, NT)].astype(F32).reshape(192, 128) for q in range(NX)
    ]
    sq2[z] = row_squares(raw2)
    lhs2 = unpacked([raw2[q] * gains[q, 1:2, :] for q in range(NX)])
    partial2 = jnp.dot(lhs2, w_up[...].reshape(256, 256), preferred_element_type=F32)
    for half in range(2):
        for pz in range(NZ):
            at = half * 192 + pz * 24
            up_out[pz, half] = partial2[at : at + 24].astype(BF16)

    for (dz,) in ALONG_Z:
        copy_to(up_out.at[zs[dz]], up_in.at[z], 11, kvs[dz][0], t).start()
        copy_to(sq2.at[z], sq2.at[z], 10, kvs[dz][0], t).start()
    up_in[z] = up_out[z]
    leaving.append((sq2.at[pl.ds(0, 7)], 10))
    leaving.append((up_in.at[pl.ds(0, 7)], 11))
    wait_for(sq2.at[pl.ds(0, 7)], recv_sems.at[10])
    squares2 = sq2[0]
    for q in range(1, NZ):
        squares2 = squares2 + sq2[q]
    scales = [
        lax.rsqrt(column_of(squares2[q : q + 1, :], z * 24, 24) / WIDTH + NORM_EPS)
        for q in range(2)
    ]
    wait_for(up_in.at[pl.ds(0, 7)], recv_sems.at[11])

    for half in range(2):
        total = up_in[0, half].astype(F32)
        for q in range(1, NZ):
            total = total + up_in[q, half].astype(F32)
        total = jnp.maximum(total * scales[half], 0.0)
        hidden_all[z, half] = (total * total).astype(BF16)

    own_hidden = hidden_all.at[z]
    for (dz,) in ALONG_Z:
        copy_to(own_hidden, own_hidden, 12, kvs[dz][0], t, hidden_sems.at[z]).start()
    leaving.append((hidden_all.at[pl.ds(0, 7)], 12))
    wait_for(w_down.at[pl.ds(0, 3)], recv_sems.at[7])

    down_at = t * NX + x
    for dz in NEAR_Z:
        pt = zs[dz]
        if dz:
            wait_for(hidden_all.at[pt], hidden_sems.at[pt])
        partial = dot_t(hidden_all[pt].reshape(48, 256), w_down[...].reshape(256, 256))
        for pair in range(2):
            upper = partial[0:24, 128 * pair : 128 * pair + 128]
            lower = partial[24:48, 128 * pair : 128 * pair + 128]
            down_out[pt * NX + 2 * pair] = jnp.where(low, upper, swap_lanes(lower)).astype(BF16)
            down_out[pt * NX + 2 * pair + 1] = jnp.where(low, swap_lanes(upper), lower).astype(
                BF16
            )
        for dx in (2, 1, 3):
            copy_to(
                down_out.at[pt * NX + xs[dx]], down_in.at[down_at], 13, kvs[0][dx], pt
            ).start()

        @pl.when(pt != t)
        def _():
            copy_to(down_out.at[pt * NX + x], down_in.at[down_at], 13, kv, pt).start()

        @pl.when(pt == t)
        def _():
            down_in[down_at] = down_out[down_at]

    leaving.append((down_in.at[pl.ds(0, 31)], 13))
    wait_for(down_in.at[pl.ds(0, 31)], recv_sems.at[13])
    total = down_in[0].astype(F32)
    for q in range(1, 32):
        total = total + down_in[q].astype(F32)
    total = mixed_all[x * NT + t].astype(F32) + total
    out_ref[...] = jnp.concatenate([total[:, 0:64], total[:, 64:128]], axis=0).astype(BF16)

    finish()


def place(out_v, next_v, out_hbm, next_hbm, sems):
    copies = [
        pltpu.make_async_copy(
            next_v.at[pl.ds(2 * q, 2)], next_hbm.at[pl.ds(2 * q, 2)], sems.at[q]
        )
        for q in range(6)
    ]
    copies.append(pltpu.make_async_copy(out_v, out_hbm, sems.at[6]))
    for copy in copies:
        copy.start()
    for copy in copies:
        copy.wait()


def body(
    tokens,
    norm_gain,
    w_query,
    w_forget,
    w_input,
    w_gate,
    lower_bound,
    head_gain,
    recur_state,
    w_out,
    mixer_gain,
    w_up,
    w_down,
):
    bound = lower_bound.reshape(2, 128)
    any_spec = pl.BlockSpec(memory_space=pltpu.HBM)
    vmem_spec = pl.BlockSpec(memory_space=pltpu.VMEM)
    out, next_state = pl.pallas_call(
        kernel,
        out_shape=(
            jax.ShapeDtypeStruct(tokens.shape, tokens.dtype),
            jax.ShapeDtypeStruct(recur_state.shape, recur_state.dtype),
        ),
        in_specs=[any_spec] * 13,
        out_specs=(vmem_spec, vmem_spec),
        scratch_shapes=[
            pltpu.VMEM((48, 64), BF16),
            pltpu.VMEM((2, 1, 64), F32),
            pltpu.VMEM((4, 64, 256), BF16),
            pltpu.VMEM((2, 128), F32),
            pltpu.VMEM((2, 128), F32),
            pltpu.VMEM((12, 2, 128, 128), F32),
            pltpu.VMEM((64, 256), BF16),
            pltpu.VMEM((64, 1024), BF16),
            pltpu.VMEM((64, 1024), BF16),
            pltpu.VMEM((4, 2, 128), F32),
            pltpu.VMEM((4, 64, 256), BF16),
            pltpu.VMEM((4, 64, 256), BF16),
            pltpu.VMEM((4, 64, 256), BF16),
            pltpu.VMEM((8, 64, 256), BF16),
            pltpu.VMEM((32, 24, 128), BF16),
            pltpu.VMEM((8, 2, 256), F32),
            pltpu.VMEM((32, 24, 128), BF16),
            pltpu.VMEM((32, 24, 128), BF16),
            pltpu.VMEM((24, 128), BF16),
            pltpu.VMEM((32, 24, 128), BF16),
            pltpu.VMEM((32, 24, 128), BF16),
            pltpu.VMEM((8, 2, 256), F32),
            pltpu.VMEM((8, 2, 24, 256), BF16),
            pltpu.VMEM((8, 2, 24, 256), BF16),
            pltpu.VMEM((8, 2, 24, 256), BF16),
            pltpu.VMEM((32, 24, 128), BF16),
            pltpu.VMEM((32, 24, 128), BF16),
            pltpu.VMEM((24, 128), F32),
            pltpu.SemaphoreType.DMA((13,)),
            pltpu.SemaphoreType.DMA((14,)),
            pltpu.SemaphoreType.DMA((14,)),
            pltpu.SemaphoreType.DMA((8,)),
            pltpu.SemaphoreType.REGULAR,
        ],
        compiler_params=pltpu.CompilerParams(collective_id=0, has_side_effects=True, vmem_limit_bytes=16 * 1024 * 1024),
        name="decode_layer",
    )(*(pltpu.with_memory_space_constraint(a, pltpu.HBM) for a in (
        tokens,
        norm_gain.reshape(1, 64),
        mixer_gain.reshape(1, 64),
        w_query,
        w_forget,
        w_input,
        w_gate,
        bound,
        head_gain,
        recur_state,
        w_out.T,
        w_up,
        w_down.T,
    )))
    return pl.pallas_call(
        place,
        out_shape=(
            jax.ShapeDtypeStruct(out.shape, out.dtype),
            jax.ShapeDtypeStruct(next_state.shape, next_state.dtype),
        ),
        in_specs=[vmem_spec, vmem_spec],
        out_specs=(any_spec, any_spec),
        scratch_shapes=[pltpu.SemaphoreType.DMA((7,))],
        compiler_params=pltpu.CompilerParams(vmem_limit_bytes=4 * 1024 * 1024),
        name="place_outputs",
    )(out, next_state)


def solution(mesh):
    in_specs = (
        P("tp", "kv"),
        P("kv"),
        P("kv", "tp"),
        P("kv", "tp"),
        P("kv", "tp"),
        P("kv", "tp"),
        P("tp"),
        P("tp", None),
        P("kv", "tp", None, None),
        P("tp", "kv"),
        P("kv"),
        P("kv", "tp"),
        P("tp", "kv"),
    )
    out_specs = (P("tp", "kv"), P("kv", "tp", None, None))
    return jax.shard_map(body, mesh=mesh, in_specs=in_specs, out_specs=out_specs, check_vma=False)
```

```python
import itertools

import jax
import jax.numpy as jnp
from jax import lax
from jax.experimental import pallas as pl
from jax.experimental.pallas import tpu as pltpu
from jax.sharding import PartitionSpec as P

NORM_EPS = 1e-05
MESH = pl.DeviceIdType.MESH
F32 = jnp.float32
BF16 = jnp.bfloat16

NZ, NX, NT = 8, 4, 8
WIDTH = 2048.0


def hops(step, size):
    return min(step, size - step)


def by_distance(sizes):
    steps = list(itertools.product(*(range(n) for n in sizes)))[1:]
    return sorted(steps, key=lambda d: (-sum(hops(s, n) for s, n in zip(d, sizes)), d))


PLANE = by_distance((4, 4, 2))
COLUMN = by_distance((8, 4))
ALONG_X = by_distance((4,))
ALONG_Y = by_distance((4, 2))
ROW = by_distance((4, 2))
ALONG_Z = by_distance((8,))
NEAR_Z = [0, 1, 7, 2, 6, 3, 5, 4]


def wait_for(ref, sem):
    pltpu.make_async_copy(ref, ref, sem).wait()


def swap_lanes(value):
    return pltpu.roll(value, 64, 1)


def dot_t(a, b):
    return lax.dot_general(a, b, (((1,), (1,)), ((), ())), preferred_element_type=F32)


def low_lanes(shape):
    return lax.broadcasted_iota(jnp.int32, shape, 1) < 64


def unpacked(pieces):
    low = low_lanes(pieces[0].shape)
    swapped = [swap_lanes(p) for p in pieces]
    first = [jnp.where(low, pieces[i], swapped[i + 1]).astype(BF16) for i in (0, 2)]
    second = [jnp.where(low, swapped[i], pieces[i + 1]).astype(BF16) for i in (0, 2)]
    return jnp.concatenate(
        [jnp.concatenate(first, axis=1), jnp.concatenate(second, axis=1)], axis=0
    )


def row_squares(pieces):
    total = pieces[0] * pieces[0]
    for p in pieces[1:]:
        total = total + p * p
    spare = -total.shape[0] % 128
    total = jnp.concatenate([total, jnp.zeros((spare, 128), F32)], axis=0)
    high = total.astype(BF16)
    rest = (total - high.astype(F32)).astype(BF16)
    lane = lax.broadcasted_iota(jnp.int32, (8, 128), 1)
    row = lax.broadcasted_iota(jnp.int32, (8, 128), 0)
    pick = jnp.where((lane // 64) == row, 1.0, 0.0).astype(BF16)
    dims = (((1,), (1,)), ((), ()))
    sums = lax.dot_general(pick, high, dims, preferred_element_type=F32)
    sums = sums + lax.dot_general(pick, rest, dims, preferred_element_type=F32)
    return sums[0:2, :]


def column_of(values, base, period, rows=24):
    shape = (rows, values.shape[1])
    lane = lax.broadcasted_iota(jnp.int32, shape, 1)
    row = lax.broadcasted_iota(jnp.int32, shape, 0)
    return jnp.sum(
        jnp.where(lane == base + row % period, values, 0.0), axis=1, keepdims=True
    )


def kernel(
    tokens_hbm,
    norm_gain_hbm,
    mixer_gain_hbm,
    wq_hbm,
    wf_hbm,
    wi_hbm,
    wg_hbm,
    bound_hbm,
    head_gain_hbm,
    state_hbm,
    wout_hbm,
    wup_hbm,
    wdown_hbm,
    out_ref,
    next_v,
    tok_v,
    gain_v,
    w4_v,
    bound_v,
    head_gain_v,
    state_v,
    wout_v,
    wup_v,
    wdown_v,
    gains,
    w_first,
    w_up,
    w_down,
    w_out,
    tok_all,
    sq1,
    proj_out,
    proj_in,
    mix_own,
    mix_all,
    mixed_all,
    sq2,
    up_out,
    up_in,
    hidden_all,
    down_out,
    down_in,
    read_v,
    in_sems,
    send_sems,
    recv_sems,
    hidden_sems,
    far_sem,
):
    kv, t = lax.axis_index("kv"), lax.axis_index("tp")
    z, x = kv // NX, kv % NX
    y, core = t // 2, t % 2
    has_self = t == z

    xs = [(x + d) % 4 for d in range(4)]
    ys = [(y + d) % 4 for d in range(4)]
    zs = [(z + d) % 8 for d in range(8)]
    cores = [core, 1 - core]
    kvs = [[pz * NX + px for px in xs] for pz in zs]
    ts = [[2 * py + pc for pc in cores] for py in ys]

    def copy_to(src, dst, k, pkv, pt, arrived=None):
        return pltpu.make_async_remote_copy(
            src_ref=src,
            dst_ref=dst,
            send_sem=send_sems.at[k],
            recv_sem=recv_sems.at[k] if arrived is None else arrived,
            device_id=(pkv, pt),
            device_id_type=MESH,
        )

    leaving, mix_sent = [], []

    def finish():
        for ref, k in leaving:
            wait_for(ref, send_sems.at[k])
        if mix_sent:
            @pl.when(has_self)
            def _():
                wait_for(mix_all.at[pl.ds(0, 31)], send_sems.at[8])

            @pl.when(jnp.logical_not(has_self))
            def _():
                wait_for(mix_all, send_sems.at[8])

    barrier = pltpu.get_barrier_semaphore()

    def tell(pkv, pt):
        pl.semaphore_signal(barrier, inc=1, device_id=(pkv, pt), device_id_type=MESH)

    for dx, dy, dc in PLANE:
        tell(kvs[0][dx], ts[dy][dc])
    for dz in (2, 6, 1, 7):
        for dx in (2, 1, 3, 0):
            tell(kvs[dz][dx], t)

    loads = [
        pltpu.make_async_copy(tokens_hbm, tok_v, in_sems.at[0]),
        pltpu.make_async_copy(norm_gain_hbm, gain_v.at[0], in_sems.at[1]),
        pltpu.make_async_copy(wq_hbm, w4_v.at[0], in_sems.at[2]),
        pltpu.make_async_copy(wf_hbm, w4_v.at[1], in_sems.at[3]),
        pltpu.make_async_copy(wi_hbm, w4_v.at[2], in_sems.at[4]),
        pltpu.make_async_copy(wg_hbm, w4_v.at[3], in_sems.at[5]),
        pltpu.make_async_copy(wout_hbm, wout_v, in_sems.at[6]),
        pltpu.make_async_copy(wup_hbm, wup_v, in_sems.at[7]),
        pltpu.make_async_copy(wdown_hbm, wdown_v, in_sems.at[8]),
        pltpu.make_async_copy(bound_hbm, bound_v, in_sems.at[9]),
        pltpu.make_async_copy(head_gain_hbm, head_gain_v, in_sems.at[10]),
        pltpu.make_async_copy(state_hbm, state_v, in_sems.at[11]),
        pltpu.make_async_copy(mixer_gain_hbm, gain_v.at[1], in_sems.at[12]),
    ]
    for load in loads:
        load.start()

    loads[0].wait()
    tok_f = tok_v[...].astype(F32)
    tok_all[x * NT + t] = jnp.concatenate([tok_f[0:24], tok_f[24:48]], axis=1).astype(BF16)
    loads[1].wait()
    loads[12].wait()
    for q in range(2):
        g = gain_v[q]
        gains[x, q : q + 1, :] = jnp.concatenate([g, g], axis=1)
    for k in range(2, 9):
        loads[k].wait()
    w_first[x] = w4_v[x]
    w_up[y, x] = wup_v[:, pl.ds(pl.multiple_of(x * 256, 256), 256)]
    w_out[t] = wout_v[...]
    w_down[y, x] = wdown_v[:, pl.ds(pl.multiple_of(x * 256, 256), 256)]

    pl.semaphore_wait(barrier, 31 + 16)
    for step in (2, 6):
        pl.semaphore_signal(
            far_sem, inc=1, device_id=(kvs[step][0], t), device_id_type=MESH
        )

    for (dx,) in ALONG_X:
        copy_to(gains.at[x], gains.at[x], 1, kvs[0][dx], t).start()
    own_tok = tok_all.at[x * NT + t]
    for dx, dy, dc in PLANE:
        copy_to(own_tok, own_tok, 0, kvs[0][dx], ts[dy][dc]).start()
    for (dx,) in ALONG_X:
        copy_to(w4_v.at[xs[dx]], w_first.at[x], 2, kvs[0][dx], t).start()
    leaving.append((tok_all.at[pl.ds(0, 31)], 0))
    leaving.append((gains.at[pl.ds(0, 3)], 1))
    leaving.append((w_first.at[pl.ds(0, 3)], 2))
    wait_for(gains.at[pl.ds(0, 3)], recv_sems.at[1])
    wait_for(tok_all.at[pl.ds(0, 31)], recv_sems.at[0])

    for dy, dc in ALONG_Y:
        copy_to(w_out.at[t], w_out.at[t], 3, kv, ts[dy][dc]).start()
    leaving.append((w_out.at[pl.ds(0, 7)], 3))

    for (dx,) in ALONG_X:
        cols = pl.ds(pl.multiple_of(xs[dx] * 256, 256), 256)
        copy_to(wup_v.at[:, cols], w_up.at[y, x], 6, kvs[0][dx], t).start()
        copy_to(wdown_v.at[:, cols], w_down.at[y, x], 7, kvs[0][dx], t).start()
    leaving.append((w_first.at[pl.ds(0, 3)], 6))
    leaving.append((w_first.at[pl.ds(0, 3)], 7))

    raw = [
        tok_all[pl.ds(NT * q, NT)].astype(F32).reshape(192, 128) for q in range(NX)
    ]
    sq1[z] = row_squares(raw)
    lhs = unpacked([raw[q] * gains[q, 0:1, :] for q in range(NX)])
    wait_for(w_first.at[pl.ds(0, 3)], recv_sems.at[2])
    partial = jnp.dot(lhs, w_first[...].reshape(256, 256), preferred_element_type=F32)

    for half in range(2):
        for pz in range(NZ):
            at = half * 192 + pz * 24
            left = partial[at : at + 24, 0:128]
            right = partial[at : at + 24, 128:256]
            proj_out[pz * NX + 2 * half] = jnp.concatenate(
                [left[0:12], right[0:12]], axis=0
            ).astype(BF16)
            proj_out[pz * NX + 2 * half + 1] = jnp.concatenate(
                [left[12:24], right[12:24]], axis=0
            ).astype(BF16)

    pl.semaphore_wait(far_sem, 2)

    for (dz,) in ALONG_Z:
        copy_to(sq1.at[z], sq1.at[z], 4, kvs[dz][0], t).start()
    for dz, dx in COLUMN:
        copy_to(proj_out.at[kvs[dz][dx]], proj_in.at[kv], 5, kvs[dz][dx], t).start()
    proj_in[kv] = proj_out[kv]
    leaving.append((sq1.at[pl.ds(0, 7)], 4))
    leaving.append((proj_in.at[pl.ds(0, 31)], 5))

    wait_for(w_first.at[pl.ds(0, 3)], recv_sems.at[6])
    for (dy,) in ALONG_X:
        copy_to(w_up.at[y], w_up.at[y], 14, kv, ts[dy][0]).start()
    leaving.append((w_up.at[pl.ds(0, 3)], 14))

    for k in range(9, 12):
        loads[k].wait()
    wait_for(sq1.at[pl.ds(0, 7)], recv_sems.at[4])
    wait_for(proj_in.at[pl.ds(0, 31)], recv_sems.at[5])

    squares = sq1[0]
    for q in range(1, NZ):
        squares = squares + sq1[q]
    square_row = jnp.where(x // 2 == 0, squares[0:1, :], squares[1:2, :])
    row_scale = lax.rsqrt(
        column_of(square_row, z * 24 + (x % 2) * 12, 12) / WIDTH + NORM_EPS
    )
    owned = []
    for q in range(NX):
        total = proj_in[q].astype(F32)
        for r in range(1, NZ):
            total = total + proj_in[r * NX + q].astype(F32)
        owned.append(total * row_scale)
    queries, forget_raw, values_in, gate_raw = owned
    head0 = lax.broadcasted_iota(jnp.int32, (24, 128), 0) < 12
    bound = jnp.where(head0, bound_v[0:1, :], bound_v[1:2, :])
    head_gain = jnp.where(head0, head_gain_v[0:1, :], head_gain_v[1:2, :])
    forget = bound + (1.0 - bound) * jax.nn.sigmoid(forget_raw)
    pad = jnp.zeros((104, 128), F32)
    kept = queries * forget
    kept_t = jnp.concatenate([kept, pad], axis=0).T
    fresh = jnp.sum(queries * (1.0 - forget), axis=1, keepdims=True) * values_in
    for j in range(24):
        read_v[j : j + 1, :] = jnp.sum(
            kept_t[:, j : j + 1] * state_v[j % 12, j // 12], axis=0, keepdims=True
        )
    read = read_v[...] + fresh
    read = read * lax.rsqrt(jnp.mean(read * read, axis=1, keepdims=True) + NORM_EPS) * head_gain
    mix_own[...] = (read * jax.nn.silu(gate_raw)).astype(BF16)

    mix_at = t * NX + x
    for dz, dx in COLUMN:
        copy_to(mix_own, mix_all.at[mix_at], 8, kvs[dz][dx], z).start()

    @pl.when(jnp.logical_not(has_self))
    def _():
        copy_to(mix_own, mix_all.at[mix_at], 8, kv, z).start()

    @pl.when(has_self)
    def _():
        mix_all[mix_at] = mix_own[...]

    mix_sent.append(1)
    forget_t = jnp.concatenate([forget, pad], axis=0).T
    for j in range(24):
        f = forget_t[:, j : j + 1]
        next_v[j % 12, j // 12] = f * state_v[j % 12, j // 12] + (1.0 - f) * values_in[j : j + 1, :]
    wait_for(w_out.at[pl.ds(0, 7)], recv_sems.at[3])

    @pl.when(has_self)
    def _():
        wait_for(mix_all.at[pl.ds(0, 31)], recv_sems.at[8])

    @pl.when(jnp.logical_not(has_self))
    def _():
        wait_for(mix_all, recv_sems.at[8])

    acc = jnp.zeros((96, 128), F32)
    for q in range(NT):
        both = jnp.concatenate([w_out[q, :, 0:128], w_out[q, :, 128:256]], axis=0)
        acc = acc + dot_t(mix_all[4 * q : 4 * q + 4].reshape(96, 128), both)
    folded = []
    for q in range(NX):
        part = acc[24 * q : 24 * q + 24]
        turned = swap_lanes(jnp.concatenate([part[12:24], part[0:12]], axis=0))
        folded.append(part + turned)
    low = low_lanes((24, 128))
    top = jnp.where(low, folded[0], swap_lanes(folded[2]))
    bottom = jnp.where(low, swap_lanes(folded[1]), folded[3])
    attn = jnp.where(head0, top, bottom)
    own_at = 2 * x + core
    mixed_all[own_at] = (tok_all[x * NT + t].astype(F32) + attn).astype(BF16)

    own_mixed = mixed_all.at[own_at]
    for dx, dc in ROW:
        copy_to(own_mixed, own_mixed, 9, kvs[0][dx], ts[0][dc]).start()
    leaving.append((mixed_all.at[pl.ds(0, 7)], 9))

    wait_for(w_first.at[pl.ds(0, 3)], recv_sems.at[7])
    for (dy,) in ALONG_X:
        copy_to(w_down.at[y], w_down.at[y], 15, kv, ts[dy][0]).start()
    leaving.append((w_down.at[pl.ds(0, 3)], 15))
    wait_for(w_up.at[pl.ds(0, 3)], recv_sems.at[14])
    wait_for(mixed_all.at[pl.ds(0, 7)], recv_sems.at[9])
    raw2 = [mixed_all[2 * q : 2 * q + 2].astype(F32).reshape(48, 128) for q in range(NX)]
    sq2[z] = row_squares(raw2)
    lhs2 = unpacked([raw2[q] * gains[q, 1:2, :] for q in range(NX)])
    for q in range(4):
        partial2 = jnp.dot(lhs2, w_up[q].reshape(256, 256), preferred_element_type=F32)
        up_out[2 * q] = partial2[:, 0:128].astype(BF16)
        up_out[2 * q + 1] = partial2[:, 128:256].astype(BF16)
    for (dz,) in ALONG_Z:
        copy_to(up_out.at[zs[dz]], up_in.at[z], 11, kvs[dz][0], t).start()
        copy_to(sq2.at[z], sq2.at[z], 10, kvs[dz][0], t).start()
    up_in[z] = up_out[z]
    leaving.append((sq2.at[pl.ds(0, 7)], 10))
    leaving.append((up_in.at[pl.ds(0, 7)], 11))
    wait_for(sq2.at[pl.ds(0, 7)], recv_sems.at[10])
    squares2 = sq2[0]
    for q in range(1, NZ):
        squares2 = squares2 + sq2[q]
    scale2 = jnp.concatenate(
        [
            lax.rsqrt(column_of(squares2[q : q + 1, :], 0, 48, 48) / WIDTH + NORM_EPS)
            for q in range(2)
        ],
        axis=0,
    )
    wait_for(up_in.at[pl.ds(0, 7)], recv_sems.at[11])

    total = up_in[0].astype(F32)
    for q in range(1, NZ):
        total = total + up_in[q].astype(F32)
    total = jnp.maximum(total * scale2, 0.0)
    hidden_all[z] = (total * total).astype(BF16)
    own_hidden = hidden_all.at[z]
    for (dz,) in ALONG_Z:
        copy_to(own_hidden, own_hidden, 12, kvs[dz][0], t, hidden_sems.at[z]).start()
    leaving.append((hidden_all.at[pl.ds(0, 7)], 12))
    wait_for(w_down.at[pl.ds(0, 3)], recv_sems.at[15])

    partial3 = jnp.zeros((96, 256), F32)
    for dz in NEAR_Z:
        pz = zs[dz]
        if dz:
            wait_for(hidden_all.at[pz], hidden_sems.at[pz])
        units = pl.ds(pl.multiple_of((pz % 2) * 128, 128), 128)
        partial3 = partial3 + dot_t(hidden_all[pz], w_down[pz // 2, :, :, units].reshape(256, 128))
    for half in range(2):
        for pair in range(2):
            upper = partial3[24 * half : 24 * half + 24, 128 * pair : 128 * pair + 128]
            lower = partial3[48 + 24 * half : 72 + 24 * half, 128 * pair : 128 * pair + 128]
            down_out[4 * pair + half] = jnp.where(low, upper, swap_lanes(lower)).astype(BF16)
            down_out[4 * pair + 2 + half] = jnp.where(low, swap_lanes(upper), lower).astype(BF16)
    for dx, dc in ROW:
        copy_to(
            down_out.at[2 * xs[dx] + cores[dc]], down_in.at[own_at], 13, kvs[0][dx], ts[0][dc]
        ).start()
    down_in[own_at] = down_out[own_at]
    leaving.append((down_in.at[pl.ds(0, 7)], 13))
    wait_for(down_in.at[pl.ds(0, 7)], recv_sems.at[13])
    total = down_in[0].astype(F32)
    for q in range(1, 8):
        total = total + down_in[q].astype(F32)
    total = mixed_all[own_at].astype(F32) + total
    out_ref[...] = jnp.concatenate([total[:, 0:64], total[:, 64:128]], axis=0).astype(BF16)

    finish()


def place(out_v, next_v, out_hbm, next_hbm, sems):
    copies = [
        pltpu.make_async_copy(
            next_v.at[pl.ds(2 * q, 2)], next_hbm.at[pl.ds(2 * q, 2)], sems.at[q]
        )
        for q in range(6)
    ]
    copies.append(pltpu.make_async_copy(out_v, out_hbm, sems.at[6]))
    for copy in copies:
        copy.start()
    for copy in copies:
        copy.wait()


def body(
    tokens,
    norm_gain,
    w_query,
    w_forget,
    w_input,
    w_gate,
    lower_bound,
    head_gain,
    recur_state,
    w_out,
    mixer_gain,
    w_up,
    w_down,
):
    bound = lower_bound.reshape(2, 128)
    any_spec = pl.BlockSpec(memory_space=pltpu.HBM)
    vmem_spec = pl.BlockSpec(memory_space=pltpu.VMEM)
    out, next_state = pl.pallas_call(
        kernel,
        out_shape=(
            jax.ShapeDtypeStruct(tokens.shape, tokens.dtype),
            jax.ShapeDtypeStruct(recur_state.shape, recur_state.dtype),
        ),
        in_specs=[any_spec] * 13,
        out_specs=(vmem_spec, vmem_spec),
        scratch_shapes=[
            pltpu.VMEM((48, 64), BF16),
            pltpu.VMEM((2, 1, 64), F32),
            pltpu.VMEM((4, 64, 256), BF16),
            pltpu.VMEM((2, 128), F32),
            pltpu.VMEM((2, 128), F32),
            pltpu.VMEM((12, 2, 128, 128), F32),
            pltpu.VMEM((64, 256), BF16),
            pltpu.VMEM((64, 1024), BF16),
            pltpu.VMEM((64, 1024), BF16),
            pltpu.VMEM((4, 2, 128), F32),
            pltpu.VMEM((4, 64, 256), BF16),
            pltpu.VMEM((4, 4, 64, 256), BF16),
            pltpu.VMEM((4, 4, 64, 256), BF16),
            pltpu.VMEM((8, 64, 256), BF16),
            pltpu.VMEM((32, 24, 128), BF16),
            pltpu.VMEM((8, 2, 256), F32),
            pltpu.VMEM((32, 24, 128), BF16),
            pltpu.VMEM((32, 24, 128), BF16),
            pltpu.VMEM((24, 128), BF16),
            pltpu.VMEM((32, 24, 128), BF16),
            pltpu.VMEM((8, 24, 128), BF16),
            pltpu.VMEM((8, 2, 128), F32),
            pltpu.VMEM((8, 96, 128), BF16),
            pltpu.VMEM((8, 96, 128), BF16),
            pltpu.VMEM((8, 96, 128), BF16),
            pltpu.VMEM((8, 24, 128), BF16),
            pltpu.VMEM((8, 24, 128), BF16),
            pltpu.VMEM((24, 128), F32),
            pltpu.SemaphoreType.DMA((13,)),
            pltpu.SemaphoreType.DMA((16,)),
            pltpu.SemaphoreType.DMA((16,)),
            pltpu.SemaphoreType.DMA((8,)),
            pltpu.SemaphoreType.REGULAR,
        ],
        compiler_params=pltpu.CompilerParams(collective_id=0, has_side_effects=True, vmem_limit_bytes=16 * 1024 * 1024),
        name="decode_layer",
    )(*(pltpu.with_memory_space_constraint(a, pltpu.HBM) for a in (
        tokens,
        norm_gain.reshape(1, 64),
        mixer_gain.reshape(1, 64),
        w_query,
        w_forget,
        w_input,
        w_gate,
        bound,
        head_gain,
        recur_state,
        w_out.T,
        w_up,
        w_down.T,
    )))
    return pl.pallas_call(
        place,
        out_shape=(
            jax.ShapeDtypeStruct(out.shape, out.dtype),
            jax.ShapeDtypeStruct(next_state.shape, next_state.dtype),
        ),
        in_specs=[vmem_spec, vmem_spec],
        out_specs=(any_spec, any_spec),
        scratch_shapes=[pltpu.SemaphoreType.DMA((7,))],
        compiler_params=pltpu.CompilerParams(vmem_limit_bytes=4 * 1024 * 1024),
        name="place_outputs",
    )(out, next_state)


def solution(mesh):
    in_specs = (
        P("tp", "kv"),
        P("kv"),
        P("kv", "tp"),
        P("kv", "tp"),
        P("kv", "tp"),
        P("kv", "tp"),
        P("tp"),
        P("tp", None),
        P("kv", "tp", None, None),
        P("tp", "kv"),
        P("kv"),
        P("kv", "tp"),
        P("tp", "kv"),
    )
    out_specs = (P("tp", "kv"), P("kv", "tp", None, None))
    return jax.shard_map(body, mesh=mesh, in_specs=in_specs, out_specs=out_specs, check_vma=False)
```

```python
import itertools

import jax
import jax.numpy as jnp
from jax import lax
from jax.experimental import pallas as pl
from jax.experimental.pallas import tpu as pltpu
from jax.sharding import PartitionSpec as P

NORM_EPS = 1e-05
MESH = pl.DeviceIdType.MESH
F32 = jnp.float32
BF16 = jnp.bfloat16

NZ, NX, NT = 8, 4, 8
WIDTH = 2048.0


def hops(step, size):
    return min(step, size - step)


def by_distance(sizes):
    steps = list(itertools.product(*(range(n) for n in sizes)))[1:]
    return sorted(steps, key=lambda d: (-sum(hops(s, n) for s, n in zip(d, sizes)), d))


PLANE = by_distance((4, 4, 2))
COLUMN = by_distance((8, 4))
ALONG_X = by_distance((4,))
ALONG_Y = by_distance((4, 2))
PAIR = by_distance((2, 4))
ROW = by_distance((2, 4, 2))
ALONG_Z = by_distance((8,))
NEAR_Z = [0, 1, 7, 2, 6, 3, 5, 4]


def wait_for(ref, sem):
    pltpu.make_async_copy(ref, ref, sem).wait()


def swap_lanes(value):
    return pltpu.roll(value, 64, 1)


def dot_t(a, b):
    return lax.dot_general(a, b, (((1,), (1,)), ((), ())), preferred_element_type=F32)


def low_lanes(shape):
    return lax.broadcasted_iota(jnp.int32, shape, 1) < 64


def unpacked(pieces):
    low = low_lanes(pieces[0].shape)
    swapped = [swap_lanes(p) for p in pieces]
    first = [jnp.where(low, pieces[i], swapped[i + 1]).astype(BF16) for i in range(0, len(pieces), 2)]
    second = [jnp.where(low, swapped[i], pieces[i + 1]).astype(BF16) for i in range(0, len(pieces), 2)]
    return jnp.concatenate(
        [jnp.concatenate(first, axis=1), jnp.concatenate(second, axis=1)], axis=0
    )


def row_squares(pieces):
    total = pieces[0] * pieces[0]
    for p in pieces[1:]:
        total = total + p * p
    spare = -total.shape[0] % 128
    total = jnp.concatenate([total, jnp.zeros((spare, 128), F32)], axis=0)
    high = total.astype(BF16)
    rest = (total - high.astype(F32)).astype(BF16)
    lane = lax.broadcasted_iota(jnp.int32, (8, 128), 1)
    row = lax.broadcasted_iota(jnp.int32, (8, 128), 0)
    pick = jnp.where((lane // 64) == row, 1.0, 0.0).astype(BF16)
    dims = (((1,), (1,)), ((), ()))
    sums = lax.dot_general(pick, high, dims, preferred_element_type=F32)
    sums = sums + lax.dot_general(pick, rest, dims, preferred_element_type=F32)
    return sums[0:2, :]


def column_of(values, base, period, rows=24):
    shape = (rows, values.shape[1])
    lane = lax.broadcasted_iota(jnp.int32, shape, 1)
    row = lax.broadcasted_iota(jnp.int32, shape, 0)
    return jnp.sum(
        jnp.where(lane == base + row % period, values, 0.0), axis=1, keepdims=True
    )


def kernel(
    tokens_hbm,
    norm_gain_hbm,
    mixer_gain_hbm,
    wq_hbm,
    wf_hbm,
    wi_hbm,
    wg_hbm,
    bound_hbm,
    head_gain_hbm,
    state_hbm,
    wout_hbm,
    wup_hbm,
    wdown_hbm,
    out_ref,
    next_v,
    tok_v,
    gain_v,
    w4_v,
    bound_v,
    head_gain_v,
    state_v,
    wout_v,
    wup_v,
    wdown_v,
    gains,
    w_first,
    w_up,
    w_down,
    w_out,
    tok_all,
    sq1,
    proj_out,
    proj_in,
    mix_own,
    mix_all,
    mixed_all,
    sq2,
    up_out,
    up_in,
    hidden_all,
    down_out,
    down_in,
    read_v,
    in_sems,
    send_sems,
    recv_sems,
    hidden_sems,
    far_sem,
):
    kv, t = lax.axis_index("kv"), lax.axis_index("tp")
    z, x = kv // NX, kv % NX
    y, core = t // 2, t % 2
    has_self = t == z

    xs = [(x + d) % 4 for d in range(4)]
    ys = [(y + d) % 4 for d in range(4)]
    zs = [(z + d) % 8 for d in range(8)]
    cores = [core, 1 - core]
    kvs = [[pz * NX + px for px in xs] for pz in zs]
    ts = [[2 * py + pc for pc in cores] for py in ys]

    def copy_to(src, dst, k, pkv, pt, arrived=None):
        return pltpu.make_async_remote_copy(
            src_ref=src,
            dst_ref=dst,
            send_sem=send_sems.at[k],
            recv_sem=recv_sems.at[k] if arrived is None else arrived,
            device_id=(pkv, pt),
            device_id_type=MESH,
        )

    leaving, mix_sent = [], []

    def finish():
        for ref, k in leaving:
            wait_for(ref, send_sems.at[k])
        if mix_sent:
            @pl.when(has_self)
            def _():
                wait_for(mix_all.at[pl.ds(0, 31)], send_sems.at[8])

            @pl.when(jnp.logical_not(has_self))
            def _():
                wait_for(mix_all, send_sems.at[8])

    pair, odd = z // 2, z % 2
    pair_kvs = [kvs[0], [(z + 1 - 2 * odd) * NX + px for px in xs]]
    pair_odd = [odd, 1 - odd]
    in_pair = odd * NX + x

    barrier = pltpu.get_barrier_semaphore()

    def tell(pkv, pt):
        pl.semaphore_signal(barrier, inc=1, device_id=(pkv, pt), device_id_type=MESH)

    for dx, dy, dc in PLANE:
        tell(kvs[0][dx], ts[dy][dc])
    for dz in (2, 6, 1, 7):
        for dx in (2, 1, 3, 0):
            tell(kvs[dz][dx], t)

    loads = [
        pltpu.make_async_copy(tokens_hbm, tok_v, in_sems.at[0]),
        pltpu.make_async_copy(norm_gain_hbm, gain_v.at[0], in_sems.at[1]),
        pltpu.make_async_copy(wq_hbm, w4_v.at[0], in_sems.at[2]),
        pltpu.make_async_copy(wf_hbm, w4_v.at[1], in_sems.at[3]),
        pltpu.make_async_copy(wi_hbm, w4_v.at[2], in_sems.at[4]),
        pltpu.make_async_copy(wg_hbm, w4_v.at[3], in_sems.at[5]),
        pltpu.make_async_copy(wout_hbm, wout_v, in_sems.at[6]),
        pltpu.make_async_copy(wup_hbm, wup_v, in_sems.at[7]),
        pltpu.make_async_copy(wdown_hbm, wdown_v, in_sems.at[8]),
        pltpu.make_async_copy(bound_hbm, bound_v, in_sems.at[9]),
        pltpu.make_async_copy(head_gain_hbm, head_gain_v, in_sems.at[10]),
        pltpu.make_async_copy(state_hbm, state_v, in_sems.at[11]),
        pltpu.make_async_copy(mixer_gain_hbm, gain_v.at[1], in_sems.at[12]),
    ]
    for load in loads:
        load.start()

    def units_of(px, p):
        return pl.ds(pl.multiple_of(px * 256 + p * 128, 128), 128)

    loads[0].wait()
    tok_f = tok_v[...].astype(F32)
    tok_all[x * NT + t] = jnp.concatenate([tok_f[0:24], tok_f[24:48]], axis=1).astype(BF16)
    loads[1].wait()
    loads[12].wait()
    for q in range(2):
        g = gain_v[q]
        gains[in_pair, q : q + 1, :] = jnp.concatenate([g, g], axis=1)
    for k in range(2, 9):
        loads[k].wait()
    w_first[x] = w4_v[x]
    w_up[y, in_pair] = wup_v[:, units_of(x, odd)]
    w_out[t] = wout_v[...]
    w_down[y, in_pair] = wdown_v[:, units_of(x, odd)]

    pl.semaphore_wait(barrier, 31 + 16)
    for step in (2, 6):
        pl.semaphore_signal(
            far_sem, inc=1, device_id=(kvs[step][0], t), device_id_type=MESH
        )

    for dp, dx in PAIR:
        copy_to(gains.at[in_pair], gains.at[in_pair], 1, pair_kvs[dp][dx], t).start()
    own_tok = tok_all.at[x * NT + t]
    for dx, dy, dc in PLANE:
        copy_to(own_tok, own_tok, 0, kvs[0][dx], ts[dy][dc]).start()
    for (dx,) in ALONG_X:
        copy_to(w4_v.at[xs[dx]], w_first.at[x], 2, kvs[0][dx], t).start()
    leaving.append((tok_all.at[pl.ds(0, 31)], 0))
    leaving.append((gains.at[pl.ds(0, 7)], 1))
    leaving.append((w_first.at[pl.ds(0, 3)], 2))
    wait_for(gains.at[pl.ds(0, 7)], recv_sems.at[1])
    wait_for(tok_all.at[pl.ds(0, 31)], recv_sems.at[0])

    for dy, dc in ALONG_Y:
        copy_to(w_out.at[t], w_out.at[t], 3, kv, ts[dy][dc]).start()
    leaving.append((w_out.at[pl.ds(0, 7)], 3))

    for dp, dx in PAIR:
        cols = units_of(xs[dx], pair_odd[dp])
        copy_to(wup_v.at[:, cols], w_up.at[y, in_pair], 6, pair_kvs[dp][dx], t).start()
        copy_to(wdown_v.at[:, cols], w_down.at[y, in_pair], 7, pair_kvs[dp][dx], t).start()
    leaving.append((w_up.at[0, pl.ds(0, 7)], 6))
    leaving.append((w_up.at[0, pl.ds(0, 7)], 7))

    raw = [
        tok_all[pl.ds(NT * q, NT)].astype(F32).reshape(192, 128) for q in range(NX)
    ]
    sq1[z] = row_squares(raw)
    lhs = unpacked([raw[q] * gains[odd * NX + q, 0:1, :] for q in range(NX)])
    wait_for(w_first.at[pl.ds(0, 3)], recv_sems.at[2])
    partial = jnp.dot(lhs, w_first[...].reshape(256, 256), preferred_element_type=F32)

    for half in range(2):
        for pz in range(NZ):
            at = half * 192 + pz * 24
            left = partial[at : at + 24, 0:128]
            right = partial[at : at + 24, 128:256]
            proj_out[pz * NX + 2 * half] = jnp.concatenate(
                [left[0:12], right[0:12]], axis=0
            ).astype(BF16)
            proj_out[pz * NX + 2 * half + 1] = jnp.concatenate(
                [left[12:24], right[12:24]], axis=0
            ).astype(BF16)

    pl.semaphore_wait(far_sem, 2)

    for (dz,) in ALONG_Z:
        copy_to(sq1.at[z], sq1.at[z], 4, kvs[dz][0], t).start()
    for dz, dx in COLUMN:
        copy_to(proj_out.at[kvs[dz][dx]], proj_in.at[kv], 5, kvs[dz][dx], t).start()
    proj_in[kv] = proj_out[kv]
    leaving.append((sq1.at[pl.ds(0, 7)], 4))
    leaving.append((proj_in.at[pl.ds(0, 31)], 5))

    wait_for(w_up.at[0, pl.ds(0, 7)], recv_sems.at[6])
    for (dy,) in ALONG_X:
        copy_to(w_up.at[y], w_up.at[y], 14, kv, ts[dy][0]).start()
    leaving.append((w_up.at[pl.ds(0, 3)], 14))

    for k in range(9, 12):
        loads[k].wait()
    wait_for(sq1.at[pl.ds(0, 7)], recv_sems.at[4])
    wait_for(proj_in.at[pl.ds(0, 31)], recv_sems.at[5])

    squares = sq1[0]
    for q in range(1, NZ):
        squares = squares + sq1[q]
    square_row = jnp.where(x // 2 == 0, squares[0:1, :], squares[1:2, :])
    row_scale = lax.rsqrt(
        column_of(square_row, z * 24 + (x % 2) * 12, 12) / WIDTH + NORM_EPS
    )
    owned = []
    for q in range(NX):
        total = proj_in[q].astype(F32)
        for r in range(1, NZ):
            total = total + proj_in[r * NX + q].astype(F32)
        owned.append(total * row_scale)
    queries, forget_raw, values_in, gate_raw = owned
    head0 = lax.broadcasted_iota(jnp.int32, (24, 128), 0) < 12
    bound = jnp.where(head0, bound_v[0:1, :], bound_v[1:2, :])
    head_gain = jnp.where(head0, head_gain_v[0:1, :], head_gain_v[1:2, :])
    forget = bound + (1.0 - bound) * jax.nn.sigmoid(forget_raw)
    pad = jnp.zeros((104, 128), F32)
    kept = queries * forget
    kept_t = jnp.concatenate([kept, pad], axis=0).T
    fresh = jnp.sum(queries * (1.0 - forget), axis=1, keepdims=True) * values_in
    for j in range(24):
        read_v[j : j + 1, :] = jnp.sum(
            kept_t[:, j : j + 1] * state_v[j % 12, j // 12], axis=0, keepdims=True
        )
    read = read_v[...] + fresh
    read = read * lax.rsqrt(jnp.mean(read * read, axis=1, keepdims=True) + NORM_EPS) * head_gain
    mix_own[...] = (read * jax.nn.silu(gate_raw)).astype(BF16)

    mix_at = t * NX + x
    for dz, dx in COLUMN:
        copy_to(mix_own, mix_all.at[mix_at], 8, kvs[dz][dx], z).start()

    @pl.when(jnp.logical_not(has_self))
    def _():
        copy_to(mix_own, mix_all.at[mix_at], 8, kv, z).start()

    @pl.when(has_self)
    def _():
        mix_all[mix_at] = mix_own[...]

    mix_sent.append(1)
    forget_t = jnp.concatenate([forget, pad], axis=0).T
    for j in range(24):
        f = forget_t[:, j : j + 1]
        next_v[j % 12, j // 12] = f * state_v[j % 12, j // 12] + (1.0 - f) * values_in[j : j + 1, :]
    wait_for(w_out.at[pl.ds(0, 7)], recv_sems.at[3])

    @pl.when(has_self)
    def _():
        wait_for(mix_all.at[pl.ds(0, 31)], recv_sems.at[8])

    @pl.when(jnp.logical_not(has_self))
    def _():
        wait_for(mix_all, recv_sems.at[8])

    acc = jnp.zeros((96, 128), F32)
    for q in range(NT):
        both = jnp.concatenate([w_out[q, :, 0:128], w_out[q, :, 128:256]], axis=0)
        acc = acc + dot_t(mix_all[4 * q : 4 * q + 4].reshape(96, 128), both)
    folded = []
    for q in range(NX):
        part = acc[24 * q : 24 * q + 24]
        turned = swap_lanes(jnp.concatenate([part[12:24], part[0:12]], axis=0))
        folded.append(part + turned)
    low = low_lanes((24, 128))
    top = jnp.where(low, folded[0], swap_lanes(folded[2]))
    bottom = jnp.where(low, swap_lanes(folded[1]), folded[3])
    attn = jnp.where(head0, top, bottom)
    own_at = 2 * in_pair + core
    mixed_all[own_at] = (tok_all[x * NT + t].astype(F32) + attn).astype(BF16)

    own_mixed = mixed_all.at[own_at]
    for dp, dx, dc in ROW:
        copy_to(own_mixed, own_mixed, 9, pair_kvs[dp][dx], ts[0][dc]).start()
    leaving.append((mixed_all.at[pl.ds(0, 15)], 9))

    wait_for(w_up.at[0, pl.ds(0, 7)], recv_sems.at[7])
    for (dy,) in ALONG_X:
        copy_to(w_down.at[y], w_down.at[y], 15, kv, ts[dy][0]).start()
    leaving.append((w_down.at[pl.ds(0, 3)], 15))
    wait_for(w_up.at[pl.ds(0, 3)], recv_sems.at[14])
    wait_for(mixed_all.at[pl.ds(0, 15)], recv_sems.at[9])
    raw2 = [mixed_all[2 * q : 2 * q + 2].astype(F32).reshape(48, 128) for q in range(8)]
    sq2[pair] = row_squares(raw2)
    lhs2 = unpacked([raw2[q] * gains[q, 1:2, :] for q in range(8)])
    for q in range(4):
        up_out[q] = jnp.dot(
            lhs2, w_up[q].reshape(512, 128), preferred_element_type=F32
        ).astype(BF16)
    for dz in (4, 2, 6):
        copy_to(up_out.at[zs[dz] // 2], up_in.at[pair], 11, kvs[dz][0], t).start()
        copy_to(sq2.at[pair], sq2.at[pair], 10, kvs[dz][0], t).start()
    up_in[pair] = up_out[pair]
    leaving.append((sq2.at[pl.ds(0, 3)], 10))
    leaving.append((up_in.at[pl.ds(0, 3)], 11))
    wait_for(sq2.at[pl.ds(0, 3)], recv_sems.at[10])
    squares2 = sq2[0] + sq2[1] + sq2[2] + sq2[3]
    scale2 = jnp.concatenate(
        [
            lax.rsqrt(column_of(squares2[q : q + 1, :], 0, 48, 48) / WIDTH + NORM_EPS)
            for q in range(2)
        ],
        axis=0,
    )
    wait_for(up_in.at[pl.ds(0, 3)], recv_sems.at[11])

    total = up_in[0].astype(F32)
    for q in range(1, 4):
        total = total + up_in[q].astype(F32)
    total = jnp.maximum(total * scale2, 0.0)
    hidden_all[pair] = (total * total).astype(BF16)
    own_hidden = hidden_all.at[pair]
    for dz in (4, 2, 6):
        copy_to(own_hidden, own_hidden, 12, kvs[dz][0], t, hidden_sems.at[pair]).start()
    leaving.append((hidden_all.at[pl.ds(0, 3)], 12))
    wait_for(w_down.at[pl.ds(0, 3)], recv_sems.at[15])

    partial3 = jnp.zeros((96, 512), F32)
    for dz in (0, 2, 6, 4):
        pq = zs[dz] // 2
        if dz:
            wait_for(hidden_all.at[pq], hidden_sems.at[pq])
        partial3 = partial3 + dot_t(hidden_all[pq], w_down[pq].reshape(512, 128))
    for half in range(2):
        for two in range(4):
            upper = partial3[24 * half : 24 * half + 24, 128 * two : 128 * two + 128]
            lower = partial3[48 + 24 * half : 72 + 24 * half, 128 * two : 128 * two + 128]
            down_out[4 * two + half] = jnp.where(low, upper, swap_lanes(lower)).astype(BF16)
            down_out[4 * two + 2 + half] = jnp.where(low, swap_lanes(upper), lower).astype(BF16)
    for dp, dx, dc in ROW:
        copy_to(
            down_out.at[2 * (pair_odd[dp] * NX + xs[dx]) + cores[dc]],
            down_in.at[own_at],
            13,
            pair_kvs[dp][dx],
            ts[0][dc],
        ).start()
    down_in[own_at] = down_out[own_at]
    leaving.append((down_in.at[pl.ds(0, 15)], 13))
    wait_for(down_in.at[pl.ds(0, 15)], recv_sems.at[13])
    total = down_in[0].astype(F32)
    for q in range(1, 16):
        total = total + down_in[q].astype(F32)
    total = mixed_all[own_at].astype(F32) + total
    out_ref[...] = jnp.concatenate([total[:, 0:64], total[:, 64:128]], axis=0).astype(BF16)

    finish()


def place(out_v, next_v, out_hbm, next_hbm, sems):
    copies = [
        pltpu.make_async_copy(
            next_v.at[pl.ds(2 * q, 2)], next_hbm.at[pl.ds(2 * q, 2)], sems.at[q]
        )
        for q in range(6)
    ]
    copies.append(pltpu.make_async_copy(out_v, out_hbm, sems.at[6]))
    for copy in copies:
        copy.start()
    for copy in copies:
        copy.wait()


def body(
    tokens,
    norm_gain,
    w_query,
    w_forget,
    w_input,
    w_gate,
    lower_bound,
    head_gain,
    recur_state,
    w_out,
    mixer_gain,
    w_up,
    w_down,
):
    bound = lower_bound.reshape(2, 128)
    any_spec = pl.BlockSpec(memory_space=pltpu.HBM)
    vmem_spec = pl.BlockSpec(memory_space=pltpu.VMEM)
    out, next_state = pl.pallas_call(
        kernel,
        out_shape=(
            jax.ShapeDtypeStruct(tokens.shape, tokens.dtype),
            jax.ShapeDtypeStruct(recur_state.shape, recur_state.dtype),
        ),
        in_specs=[any_spec] * 13,
        out_specs=(vmem_spec, vmem_spec),
        scratch_shapes=[
            pltpu.VMEM((48, 64), BF16),
            pltpu.VMEM((2, 1, 64), F32),
            pltpu.VMEM((4, 64, 256), BF16),
            pltpu.VMEM((2, 128), F32),
            pltpu.VMEM((2, 128), F32),
            pltpu.VMEM((12, 2, 128, 128), F32),
            pltpu.VMEM((64, 256), BF16),
            pltpu.VMEM((64, 1024), BF16),
            pltpu.VMEM((64, 1024), BF16),
            pltpu.VMEM((8, 2, 128), F32),
            pltpu.VMEM((4, 64, 256), BF16),
            pltpu.VMEM((4, 8, 64, 128), BF16),
            pltpu.VMEM((4, 8, 64, 128), BF16),
            pltpu.VMEM((8, 64, 256), BF16),
            pltpu.VMEM((32, 24, 128), BF16),
            pltpu.VMEM((8, 2, 256), F32),
            pltpu.VMEM((32, 24, 128), BF16),
            pltpu.VMEM((32, 24, 128), BF16),
            pltpu.VMEM((24, 128), BF16),
            pltpu.VMEM((32, 24, 128), BF16),
            pltpu.VMEM((16, 24, 128), BF16),
            pltpu.VMEM((4, 2, 128), F32),
            pltpu.VMEM((4, 96, 128), BF16),
            pltpu.VMEM((4, 96, 128), BF16),
            pltpu.VMEM((4, 96, 128), BF16),
            pltpu.VMEM((16, 24, 128), BF16),
            pltpu.VMEM((16, 24, 128), BF16),
            pltpu.VMEM((24, 128), F32),
            pltpu.SemaphoreType.DMA((13,)),
            pltpu.SemaphoreType.DMA((16,)),
            pltpu.SemaphoreType.DMA((16,)),
            pltpu.SemaphoreType.DMA((8,)),
            pltpu.SemaphoreType.REGULAR,
        ],
        compiler_params=pltpu.CompilerParams(collective_id=0, has_side_effects=True, vmem_limit_bytes=16 * 1024 * 1024),
        name="decode_layer",
    )(*(pltpu.with_memory_space_constraint(a, pltpu.HBM) for a in (
        tokens,
        norm_gain.reshape(1, 64),
        mixer_gain.reshape(1, 64),
        w_query,
        w_forget,
        w_input,
        w_gate,
        bound,
        head_gain,
        recur_state,
        w_out.T,
        w_up,
        w_down.T,
    )))
    return pl.pallas_call(
        place,
        out_shape=(
            jax.ShapeDtypeStruct(out.shape, out.dtype),
            jax.ShapeDtypeStruct(next_state.shape, next_state.dtype),
        ),
        in_specs=[vmem_spec, vmem_spec],
        out_specs=(any_spec, any_spec),
        scratch_shapes=[pltpu.SemaphoreType.DMA((7,))],
        compiler_params=pltpu.CompilerParams(vmem_limit_bytes=4 * 1024 * 1024),
        name="place_outputs",
    )(out, next_state)


def solution(mesh):
    in_specs = (
        P("tp", "kv"),
        P("kv"),
        P("kv", "tp"),
        P("kv", "tp"),
        P("kv", "tp"),
        P("kv", "tp"),
        P("tp"),
        P("tp", None),
        P("kv", "tp", None, None),
        P("tp", "kv"),
        P("kv"),
        P("kv", "tp"),
        P("tp", "kv"),
    )
    out_specs = (P("tp", "kv"), P("kv", "tp", None, None))
    return jax.shard_map(body, mesh=mesh, in_specs=in_specs, out_specs=out_specs, check_vma=False)
```

```python
import itertools

import jax
import jax.numpy as jnp
from jax import lax
from jax.experimental import pallas as pl
from jax.experimental.pallas import tpu as pltpu
from jax.sharding import PartitionSpec as P

NORM_EPS = 1e-05
MESH = pl.DeviceIdType.MESH
F32 = jnp.float32
BF16 = jnp.bfloat16

NZ, NX, NT = 8, 4, 8
WIDTH = 2048.0


def hops(step, size):
    return min(step, size - step)


def by_distance(sizes):
    steps = list(itertools.product(*(range(n) for n in sizes)))[1:]
    return sorted(steps, key=lambda d: (-sum(hops(s, n) for s, n in zip(d, sizes)), d))


PLANE = by_distance((4, 4, 2))
COLUMN = by_distance((8, 4))
ALONG_X = by_distance((4,))
ALONG_Y = by_distance((4, 2))
PAIR = by_distance((2, 4))
ROW = by_distance((2, 4, 2))
ALONG_Z = by_distance((8,))
NEAR_Z = [0, 1, 7, 2, 6, 3, 5, 4]


def wait_for(ref, sem):
    pltpu.make_async_copy(ref, ref, sem).wait()


def swap_lanes(value):
    return pltpu.roll(value, 64, 1)


def dot_t(a, b):
    return lax.dot_general(a, b, (((1,), (1,)), ((), ())), preferred_element_type=F32)


def low_lanes(shape):
    return lax.broadcasted_iota(jnp.int32, shape, 1) < 64


def unpacked(pieces):
    low = low_lanes(pieces[0].shape)
    swapped = [swap_lanes(p) for p in pieces]
    first = [jnp.where(low, pieces[i], swapped[i + 1]).astype(BF16) for i in range(0, len(pieces), 2)]
    second = [jnp.where(low, swapped[i], pieces[i + 1]).astype(BF16) for i in range(0, len(pieces), 2)]
    return jnp.concatenate(
        [jnp.concatenate(first, axis=1), jnp.concatenate(second, axis=1)], axis=0
    )


def row_squares(pieces):
    total = pieces[0] * pieces[0]
    for p in pieces[1:]:
        total = total + p * p
    spare = -total.shape[0] % 128
    total = jnp.concatenate([total, jnp.zeros((spare, 128), F32)], axis=0)
    high = total.astype(BF16)
    rest = (total - high.astype(F32)).astype(BF16)
    lane = lax.broadcasted_iota(jnp.int32, (8, 128), 1)
    row = lax.broadcasted_iota(jnp.int32, (8, 128), 0)
    pick = jnp.where((lane // 64) == row, 1.0, 0.0).astype(BF16)
    dims = (((1,), (1,)), ((), ()))
    sums = lax.dot_general(pick, high, dims, preferred_element_type=F32)
    sums = sums + lax.dot_general(pick, rest, dims, preferred_element_type=F32)
    return sums[0:2, :]


def column_of(values, base, period, rows=24):
    shape = (rows, values.shape[1])
    lane = lax.broadcasted_iota(jnp.int32, shape, 1)
    row = lax.broadcasted_iota(jnp.int32, shape, 0)
    return jnp.sum(
        jnp.where(lane == base + row % period, values, 0.0), axis=1, keepdims=True
    )


def kernel(
    tokens_hbm,
    norm_gain_hbm,
    mixer_gain_hbm,
    wq_hbm,
    wf_hbm,
    wi_hbm,
    wg_hbm,
    bound_hbm,
    head_gain_hbm,
    state_hbm,
    wout_hbm,
    wup_hbm,
    wdown_hbm,
    out_ref,
    next_v,
    tok_v,
    gain_v,
    w4_v,
    bound_v,
    head_gain_v,
    state_v,
    wout_v,
    wup_v,
    wdown_v,
    gains,
    w_first,
    w_up,
    w_down,
    w_out,
    tok_all,
    sq1,
    proj_out,
    proj_in,
    mix_own,
    mix_all,
    mixed_all,
    sq2,
    up_out,
    up_in,
    hidden_all,
    down_out,
    down_in,
    read_v,
    in_sems,
    send_sems,
    recv_sems,
    hidden_sems,
    far_sem,
):
    kv, t = lax.axis_index("kv"), lax.axis_index("tp")
    z, x = kv // NX, kv % NX
    y, core = t // 2, t % 2
    has_self = t == z

    xs = [(x + d) % 4 for d in range(4)]
    ys = [(y + d) % 4 for d in range(4)]
    zs = [(z + d) % 8 for d in range(8)]
    cores = [core, 1 - core]
    kvs = [[pz * NX + px for px in xs] for pz in zs]
    ts = [[2 * py + pc for pc in cores] for py in ys]

    def copy_to(src, dst, k, pkv, pt, arrived=None):
        return pltpu.make_async_remote_copy(
            src_ref=src,
            dst_ref=dst,
            send_sem=send_sems.at[k],
            recv_sem=recv_sems.at[k] if arrived is None else arrived,
            device_id=(pkv, pt),
            device_id_type=MESH,
        )

    leaving, mix_sent = [], []

    def finish():
        for ref, k in leaving:
            wait_for(ref, send_sems.at[k])
        if mix_sent:
            @pl.when(has_self)
            def _():
                wait_for(mix_all.at[pl.ds(0, 31)], send_sems.at[8])

            @pl.when(jnp.logical_not(has_self))
            def _():
                wait_for(mix_all, send_sems.at[8])

    pair, odd = z // 2, z % 2
    pair_kvs = [kvs[0], [(z + 1 - 2 * odd) * NX + px for px in xs]]
    pair_odd = [odd, 1 - odd]
    in_pair = odd * NX + x

    barrier = pltpu.get_barrier_semaphore()

    def tell(pkv, pt):
        pl.semaphore_signal(barrier, inc=1, device_id=(pkv, pt), device_id_type=MESH)

    for dx, dy, dc in PLANE:
        tell(kvs[0][dx], ts[dy][dc])
    for dz in (2, 6, 1, 7):
        for dx in (2, 1, 3, 0):
            tell(kvs[dz][dx], t)

    loads = [
        pltpu.make_async_copy(tokens_hbm, tok_v, in_sems.at[0]),
        pltpu.make_async_copy(norm_gain_hbm, gain_v.at[0], in_sems.at[1]),
        pltpu.make_async_copy(wq_hbm, w4_v.at[0], in_sems.at[2]),
        pltpu.make_async_copy(wf_hbm, w4_v.at[1], in_sems.at[3]),
        pltpu.make_async_copy(wi_hbm, w4_v.at[2], in_sems.at[4]),
        pltpu.make_async_copy(wg_hbm, w4_v.at[3], in_sems.at[5]),
        pltpu.make_async_copy(wout_hbm, wout_v, in_sems.at[6]),
        pltpu.make_async_copy(wup_hbm, wup_v, in_sems.at[7]),
        pltpu.make_async_copy(wdown_hbm, wdown_v, in_sems.at[8]),
        pltpu.make_async_copy(bound_hbm, bound_v, in_sems.at[9]),
        pltpu.make_async_copy(head_gain_hbm, head_gain_v, in_sems.at[10]),
        pltpu.make_async_copy(state_hbm, state_v, in_sems.at[11]),
        pltpu.make_async_copy(mixer_gain_hbm, gain_v.at[1], in_sems.at[12]),
    ]
    for load in loads:
        load.start()

    def units_of(px, p):
        return pl.ds(pl.multiple_of(px * 256 + p * 128, 128), 128)

    loads[0].wait()
    tok_f = tok_v[...].astype(F32)
    tok_all[x * NT + t] = jnp.concatenate([tok_f[0:24], tok_f[24:48]], axis=1).astype(BF16)
    loads[1].wait()
    loads[12].wait()
    for q in range(2):
        g = gain_v[q]
        gains[in_pair, q : q + 1, :] = jnp.concatenate([g, g], axis=1)
    for k in range(2, 9):
        loads[k].wait()
    w_first[x] = w4_v[x]
    w_up[y, in_pair] = wup_v[:, units_of(x, odd)]
    w_out[t] = wout_v[...]
    w_down[y, in_pair] = wdown_v[:, units_of(x, odd)]

    pl.semaphore_wait(barrier, 31 + 16)
    for step in (2, 6):
        pl.semaphore_signal(
            far_sem, inc=1, device_id=(kvs[step][0], t), device_id_type=MESH
        )

    for dp, dx in PAIR:
        copy_to(gains.at[in_pair], gains.at[in_pair], 1, pair_kvs[dp][dx], t).start()
    own_tok = tok_all.at[x * NT + t]
    for dx, dy, dc in PLANE:
        copy_to(own_tok, own_tok, 0, kvs[0][dx], ts[dy][dc]).start()
    for (dx,) in ALONG_X:
        copy_to(w4_v.at[xs[dx]], w_first.at[x], 2, kvs[0][dx], t).start()
    leaving.append((tok_all.at[pl.ds(0, 31)], 0))
    leaving.append((gains.at[pl.ds(0, 7)], 1))
    leaving.append((w_first.at[pl.ds(0, 3)], 2))
    wait_for(gains.at[pl.ds(0, 7)], recv_sems.at[1])
    wait_for(tok_all.at[pl.ds(0, 31)], recv_sems.at[0])

    for dy, dc in ALONG_Y:
        copy_to(w_out.at[t], w_out.at[t], 3, kv, ts[dy][dc]).start()
    leaving.append((w_out.at[pl.ds(0, 7)], 3))


    raw = [
        tok_all[pl.ds(NT * q, NT)].astype(F32).reshape(192, 128) for q in range(NX)
    ]
    sq1[z] = row_squares(raw)
    lhs = unpacked([raw[q] * gains[odd * NX + q, 0:1, :] for q in range(NX)])
    wait_for(w_first.at[pl.ds(0, 3)], recv_sems.at[2])
    partial = jnp.dot(lhs, w_first[...].reshape(256, 256), preferred_element_type=F32)

    for half in range(2):
        for pz in range(NZ):
            at = half * 192 + pz * 24
            left = partial[at : at + 24, 0:128]
            right = partial[at : at + 24, 128:256]
            proj_out[pz * NX + 2 * half] = jnp.concatenate(
                [left[0:12], right[0:12]], axis=0
            ).astype(BF16)
            proj_out[pz * NX + 2 * half + 1] = jnp.concatenate(
                [left[12:24], right[12:24]], axis=0
            ).astype(BF16)

    pl.semaphore_wait(far_sem, 2)

    for (dz,) in ALONG_Z:
        copy_to(sq1.at[z], sq1.at[z], 4, kvs[dz][0], t).start()
    for dz, dx in COLUMN:
        copy_to(proj_out.at[kvs[dz][dx]], proj_in.at[kv], 5, kvs[dz][dx], t).start()
    proj_in[kv] = proj_out[kv]
    leaving.append((sq1.at[pl.ds(0, 7)], 4))
    leaving.append((proj_in.at[pl.ds(0, 31)], 5))
    for dp, dx in PAIR:
        cols = units_of(xs[dx], pair_odd[dp])
        copy_to(wup_v.at[:, cols], w_up.at[y, in_pair], 6, pair_kvs[dp][dx], t).start()
        copy_to(wdown_v.at[:, cols], w_down.at[y, in_pair], 7, pair_kvs[dp][dx], t).start()
    leaving.append((w_up.at[0, pl.ds(0, 7)], 6))
    leaving.append((w_up.at[0, pl.ds(0, 7)], 7))


    for k in range(9, 12):
        loads[k].wait()
    wait_for(sq1.at[pl.ds(0, 7)], recv_sems.at[4])
    wait_for(proj_in.at[pl.ds(0, 31)], recv_sems.at[5])

    squares = sq1[0]
    for q in range(1, NZ):
        squares = squares + sq1[q]
    square_row = jnp.where(x // 2 == 0, squares[0:1, :], squares[1:2, :])
    row_scale = lax.rsqrt(
        column_of(square_row, z * 24 + (x % 2) * 12, 12) / WIDTH + NORM_EPS
    )
    owned = []
    for q in range(NX):
        total = proj_in[q].astype(F32)
        for r in range(1, NZ):
            total = total + proj_in[r * NX + q].astype(F32)
        owned.append(total * row_scale)
    queries, forget_raw, values_in, gate_raw = owned
    head0 = lax.broadcasted_iota(jnp.int32, (24, 128), 0) < 12
    bound = jnp.where(head0, bound_v[0:1, :], bound_v[1:2, :])
    head_gain = jnp.where(head0, head_gain_v[0:1, :], head_gain_v[1:2, :])
    forget = bound + (1.0 - bound) * jax.nn.sigmoid(forget_raw)
    pad = jnp.zeros((104, 128), F32)
    kept = queries * forget
    kept_t = jnp.concatenate([kept, pad], axis=0).T
    fresh = jnp.sum(queries * (1.0 - forget), axis=1, keepdims=True) * values_in
    for j in range(24):
        read_v[j : j + 1, :] = jnp.sum(
            kept_t[:, j : j + 1] * state_v[j % 12, j // 12], axis=0, keepdims=True
        )
    read = read_v[...] + fresh
    read = read * lax.rsqrt(jnp.mean(read * read, axis=1, keepdims=True) + NORM_EPS) * head_gain
    mix_own[...] = (read * jax.nn.silu(gate_raw)).astype(BF16)

    mix_at = t * NX + x
    for dz, dx in COLUMN:
        copy_to(mix_own, mix_all.at[mix_at], 8, kvs[dz][dx], z).start()

    @pl.when(jnp.logical_not(has_self))
    def _():
        copy_to(mix_own, mix_all.at[mix_at], 8, kv, z).start()

    @pl.when(has_self)
    def _():
        mix_all[mix_at] = mix_own[...]

    wait_for(w_up.at[0, pl.ds(0, 7)], recv_sems.at[6])
    for (dy,) in ALONG_X:
        copy_to(w_up.at[y], w_up.at[y], 14, kv, ts[dy][0]).start()
    leaving.append((w_up.at[pl.ds(0, 3)], 14))
    mix_sent.append(1)
    forget_t = jnp.concatenate([forget, pad], axis=0).T
    for j in range(24):
        f = forget_t[:, j : j + 1]
        next_v[j % 12, j // 12] = f * state_v[j % 12, j // 12] + (1.0 - f) * values_in[j : j + 1, :]
    wait_for(w_out.at[pl.ds(0, 7)], recv_sems.at[3])

    @pl.when(has_self)
    def _():
        wait_for(mix_all.at[pl.ds(0, 31)], recv_sems.at[8])

    @pl.when(jnp.logical_not(has_self))
    def _():
        wait_for(mix_all, recv_sems.at[8])

    acc = jnp.zeros((96, 128), F32)
    for q in range(NT):
        both = jnp.concatenate([w_out[q, :, 0:128], w_out[q, :, 128:256]], axis=0)
        acc = acc + dot_t(mix_all[4 * q : 4 * q + 4].reshape(96, 128), both)
    folded = []
    for q in range(NX):
        part = acc[24 * q : 24 * q + 24]
        turned = swap_lanes(jnp.concatenate([part[12:24], part[0:12]], axis=0))
        folded.append(part + turned)
    low = low_lanes((24, 128))
    top = jnp.where(low, folded[0], swap_lanes(folded[2]))
    bottom = jnp.where(low, swap_lanes(folded[1]), folded[3])
    attn = jnp.where(head0, top, bottom)
    own_at = 2 * in_pair + core
    mixed_all[own_at] = (tok_all[x * NT + t].astype(F32) + attn).astype(BF16)

    own_mixed = mixed_all.at[own_at]
    for dp, dx, dc in ROW:
        copy_to(own_mixed, own_mixed, 9, pair_kvs[dp][dx], ts[0][dc]).start()
    leaving.append((mixed_all.at[pl.ds(0, 15)], 9))

    wait_for(w_up.at[0, pl.ds(0, 7)], recv_sems.at[7])
    for (dy,) in ALONG_X:
        copy_to(w_down.at[y], w_down.at[y], 15, kv, ts[dy][0]).start()
    leaving.append((w_down.at[pl.ds(0, 3)], 15))
    wait_for(w_up.at[pl.ds(0, 3)], recv_sems.at[14])
    wait_for(mixed_all.at[pl.ds(0, 15)], recv_sems.at[9])
    raw2 = [mixed_all[2 * q : 2 * q + 2].astype(F32).reshape(48, 128) for q in range(8)]
    sq2[pair] = row_squares(raw2)
    lhs2 = unpacked([raw2[q] * gains[q, 1:2, :] for q in range(8)])
    for q in range(4):
        up_out[q] = jnp.dot(
            lhs2, w_up[q].reshape(512, 128), preferred_element_type=F32
        ).astype(BF16)
    for dz in (4, 2, 6):
        copy_to(up_out.at[zs[dz] // 2], up_in.at[pair], 11, kvs[dz][0], t).start()
        copy_to(sq2.at[pair], sq2.at[pair], 10, kvs[dz][0], t).start()
    up_in[pair] = up_out[pair]
    leaving.append((sq2.at[pl.ds(0, 3)], 10))
    leaving.append((up_in.at[pl.ds(0, 3)], 11))
    wait_for(sq2.at[pl.ds(0, 3)], recv_sems.at[10])
    squares2 = sq2[0] + sq2[1] + sq2[2] + sq2[3]
    scale2 = jnp.concatenate(
        [
            lax.rsqrt(column_of(squares2[q : q + 1, :], 0, 48, 48) / WIDTH + NORM_EPS)
            for q in range(2)
        ],
        axis=0,
    )
    wait_for(up_in.at[pl.ds(0, 3)], recv_sems.at[11])

    total = up_in[0].astype(F32)
    for q in range(1, 4):
        total = total + up_in[q].astype(F32)
    total = jnp.maximum(total * scale2, 0.0)
    hidden_all[pair] = (total * total).astype(BF16)
    own_hidden = hidden_all.at[pair]
    for dz in (4, 2, 6):
        copy_to(own_hidden, own_hidden, 12, kvs[dz][0], t, hidden_sems.at[pair]).start()
    leaving.append((hidden_all.at[pl.ds(0, 3)], 12))
    wait_for(w_down.at[pl.ds(0, 3)], recv_sems.at[15])

    partial3 = jnp.zeros((96, 512), F32)
    for dz in (0, 2, 6, 4):
        pq = zs[dz] // 2
        if dz:
            wait_for(hidden_all.at[pq], hidden_sems.at[pq])
        partial3 = partial3 + dot_t(hidden_all[pq], w_down[pq].reshape(512, 128))
    for half in range(2):
        for two in range(4):
            upper = partial3[24 * half : 24 * half + 24, 128 * two : 128 * two + 128]
            lower = partial3[48 + 24 * half : 72 + 24 * half, 128 * two : 128 * two + 128]
            down_out[4 * two + half] = jnp.where(low, upper, swap_lanes(lower)).astype(BF16)
            down_out[4 * two + 2 + half] = jnp.where(low, swap_lanes(upper), lower).astype(BF16)
    for dp, dx, dc in ROW:
        copy_to(
            down_out.at[2 * (pair_odd[dp] * NX + xs[dx]) + cores[dc]],
            down_in.at[own_at],
            13,
            pair_kvs[dp][dx],
            ts[0][dc],
        ).start()
    down_in[own_at] = down_out[own_at]
    leaving.append((down_in.at[pl.ds(0, 15)], 13))
    wait_for(down_in.at[pl.ds(0, 15)], recv_sems.at[13])
    total = down_in[0].astype(F32)
    for q in range(1, 16):
        total = total + down_in[q].astype(F32)
    total = mixed_all[own_at].astype(F32) + total
    out_ref[...] = jnp.concatenate([total[:, 0:64], total[:, 64:128]], axis=0).astype(BF16)

    finish()


def place(out_v, next_v, out_hbm, next_hbm, sems):
    copies = [
        pltpu.make_async_copy(
            next_v.at[pl.ds(2 * q, 2)], next_hbm.at[pl.ds(2 * q, 2)], sems.at[q]
        )
        for q in range(6)
    ]
    copies.append(pltpu.make_async_copy(out_v, out_hbm, sems.at[6]))
    for copy in copies:
        copy.start()
    for copy in copies:
        copy.wait()


def body(
    tokens,
    norm_gain,
    w_query,
    w_forget,
    w_input,
    w_gate,
    lower_bound,
    head_gain,
    recur_state,
    w_out,
    mixer_gain,
    w_up,
    w_down,
):
    bound = lower_bound.reshape(2, 128)
    any_spec = pl.BlockSpec(memory_space=pltpu.HBM)
    vmem_spec = pl.BlockSpec(memory_space=pltpu.VMEM)
    out, next_state = pl.pallas_call(
        kernel,
        out_shape=(
            jax.ShapeDtypeStruct(tokens.shape, tokens.dtype),
            jax.ShapeDtypeStruct(recur_state.shape, recur_state.dtype),
        ),
        in_specs=[any_spec] * 13,
        out_specs=(vmem_spec, vmem_spec),
        scratch_shapes=[
            pltpu.VMEM((48, 64), BF16),
            pltpu.VMEM((2, 1, 64), F32),
            pltpu.VMEM((4, 64, 256), BF16),
            pltpu.VMEM((2, 128), F32),
            pltpu.VMEM((2, 128), F32),
            pltpu.VMEM((12, 2, 128, 128), F32),
            pltpu.VMEM((64, 256), BF16),
            pltpu.VMEM((64, 1024), BF16),
            pltpu.VMEM((64, 1024), BF16),
            pltpu.VMEM((8, 2, 128), F32),
            pltpu.VMEM((4, 64, 256), BF16),
            pltpu.VMEM((4, 8, 64, 128), BF16),
            pltpu.VMEM((4, 8, 64, 128), BF16),
            pltpu.VMEM((8, 64, 256), BF16),
            pltpu.VMEM((32, 24, 128), BF16),
            pltpu.VMEM((8, 2, 256), F32),
            pltpu.VMEM((32, 24, 128), BF16),
            pltpu.VMEM((32, 24, 128), BF16),
            pltpu.VMEM((24, 128), BF16),
            pltpu.VMEM((32, 24, 128), BF16),
            pltpu.VMEM((16, 24, 128), BF16),
            pltpu.VMEM((4, 2, 128), F32),
            pltpu.VMEM((4, 96, 128), BF16),
            pltpu.VMEM((4, 96, 128), BF16),
            pltpu.VMEM((4, 96, 128), BF16),
            pltpu.VMEM((16, 24, 128), BF16),
            pltpu.VMEM((16, 24, 128), BF16),
            pltpu.VMEM((24, 128), F32),
            pltpu.SemaphoreType.DMA((13,)),
            pltpu.SemaphoreType.DMA((16,)),
            pltpu.SemaphoreType.DMA((16,)),
            pltpu.SemaphoreType.DMA((8,)),
            pltpu.SemaphoreType.REGULAR,
        ],
        compiler_params=pltpu.CompilerParams(collective_id=0, has_side_effects=True, vmem_limit_bytes=16 * 1024 * 1024),
        name="decode_layer",
    )(*(pltpu.with_memory_space_constraint(a, pltpu.HBM) for a in (
        tokens,
        norm_gain.reshape(1, 64),
        mixer_gain.reshape(1, 64),
        w_query,
        w_forget,
        w_input,
        w_gate,
        bound,
        head_gain,
        recur_state,
        w_out.T,
        w_up,
        w_down.T,
    )))
    return pl.pallas_call(
        place,
        out_shape=(
            jax.ShapeDtypeStruct(out.shape, out.dtype),
            jax.ShapeDtypeStruct(next_state.shape, next_state.dtype),
        ),
        in_specs=[vmem_spec, vmem_spec],
        out_specs=(any_spec, any_spec),
        scratch_shapes=[pltpu.SemaphoreType.DMA((7,))],
        compiler_params=pltpu.CompilerParams(vmem_limit_bytes=4 * 1024 * 1024),
        name="place_outputs",
    )(out, next_state)


def solution(mesh):
    in_specs = (
        P("tp", "kv"),
        P("kv"),
        P("kv", "tp"),
        P("kv", "tp"),
        P("kv", "tp"),
        P("kv", "tp"),
        P("tp"),
        P("tp", None),
        P("kv", "tp", None, None),
        P("tp", "kv"),
        P("kv"),
        P("kv", "tp"),
        P("tp", "kv"),
    )
    out_specs = (P("tp", "kv"), P("kv", "tp", None, None))
    return jax.shard_map(body, mesh=mesh, in_specs=in_specs, out_specs=out_specs, check_vma=False)
```

```python
import itertools

import jax
import jax.numpy as jnp
from jax import lax
from jax.experimental import pallas as pl
from jax.experimental.pallas import tpu as pltpu
from jax.sharding import PartitionSpec as P

NORM_EPS = 1e-05
MESH = pl.DeviceIdType.MESH
F32 = jnp.float32
BF16 = jnp.bfloat16

NZ, NX, NT = 8, 4, 8
WIDTH = 2048.0


def hops(step, size):
    return min(step, size - step)


def by_distance(sizes):
    steps = list(itertools.product(*(range(n) for n in sizes)))[1:]
    return sorted(steps, key=lambda d: (-sum(hops(s, n) for s, n in zip(d, sizes)), d))


PLANE = by_distance((4, 4, 2))
COLUMN = by_distance((8, 4))
ALONG_X = by_distance((4,))
ALONG_Y = by_distance((4, 2))
PAIR = by_distance((2, 4))
ROW = by_distance((2, 4, 2))
ALONG_Z = by_distance((8,))
NEAR_Z = [0, 1, 7, 2, 6, 3, 5, 4]


def wait_for(ref, sem):
    pltpu.make_async_copy(ref, ref, sem).wait()


def swap_lanes(value):
    return pltpu.roll(value, 64, 1)


def dot_t(a, b):
    return lax.dot_general(a, b, (((1,), (1,)), ((), ())), preferred_element_type=F32)


def low_lanes(shape):
    return lax.broadcasted_iota(jnp.int32, shape, 1) < 64


def unpacked(pieces):
    low = low_lanes(pieces[0].shape)
    swapped = [swap_lanes(p) for p in pieces]
    first = [jnp.where(low, pieces[i], swapped[i + 1]).astype(BF16) for i in range(0, len(pieces), 2)]
    second = [jnp.where(low, swapped[i], pieces[i + 1]).astype(BF16) for i in range(0, len(pieces), 2)]
    return jnp.concatenate(
        [jnp.concatenate(first, axis=1), jnp.concatenate(second, axis=1)], axis=0
    )


def row_squares(pieces):
    total = pieces[0] * pieces[0]
    for p in pieces[1:]:
        total = total + p * p
    spare = -total.shape[0] % 128
    total = jnp.concatenate([total, jnp.zeros((spare, 128), F32)], axis=0)
    high = total.astype(BF16)
    rest = (total - high.astype(F32)).astype(BF16)
    lane = lax.broadcasted_iota(jnp.int32, (8, 128), 1)
    row = lax.broadcasted_iota(jnp.int32, (8, 128), 0)
    pick = jnp.where((lane // 64) == row, 1.0, 0.0).astype(BF16)
    dims = (((1,), (1,)), ((), ()))
    sums = lax.dot_general(pick, high, dims, preferred_element_type=F32)
    sums = sums + lax.dot_general(pick, rest, dims, preferred_element_type=F32)
    return sums[0:2, :]


def column_of(values, base, period, rows=24):
    shape = (rows, values.shape[1])
    lane = lax.broadcasted_iota(jnp.int32, shape, 1)
    row = lax.broadcasted_iota(jnp.int32, shape, 0)
    return jnp.sum(
        jnp.where(lane == base + row % period, values, 0.0), axis=1, keepdims=True
    )


def kernel(
    tokens_hbm,
    norm_gain_hbm,
    mixer_gain_hbm,
    wq_hbm,
    wf_hbm,
    wi_hbm,
    wg_hbm,
    bound_hbm,
    head_gain_hbm,
    state_hbm,
    wout_hbm,
    wup_hbm,
    wdown_hbm,
    out_ref,
    next_v,
    tok_v,
    gain_v,
    w4_v,
    bound_v,
    head_gain_v,
    state_v,
    wout_v,
    wup_v,
    wdown_v,
    gains,
    w_first,
    w_up,
    w_down,
    w_out,
    tok_all,
    sq1,
    proj_out,
    proj_in,
    mix_own,
    mix_all,
    mixed_all,
    sq2,
    up_out,
    up_in,
    hidden_all,
    down_out,
    down_in,
    read_v,
    in_sems,
    send_sems,
    recv_sems,
    hidden_sems,
    far_sem,
):
    kv, t = lax.axis_index("kv"), lax.axis_index("tp")
    z, x = kv // NX, kv % NX
    y, core = t // 2, t % 2
    has_self = t == z

    xs = [(x + d) % 4 for d in range(4)]
    ys = [(y + d) % 4 for d in range(4)]
    zs = [(z + d) % 8 for d in range(8)]
    cores = [core, 1 - core]
    kvs = [[pz * NX + px for px in xs] for pz in zs]
    ts = [[2 * py + pc for pc in cores] for py in ys]

    def copy_to(src, dst, k, pkv, pt, arrived=None):
        return pltpu.make_async_remote_copy(
            src_ref=src,
            dst_ref=dst,
            send_sem=send_sems.at[k],
            recv_sem=recv_sems.at[k] if arrived is None else arrived,
            device_id=(pkv, pt),
            device_id_type=MESH,
        )

    leaving, mix_sent = [], []

    def finish():
        for ref, k in leaving:
            wait_for(ref, send_sems.at[k])
        if mix_sent:
            @pl.when(has_self)
            def _():
                wait_for(mix_all.at[pl.ds(0, 31)], send_sems.at[8])

            @pl.when(jnp.logical_not(has_self))
            def _():
                wait_for(mix_all, send_sems.at[8])

    pair, odd = z // 2, z % 2
    pair_kvs = [kvs[0], [(z + 1 - 2 * odd) * NX + px for px in xs]]
    pair_odd = [odd, 1 - odd]
    in_pair = odd * NX + x

    barrier = pltpu.get_barrier_semaphore()

    def tell(pkv, pt):
        pl.semaphore_signal(barrier, inc=1, device_id=(pkv, pt), device_id_type=MESH)

    for dx, dy, dc in PLANE:
        tell(kvs[0][dx], ts[dy][dc])
    for dz in (2, 6, 1, 7):
        for dx in (2, 1, 3, 0):
            tell(kvs[dz][dx], t)

    loads = [
        pltpu.make_async_copy(tokens_hbm, tok_v, in_sems.at[0]),
        pltpu.make_async_copy(norm_gain_hbm, gain_v.at[0], in_sems.at[1]),
        pltpu.make_async_copy(wq_hbm, w4_v.at[0], in_sems.at[2]),
        pltpu.make_async_copy(wf_hbm, w4_v.at[1], in_sems.at[3]),
        pltpu.make_async_copy(wi_hbm, w4_v.at[2], in_sems.at[4]),
        pltpu.make_async_copy(wg_hbm, w4_v.at[3], in_sems.at[5]),
        pltpu.make_async_copy(wout_hbm, wout_v, in_sems.at[6]),
        pltpu.make_async_copy(wup_hbm, wup_v, in_sems.at[7]),
        pltpu.make_async_copy(wdown_hbm, wdown_v, in_sems.at[8]),
        pltpu.make_async_copy(bound_hbm, bound_v, in_sems.at[9]),
        pltpu.make_async_copy(head_gain_hbm, head_gain_v, in_sems.at[10]),
        pltpu.make_async_copy(state_hbm, state_v, in_sems.at[11]),
        pltpu.make_async_copy(mixer_gain_hbm, gain_v.at[1], in_sems.at[12]),
    ]
    for load in loads:
        load.start()

    def units_of(px, p):
        return pl.ds(pl.multiple_of(px * 256 + p * 128, 128), 128)

    loads[0].wait()
    tok_f = tok_v[...].astype(F32)
    tok_all[x * NT + t] = jnp.concatenate([tok_f[0:24], tok_f[24:48]], axis=1).astype(BF16)
    loads[1].wait()
    loads[12].wait()
    for q in range(2):
        g = gain_v[q]
        gains[in_pair, q : q + 1, :] = jnp.concatenate([g, g], axis=1)
    for k in range(2, 9):
        loads[k].wait()
    w_first[x] = w4_v[x]
    w_up[y, in_pair] = wup_v[:, units_of(x, odd)]
    w_out[t] = wout_v[...]
    w_down[y, in_pair] = wdown_v[:, units_of(x, odd)]

    pl.semaphore_wait(barrier, 31 + 16)
    for step in (2, 6):
        pl.semaphore_signal(
            far_sem, inc=1, device_id=(kvs[step][0], t), device_id_type=MESH
        )

    for dp, dx in PAIR:
        copy_to(gains.at[in_pair], gains.at[in_pair], 1, pair_kvs[dp][dx], t).start()
    own_tok = tok_all.at[x * NT + t]
    for dx, dy, dc in PLANE:
        copy_to(own_tok, own_tok, 0, kvs[0][dx], ts[dy][dc]).start()
    for (dx,) in ALONG_X:
        copy_to(w4_v.at[xs[dx]], w_first.at[x], 2, kvs[0][dx], t).start()
    leaving.append((tok_all.at[pl.ds(0, 31)], 0))
    leaving.append((gains.at[pl.ds(0, 7)], 1))
    leaving.append((w_first.at[pl.ds(0, 3)], 2))
    wait_for(gains.at[pl.ds(0, 7)], recv_sems.at[1])
    wait_for(tok_all.at[pl.ds(0, 31)], recv_sems.at[0])


    raw = [
        tok_all[pl.ds(NT * q, NT)].astype(F32).reshape(192, 128) for q in range(NX)
    ]
    sq1[z] = row_squares(raw)
    lhs = unpacked([raw[q] * gains[odd * NX + q, 0:1, :] for q in range(NX)])
    wait_for(w_first.at[pl.ds(0, 3)], recv_sems.at[2])
    partial = jnp.dot(lhs, w_first[...].reshape(256, 256), preferred_element_type=F32)

    for half in range(2):
        for pz in range(NZ):
            at = half * 192 + pz * 24
            left = partial[at : at + 24, 0:128]
            right = partial[at : at + 24, 128:256]
            proj_out[pz * NX + 2 * half] = jnp.concatenate(
                [left[0:12], right[0:12]], axis=0
            ).astype(BF16)
            proj_out[pz * NX + 2 * half + 1] = jnp.concatenate(
                [left[12:24], right[12:24]], axis=0
            ).astype(BF16)

    pl.semaphore_wait(far_sem, 2)

    for (dz,) in ALONG_Z:
        copy_to(sq1.at[z], sq1.at[z], 4, kvs[dz][0], t).start()
    for dz, dx in COLUMN:
        copy_to(proj_out.at[kvs[dz][dx]], proj_in.at[kv], 5, kvs[dz][dx], t).start()
    proj_in[kv] = proj_out[kv]
    leaving.append((sq1.at[pl.ds(0, 7)], 4))
    leaving.append((proj_in.at[pl.ds(0, 31)], 5))
    for dy, dc in ALONG_Y:
        copy_to(w_out.at[t], w_out.at[t], 3, kv, ts[dy][dc]).start()
    leaving.append((w_out.at[pl.ds(0, 7)], 3))
    for dp, dx in PAIR:
        cols = units_of(xs[dx], pair_odd[dp])
        copy_to(wup_v.at[:, cols], w_up.at[y, in_pair], 6, pair_kvs[dp][dx], t).start()
        copy_to(wdown_v.at[:, cols], w_down.at[y, in_pair], 7, pair_kvs[dp][dx], t).start()
    leaving.append((w_up.at[0, pl.ds(0, 7)], 6))
    leaving.append((w_up.at[0, pl.ds(0, 7)], 7))


    for k in range(9, 12):
        loads[k].wait()
    wait_for(sq1.at[pl.ds(0, 7)], recv_sems.at[4])
    wait_for(proj_in.at[pl.ds(0, 31)], recv_sems.at[5])

    squares = sq1[0]
    for q in range(1, NZ):
        squares = squares + sq1[q]
    square_row = jnp.where(x // 2 == 0, squares[0:1, :], squares[1:2, :])
    row_scale = lax.rsqrt(
        column_of(square_row, z * 24 + (x % 2) * 12, 12) / WIDTH + NORM_EPS
    )
    owned = []
    for q in range(NX):
        total = proj_in[q].astype(F32)
        for r in range(1, NZ):
            total = total + proj_in[r * NX + q].astype(F32)
        owned.append(total * row_scale)
    queries, forget_raw, values_in, gate_raw = owned
    head0 = lax.broadcasted_iota(jnp.int32, (24, 128), 0) < 12
    bound = jnp.where(head0, bound_v[0:1, :], bound_v[1:2, :])
    head_gain = jnp.where(head0, head_gain_v[0:1, :], head_gain_v[1:2, :])
    forget = bound + (1.0 - bound) * jax.nn.sigmoid(forget_raw)
    pad = jnp.zeros((104, 128), F32)
    kept = queries * forget
    kept_t = jnp.concatenate([kept, pad], axis=0).T
    fresh = jnp.sum(queries * (1.0 - forget), axis=1, keepdims=True) * values_in
    for j in range(24):
        read_v[j : j + 1, :] = jnp.sum(
            kept_t[:, j : j + 1] * state_v[j % 12, j // 12], axis=0, keepdims=True
        )
    read = read_v[...] + fresh
    read = read * lax.rsqrt(jnp.mean(read * read, axis=1, keepdims=True) + NORM_EPS) * head_gain
    mix_own[...] = (read * jax.nn.silu(gate_raw)).astype(BF16)

    mix_at = t * NX + x
    for dz, dx in COLUMN:
        copy_to(mix_own, mix_all.at[mix_at], 8, kvs[dz][dx], z).start()

    @pl.when(jnp.logical_not(has_self))
    def _():
        copy_to(mix_own, mix_all.at[mix_at], 8, kv, z).start()

    @pl.when(has_self)
    def _():
        mix_all[mix_at] = mix_own[...]

    wait_for(w_up.at[0, pl.ds(0, 7)], recv_sems.at[6])
    for (dy,) in ALONG_X:
        copy_to(w_up.at[y], w_up.at[y], 14, kv, ts[dy][0]).start()
    leaving.append((w_up.at[pl.ds(0, 3)], 14))
    mix_sent.append(1)
    forget_t = jnp.concatenate([forget, pad], axis=0).T
    for j in range(24):
        f = forget_t[:, j : j + 1]
        next_v[j % 12, j // 12] = f * state_v[j % 12, j // 12] + (1.0 - f) * values_in[j : j + 1, :]
    wait_for(w_out.at[pl.ds(0, 7)], recv_sems.at[3])

    @pl.when(has_self)
    def _():
        wait_for(mix_all.at[pl.ds(0, 31)], recv_sems.at[8])

    @pl.when(jnp.logical_not(has_self))
    def _():
        wait_for(mix_all, recv_sems.at[8])

    acc = jnp.zeros((96, 128), F32)
    for q in range(NT):
        both = jnp.concatenate([w_out[q, :, 0:128], w_out[q, :, 128:256]], axis=0)
        acc = acc + dot_t(mix_all[4 * q : 4 * q + 4].reshape(96, 128), both)
    folded = []
    for q in range(NX):
        part = acc[24 * q : 24 * q + 24]
        turned = swap_lanes(jnp.concatenate([part[12:24], part[0:12]], axis=0))
        folded.append(part + turned)
    low = low_lanes((24, 128))
    top = jnp.where(low, folded[0], swap_lanes(folded[2]))
    bottom = jnp.where(low, swap_lanes(folded[1]), folded[3])
    attn = jnp.where(head0, top, bottom)
    own_at = 2 * in_pair + core
    mixed_all[own_at] = (tok_all[x * NT + t].astype(F32) + attn).astype(BF16)

    own_mixed = mixed_all.at[own_at]
    for dp, dx, dc in ROW:
        copy_to(own_mixed, own_mixed, 9, pair_kvs[dp][dx], ts[0][dc]).start()
    leaving.append((mixed_all.at[pl.ds(0, 15)], 9))

    wait_for(w_up.at[0, pl.ds(0, 7)], recv_sems.at[7])
    for (dy,) in ALONG_X:
        copy_to(w_down.at[y], w_down.at[y], 15, kv, ts[dy][0]).start()
    leaving.append((w_down.at[pl.ds(0, 3)], 15))
    wait_for(w_up.at[pl.ds(0, 3)], recv_sems.at[14])
    wait_for(mixed_all.at[pl.ds(0, 15)], recv_sems.at[9])
    raw2 = [mixed_all[2 * q : 2 * q + 2].astype(F32).reshape(48, 128) for q in range(8)]
    sq2[pair] = row_squares(raw2)
    lhs2 = unpacked([raw2[q] * gains[q, 1:2, :] for q in range(8)])
    for q in range(4):
        up_out[q] = jnp.dot(
            lhs2, w_up[q].reshape(512, 128), preferred_element_type=F32
        ).astype(BF16)
    for dz in (4, 2, 6):
        copy_to(up_out.at[zs[dz] // 2], up_in.at[pair], 11, kvs[dz][0], t).start()
        copy_to(sq2.at[pair], sq2.at[pair], 10, kvs[dz][0], t).start()
    up_in[pair] = up_out[pair]
    leaving.append((sq2.at[pl.ds(0, 3)], 10))
    leaving.append((up_in.at[pl.ds(0, 3)], 11))
    wait_for(sq2.at[pl.ds(0, 3)], recv_sems.at[10])
    squares2 = sq2[0] + sq2[1] + sq2[2] + sq2[3]
    scale2 = jnp.concatenate(
        [
            lax.rsqrt(column_of(squares2[q : q + 1, :], 0, 48, 48) / WIDTH + NORM_EPS)
            for q in range(2)
        ],
        axis=0,
    )
    wait_for(up_in.at[pl.ds(0, 3)], recv_sems.at[11])

    total = up_in[0].astype(F32)
    for q in range(1, 4):
        total = total + up_in[q].astype(F32)
    total = jnp.maximum(total * scale2, 0.0)
    hidden_all[pair] = (total * total).astype(BF16)
    own_hidden = hidden_all.at[pair]
    for dz in (4, 2, 6):
        copy_to(own_hidden, own_hidden, 12, kvs[dz][0], t, hidden_sems.at[pair]).start()
    leaving.append((hidden_all.at[pl.ds(0, 3)], 12))
    wait_for(w_down.at[pl.ds(0, 3)], recv_sems.at[15])

    partial3 = jnp.zeros((96, 512), F32)
    for dz in (0, 2, 6, 4):
        pq = zs[dz] // 2
        if dz:
            wait_for(hidden_all.at[pq], hidden_sems.at[pq])
        partial3 = partial3 + dot_t(hidden_all[pq], w_down[pq].reshape(512, 128))
    for half in range(2):
        for two in range(4):
            upper = partial3[24 * half : 24 * half + 24, 128 * two : 128 * two + 128]
            lower = partial3[48 + 24 * half : 72 + 24 * half, 128 * two : 128 * two + 128]
            down_out[4 * two + half] = jnp.where(low, upper, swap_lanes(lower)).astype(BF16)
            down_out[4 * two + 2 + half] = jnp.where(low, swap_lanes(upper), lower).astype(BF16)
    for dp, dx, dc in ROW:
        copy_to(
            down_out.at[2 * (pair_odd[dp] * NX + xs[dx]) + cores[dc]],
            down_in.at[own_at],
            13,
            pair_kvs[dp][dx],
            ts[0][dc],
        ).start()
    down_in[own_at] = down_out[own_at]
    leaving.append((down_in.at[pl.ds(0, 15)], 13))
    wait_for(down_in.at[pl.ds(0, 15)], recv_sems.at[13])
    total = down_in[0].astype(F32)
    for q in range(1, 16):
        total = total + down_in[q].astype(F32)
    total = mixed_all[own_at].astype(F32) + total
    out_ref[...] = jnp.concatenate([total[:, 0:64], total[:, 64:128]], axis=0).astype(BF16)

    finish()


def place(out_v, next_v, out_hbm, next_hbm, sems):
    copies = [
        pltpu.make_async_copy(
            next_v.at[pl.ds(2 * q, 2)], next_hbm.at[pl.ds(2 * q, 2)], sems.at[q]
        )
        for q in range(6)
    ]
    copies.append(pltpu.make_async_copy(out_v, out_hbm, sems.at[6]))
    for copy in copies:
        copy.start()
    for copy in copies:
        copy.wait()


def body(
    tokens,
    norm_gain,
    w_query,
    w_forget,
    w_input,
    w_gate,
    lower_bound,
    head_gain,
    recur_state,
    w_out,
    mixer_gain,
    w_up,
    w_down,
):
    bound = lower_bound.reshape(2, 128)
    any_spec = pl.BlockSpec(memory_space=pltpu.HBM)
    vmem_spec = pl.BlockSpec(memory_space=pltpu.VMEM)
    out, next_state = pl.pallas_call(
        kernel,
        out_shape=(
            jax.ShapeDtypeStruct(tokens.shape, tokens.dtype),
            jax.ShapeDtypeStruct(recur_state.shape, recur_state.dtype),
        ),
        in_specs=[any_spec] * 13,
        out_specs=(vmem_spec, vmem_spec),
        scratch_shapes=[
            pltpu.VMEM((48, 64), BF16),
            pltpu.VMEM((2, 1, 64), F32),
            pltpu.VMEM((4, 64, 256), BF16),
            pltpu.VMEM((2, 128), F32),
            pltpu.VMEM((2, 128), F32),
            pltpu.VMEM((12, 2, 128, 128), F32),
            pltpu.VMEM((64, 256), BF16),
            pltpu.VMEM((64, 1024), BF16),
            pltpu.VMEM((64, 1024), BF16),
            pltpu.VMEM((8, 2, 128), F32),
            pltpu.VMEM((4, 64, 256), BF16),
            pltpu.VMEM((4, 8, 64, 128), BF16),
            pltpu.VMEM((4, 8, 64, 128), BF16),
            pltpu.VMEM((8, 64, 256), BF16),
            pltpu.VMEM((32, 24, 128), BF16),
            pltpu.VMEM((8, 2, 256), F32),
            pltpu.VMEM((32, 24, 128), BF16),
            pltpu.VMEM((32, 24, 128), BF16),
            pltpu.VMEM((24, 128), BF16),
            pltpu.VMEM((32, 24, 128), BF16),
            pltpu.VMEM((16, 24, 128), BF16),
            pltpu.VMEM((4, 2, 128), F32),
            pltpu.VMEM((4, 96, 128), BF16),
            pltpu.VMEM((4, 96, 128), BF16),
            pltpu.VMEM((4, 96, 128), BF16),
            pltpu.VMEM((16, 24, 128), BF16),
            pltpu.VMEM((16, 24, 128), BF16),
            pltpu.VMEM((24, 128), F32),
            pltpu.SemaphoreType.DMA((13,)),
            pltpu.SemaphoreType.DMA((16,)),
            pltpu.SemaphoreType.DMA((16,)),
            pltpu.SemaphoreType.DMA((8,)),
            pltpu.SemaphoreType.REGULAR,
        ],
        compiler_params=pltpu.CompilerParams(collective_id=0, has_side_effects=True, vmem_limit_bytes=16 * 1024 * 1024),
        name="decode_layer",
    )(*(pltpu.with_memory_space_constraint(a, pltpu.HBM) for a in (
        tokens,
        norm_gain.reshape(1, 64),
        mixer_gain.reshape(1, 64),
        w_query,
        w_forget,
        w_input,
        w_gate,
        bound,
        head_gain,
        recur_state,
        w_out.T,
        w_up,
        w_down.T,
    )))
    return pl.pallas_call(
        place,
        out_shape=(
            jax.ShapeDtypeStruct(out.shape, out.dtype),
            jax.ShapeDtypeStruct(next_state.shape, next_state.dtype),
        ),
        in_specs=[vmem_spec, vmem_spec],
        out_specs=(any_spec, any_spec),
        scratch_shapes=[pltpu.SemaphoreType.DMA((7,))],
        compiler_params=pltpu.CompilerParams(vmem_limit_bytes=4 * 1024 * 1024),
        name="place_outputs",
    )(out, next_state)


def solution(mesh):
    in_specs = (
        P("tp", "kv"),
        P("kv"),
        P("kv", "tp"),
        P("kv", "tp"),
        P("kv", "tp"),
        P("kv", "tp"),
        P("tp"),
        P("tp", None),
        P("kv", "tp", None, None),
        P("tp", "kv"),
        P("kv"),
        P("kv", "tp"),
        P("tp", "kv"),
    )
    out_specs = (P("tp", "kv"), P("kv", "tp", None, None))
    return jax.shard_map(body, mesh=mesh, in_specs=in_specs, out_specs=out_specs, check_vma=False)
```
